32 devices in a mesh: gr: 2 (over core), sp: 8 (over z, y), tp: 2 (over x).
Axes of the slice: x: 2, y: 2, z: 4, core: 2. Of those that a mesh axis runs over, the one named last changes fastest.
Arguments:
- tokens: bfloat16 [4, 2048, 2048], P('gr', ('sp', 'tp')), parts along dimension 0, may hold values from -6 to 6
- key_weight: bfloat16 [2048, 1024], P('sp'), may hold values from -0.125 to 0.125
- value_weight: bfloat16 [2048, 1024], P('sp'), may hold values from -0.125 to 0.125
- queries: bfloat16 [4, 1024], P('gr'), parts along dimension 0, may hold values from -6 to 6
- head_offset: float32 [16], replicated, may hold values from -14 to -3.5
- key_bias: bfloat16 [4, 2048, 16], P('gr', ('sp', 'tp')), parts along dimension 0, may hold values from -0.5 to 12.9
Outputs:
- key_cache: bfloat16 [4, 2048, 1024], P('gr', 'sp', 'tp'), parts along dimension 0
- value_cache: bfloat16 [4, 2048, 1024], P('gr', 'sp', 'tp'), parts along dimension 0
- bias_cache: bfloat16 [4, 2048, 16], P('gr', 'sp', 'tp'), parts along dimension 0
- reading: float32 [4, 1024], P('gr', 'tp'), parts along dimension 0
The draws below stay inside these ranges and needn't reach their ends.
There are 2 independent parts, one for each index of `gr`. The reference program is written for one: setup_inputs(seed, part) draws one part's arguments, and reference() takes and returns one part's arrays. A program takes and returns all parts, laid end to end along the dimension named above; an argument that names none is the same for every part. Nothing has to cross between parts.
All inputs are finite; a program needn't handle non-finite values.
Results may differ from the reference program's by a relative error of at most 0.0052.
Values may be sent and summed in bfloat16 or wider, within the bound.
A program may use at most 64 MiB of HBM per device.

```python
import jax
import jax.numpy as jnp
from jax import lax

D = 2048
HEADS = 16
HEAD_DIM = 64
GROUP_SEQUENCES = 2
POS_DEV = 128
PROMPT_LENGTH = 2048


def draw_head_offset(key, part):
    key_a, key_b, key_c, order_key = jax.random.split(jax.random.fold_in(key, 11), 4)
    scale_base = jnp.log(jnp.float32(PROMPT_LENGTH) * 14.6)
    slow_rate = jnp.log(jax.random.uniform(key_a, (HEADS,), jnp.float32, 1.0, 2.3)) - scale_base
    middle_rate = jnp.log(jax.random.uniform(key_c, (HEADS,), jnp.float32, 5.0, 9.0)) - scale_base
    fast_rate = jax.random.uniform(key_b, (HEADS,), jnp.float32, -5.0, -3.5)
    ranks = jax.random.permutation(order_key, HEADS)
    chosen = jnp.where(ranks < HEADS // 2, slow_rate, jnp.where(ranks < 3 * HEADS // 4, middle_rate, fast_rate))
    return chosen.astype(jnp.float32)


def draw_key_bias(key, part):
    key_a, key_b, third_random_key, fourth_random_key = jax.random.split(jax.random.fold_in(key, 23), 4)
    block_count = PROMPT_LENGTH // POS_DEV
    block_tier = jax.random.uniform(key_a, (GROUP_SEQUENCES, block_count, 1, HEADS), jnp.float32, 0.0, 3.4)
    block_tier = jnp.broadcast_to(block_tier, (GROUP_SEQUENCES, block_count, POS_DEV, HEADS)).reshape(GROUP_SEQUENCES, PROMPT_LENGTH, HEADS)
    coarse_portion = jnp.clip(0.25 * jax.random.normal(key_b, (GROUP_SEQUENCES, PROMPT_LENGTH, HEADS), jnp.float32), -0.5, 0.5)
    spike_places = jax.random.randint(third_random_key, (GROUP_SEQUENCES, 3), 0, PROMPT_LENGTH)
    spike_mask = jnp.any(jnp.arange(PROMPT_LENGTH)[None, :, None] == spike_places[:, None, :], axis=-1)
    spike_length = jax.random.uniform(fourth_random_key, (GROUP_SEQUENCES, PROMPT_LENGTH, 1), jnp.float32, 7.5, 9.0)
    grand_sum = block_tier + coarse_portion + jnp.where(spike_mask[:, :, None], spike_length, 0.0)
    return grand_sum.astype(jnp.bfloat16)


def levels(stream_key, shape, shards, smallest, high):
    factor_of = 1.0
    for dim, parts in shards:
        heights = jax.random.uniform(jax.random.fold_in(jax.random.fold_in(stream_key, 6), dim), (parts,), jnp.float32, smallest / len(shards), high / len(shards))
        factor_of = factor_of * jnp.repeat(jnp.exp(heights), shape[dim] // parts).reshape((-1,) + (1,) * (len(shape) - 1 - dim))
    return factor_of


def scatter_about(own_key, dims, scale, reach, pieces=(), kind=jnp.bfloat16):
    result = jax.random.normal(own_key, dims, jnp.float32) * scale
    if len(pieces) > 0:
        result = levels(own_key, dims, pieces, -0.22, 0.18) * result
    return jnp.clip(result, min=-reach, max=reach).astype(kind)


def setup_inputs(seed: int = 0, part: int = 0) -> dict:
    arg_keys = jax.random.split(jax.random.key(seed), 7)
    part_splits = jax.random.split(jax.random.fold_in(arg_keys[6], part), 7)
    return {
        "tokens": scatter_about(part_splits[0], (GROUP_SEQUENCES, PROMPT_LENGTH, D), 1.0, 6.0, ((1, 16),)),
        "key_weight": scatter_about(arg_keys[1], (D, HEADS * HEAD_DIM), D ** -0.5, 0.125, ((0, 8),)),
        "value_weight": scatter_about(arg_keys[2], (D, HEADS * HEAD_DIM), D ** -0.5, 0.125, ((0, 8),)),
        "queries": scatter_about(part_splits[3], (GROUP_SEQUENCES, HEADS * HEAD_DIM), 1.0, 6.0),
        "head_offset": draw_head_offset(jax.random.fold_in(arg_keys[6], 71), part),
        "key_bias": draw_key_bias(jax.random.fold_in(jax.random.fold_in(arg_keys[6], part), 71), part),
    }


def reference(tokens, key_weight, value_weight, queries, head_offset, key_bias):
    score_scale = HEAD_DIM ** (-0.5)

    def one_sequence(inputs):
        tok_rows, key_offsets, query_row = inputs
        key_rows = jnp.dot(tok_rows, key_weight, preferred_element_type=jnp.float32).astype(jnp.bfloat16)
        value_rows = jnp.dot(tok_rows, value_weight, preferred_element_type=jnp.float32).astype(jnp.bfloat16)
        key_heads = key_rows.reshape(PROMPT_LENGTH, HEADS, HEAD_DIM).astype(jnp.float32)
        value_heads = value_rows.reshape(PROMPT_LENGTH, HEADS, HEAD_DIM).astype(jnp.float32)
        query_heads = query_row.reshape(HEADS, HEAD_DIM).astype(jnp.float32)
        logits = jnp.einsum('thc,hc->ht', key_heads, query_heads) * score_scale
        logits = logits + head_offset[:, None] + key_offsets.astype(jnp.float32).T
        fading = jax.nn.log_sigmoid(-logits)
        beyond = lax.cumsum(fading, axis=1, reverse=True) - fading
        weights = jnp.exp(jax.nn.log_sigmoid(logits) + beyond).astype(jnp.bfloat16)
        mixture = jnp.einsum('ht,thc->hc', weights.astype(jnp.float32), value_heads)
        normed = mixture * lax.rsqrt(lax.optimization_barrier(jnp.mean(mixture * mixture, axis=1, keepdims=True)) + 1e-06)
        return (key_rows, value_rows, normed.reshape(HEADS * HEAD_DIM))
    key_rows, value_rows, reading = lax.map(one_sequence, (tokens, key_bias, queries))
    return (key_rows, value_rows, key_bias, reading)
```

```python
import functools

import jax
import jax.numpy as jnp
from jax import lax
from jax.experimental import pallas as pl
from jax.experimental.pallas import tpu as pltpu
from jax.sharding import PartitionSpec as P

MESH = pl.DeviceIdType.MESH
F32 = jnp.float32
BF16 = jnp.bfloat16
SUBS = 2
MARK = 2 * SUBS
AHEAD = 2
MIX_HOP = 2


def ring_place(index, length):
    lane, row = lax.rem(index, 2), index // 2
    return row * (1 - lane) + (length - 1 - row) * lane


def ring_index(place, length):
    lane = place // (length // 2)
    row = place * (1 - lane) + (length - 1 - place) * lane
    return 2 * row + lane


def kernel(
    dims,
    tokens, key_weight, value_weight, queries, head_offset, key_bias, own_bias,
    kv, bias_out, packed,
    tok, wts, acc, bias, query, offset, bias_all, bias_own, key_rows,
    ubuf, ucat, pout, pin, plow, tot_out, tot_in,
    local_sem, ring_send, ring_recv, pair_send, pair_recv,
    tok_send, tok_recv, bias_send, bias_recv, read_send, read_recv, mix_send, mix_recv,
):
    n, tp_count, seqs, pos, width, rows, cols, heads, head_dim, rows_h = dims
    hops = n // 2
    half_rows = rows // 2
    sub_rows = half_rows // SUBS
    span = tp_count * pos
    kv_width = tp_count * cols
    me, tp, gr = lax.axis_index("sp"), lax.axis_index("tp"), lax.axis_index("gr")
    place = ring_place(me, n)

    def owner_at(step):
        return ring_index(lax.rem(place + step + n, n), n)

    right, left = owner_at(1), owner_at(-1)
    partner = 1 - gr
    col_start = pl.multiple_of(tp * cols, 128)
    chunked = (width // n) % 128 == 0
    order = [0]
    for h in range(1, hops + 1):
        order.extend([-h, h] if h < hops else [h])
    chunk = width // n if chunked else width
    my_rows = pl.ds(pl.multiple_of(tp * pos, pos), pos)

    key_copy = pltpu.make_async_copy(key_weight, key_rows, local_sem.at[6])
    query_copy = pltpu.make_async_copy(queries, query, local_sem.at[4])
    weight_copies = [
        pltpu.make_async_copy(
            w.at[:, pl.ds(col_start, cols)], wts.at[part, me], local_sem.at[part]
        )
        for part, w in enumerate((key_weight, value_weight))
    ]
    tok_copy = pltpu.make_async_copy(tokens, tok.at[:, my_rows, :], local_sem.at[2])
    bias_copy = pltpu.make_async_copy(key_bias, bias_all, local_sem.at[3])
    own_bias_copy = pltpu.make_async_copy(own_bias, bias_own, local_sem.at[7])
    offset_copy = pltpu.make_async_copy(head_offset, offset, local_sem.at[5])
    for c in (
        weight_copies[1], tok_copy, query_copy, key_copy, weight_copies[0],
        bias_copy, own_bias_copy, offset_copy,
    ):
        c.start()

    tp_peers = [lax.rem(tp + k, tp_count) for k in range(1, tp_count)]
    barrier = pltpu.get_barrier_semaphore()
    for target in ({"sp": right}, {"sp": left}, {"gr": partner}, *({"tp": p} for p in tp_peers)):
        pl.semaphore_signal(barrier, inc=1, device_id=target, device_id_type=MESH)

    def part_of(piece):
        return 1 if piece < SUBS else 0

    def rows_of(piece, core):
        return pl.ds(pl.multiple_of(core * half_rows + (piece % SUBS) * sub_rows, sub_rows), sub_rows)

    def block_of(piece, step, core):
        if piece == MARK:
            return ubuf.at[owner_at(step)]
        return wts.at[part_of(piece), owner_at(step), rows_of(piece, core), :]

    def ring_copy(direction, hop, piece, step):
        block = block_of(piece, step, gr)
        return pltpu.make_async_remote_copy(
            src_ref=block, dst_ref=block,
            send_sem=ring_send.at[direction, hop - 1, piece],
            recv_sem=ring_recv.at[direction, hop - 1, piece],
            device_id={"sp": right if direction == 0 else left}, device_id_type=MESH,
        )

    def step_of(direction, hop):
        return -hop if direction == 0 else hop

    def sent(direction, hop, piece):
        return ring_copy(direction, hop, piece, step_of(direction, hop - 1))

    def got(direction, hop, piece):
        return ring_copy(direction, hop, piece, step_of(direction, hop))

    def used(direction, hop, piece):
        return hop < hops or (hop == hops and piece % 2 == direction)

    def pair_copy(direction, hop, piece, core):
        block = block_of(piece, step_of(direction, hop), core)
        return pltpu.make_async_remote_copy(
            src_ref=block, dst_ref=block,
            send_sem=pair_send.at[direction, hop - 1, piece],
            recv_sem=pair_recv.at[direction, hop - 1, piece],
            device_id={"gr": partner}, device_id_type=MESH,
        )

    def tok_columns(i):
        if not chunked:
            return pl.ds(0, width)
        return pl.ds(pl.multiple_of(owner_at(order[i]) * chunk, 128), chunk)

    chunk_count = len(order) if chunked else 1

    def peer_of(k):
        return lax.rem(tp + k + 1, tp_count)

    def source_of(k):
        return lax.rem(tp + tp_count - k - 1, tp_count)

    def tok_move(i, k, source):
        place_rows = pl.ds(pl.multiple_of(source * pos, pos), pos)
        block = tok.at[:, place_rows, tok_columns(i)]
        return pltpu.make_async_remote_copy(
            src_ref=block, dst_ref=block,
            send_sem=tok_send.at[i, k], recv_sem=tok_recv.at[i, k],
            device_id={"tp": peer_of(k)}, device_id_type=MESH,
        )

    def bias_move(k, source, target):
        return pltpu.make_async_remote_copy(
            src_ref=bias_all.at[:, target], dst_ref=bias.at[source],
            send_sem=bias_send.at[k], recv_sem=bias_recv.at[k],
            device_id={"tp": peer_of(k)}, device_id_type=MESH,
        )

    def read_move(k, which, source, target):
        out, into = ((pout, pin), (tot_out, tot_in))[which]
        return pltpu.make_async_remote_copy(
            src_ref=out.at[target], dst_ref=into.at[source],
            send_sem=read_send.at[which, k], recv_sem=read_recv.at[which, k],
            device_id={"tp": peer_of(k)}, device_id_type=MESH,
        )

    sent_list = []

    def launch(c):
        c.start()
        sent_list.append(c)

    issued = [0]

    def send_tokens(upto):
        while issued[0] < min(upto, chunk_count):
            for k in range(tp_count - 1):
                launch(tok_move(issued[0], k, tp))
            issued[0] += 1

    def open_ring(piece):
        for direction in range(2):
            if used(direction, 1, piece):
                launch(sent(direction, 1, piece))

    def pass_on(hop, pieces):
        for piece in pieces:
            for direction in range(2):
                if not used(direction, hop, piece):
                    continue
                got(direction, hop, piece).wait_recv()
                if hop < hops and used(direction, hop + 1, piece):
                    launch(sent(direction, hop + 1, piece))
                if piece != MARK:
                    launch(pair_copy(direction, hop, piece, gr))

    value_pieces = list(range(SUBS))
    key_pieces = list(range(SUBS, 2 * SUBS))
    first_pass = value_pieces[:1] + [MARK] + value_pieces[1:]

    pl.semaphore_wait(barrier, 3 + len(tp_peers))
    weight_copies[1].wait()
    open_ring(value_pieces[0])
    tok_copy.wait()
    send_tokens(AHEAD)

    query_copy.wait()
    key_copy.wait()
    group = tp_count * rows_h
    row = lax.broadcasted_iota(jnp.int32, (group, kv_width), 0)
    col_head = lax.broadcasted_iota(jnp.int32, (group, kv_width), 1) // head_dim
    inner = lax.rem(row, rows_h)
    mine = (row // rows_h * heads + inner == col_head) & (inner < heads)
    q = query[...].astype(F32)
    q_rows = jnp.concatenate(
        [jnp.where(mine, q[s : s + 1], 0.0) for s in range(seqs)], axis=0
    ).astype(BF16)
    ubuf[me] = lax.dot_general(
        q_rows, key_rows[...], (((1,), (1,)), ((), ())), preferred_element_type=F32
    ).astype(BF16)
    for piece in value_pieces[1:]:
        open_ring(piece)
    open_ring(MARK)
    bias_copy.wait()
    for k in range(tp_count - 1):
        launch(bias_move(k, tp, peer_of(k)))
    weight_copies[0].wait()
    own_bias_copy.wait()
    offset_copy.wait()

    for hop in range(1, hops + 1):
        pass_on(hop, first_pass)
        send_tokens(AHEAD + hop)
        if hop == max(hops - 1, 1):
            for piece in key_pieces:
                open_ring(piece)

    for owner in range(n):
        ucat[:, owner * rows : (owner + 1) * rows] = ubuf[owner]
    total_heads = offset.shape[1]
    pick_row = lax.broadcasted_iota(jnp.int32, (group, total_heads), 0)
    pick_inner = lax.rem(pick_row, rows_h)
    pick = (
        lax.broadcasted_iota(jnp.int32, (group, total_heads), 1)
        == pick_row // rows_h * heads + pick_inner
    ) & (pick_inner < heads)
    offset_col = jnp.sum(jnp.where(pick, offset[...], 0.0), axis=1, keepdims=True)
    logits = []
    for s in range(seqs):
        logits.append(
            lax.dot_general(
                ucat[s * group : (s + 1) * group, :], tok[s, my_rows, :],
                (((1,), (1,)), ((), ())), preferred_element_type=F32,
            )
            * (head_dim**-0.5)
            + offset_col
            + bias_own[s].astype(F32)
        )
    logits = jnp.concatenate(logits, axis=0)
    soft = jnp.log1p(jnp.exp(-jnp.abs(logits)))
    fading = -jnp.maximum(logits, 0.0) - soft
    taking = jnp.minimum(logits, 0.0) - soft
    high = fading.astype(BF16)
    rest = fading - high.astype(F32)
    mid = rest.astype(BF16)
    low = (rest - mid.astype(F32)).astype(BF16)
    later = (
        lax.broadcasted_iota(jnp.int32, (pos, pos), 0)
        > lax.broadcasted_iota(jnp.int32, (pos, pos), 1)
    ).astype(F32).astype(BF16)
    sums = jnp.dot(
        jnp.concatenate([high, mid, low], axis=0), later, preferred_element_type=F32
    )
    m = seqs * group
    within = sums[:m] + sums[m : 2 * m] + sums[2 * m :]
    weights = jnp.exp(taking + within).astype(BF16)
    totals = jnp.sum(fading, axis=1, keepdims=True)
    spread = jnp.broadcast_to(totals, (m, 128))
    weighted = [
        jnp.dot(
            weights[s * group : (s + 1) * group], tok[s, my_rows, :],
            preferred_element_type=F32,
        )
        for s in range(seqs)
    ]
    lows = []
    for t in range(tp_count):
        at = slice(t * rows_h, (t + 1) * rows_h)
        tot_out[t] = jnp.concatenate(
            [spread[s * group + t * rows_h : s * group + (t + 1) * rows_h] for s in range(seqs)],
            axis=0,
        )
        whole = jnp.concatenate([weighted[s][at] for s in range(seqs)], axis=0)
        upper = whole.astype(BF16)
        pout[t] = upper
        plow[t] = (whole - upper.astype(F32)).astype(BF16)
    for k in range(tp_count - 1):
        for which in range(2):
            launch(read_move(k, which, tp, peer_of(k)))
    pin[tp] = pout[tp]
    tot_in[tp] = tot_out[tp]
    send_tokens(chunk_count)

    def pair_ready(hop, pieces):
        for direction in range(2):
            for piece in pieces:
                if used(direction, hop, piece):
                    pair_copy(direction, hop, piece, partner).wait_recv()

    for hop in range(1, hops + 1):
        pair_ready(hop, value_pieces)

    def tokens_ready(i):
        for k in range(tp_count - 1):
            tok_move(i, k, source_of(k)).wait_recv()

    def multiply(i):
        owner = owner_at(order[i])
        for part in range(2):
            w = wts[part, owner]

            def body(s, carry):
                x = tok[s, :, tok_columns(i)]
                y = jnp.dot(x, w, preferred_element_type=F32)
                if i > 0:
                    y = acc[part, s] + y
                acc[part, s] = y
                return carry

            lax.fori_loop(0, seqs, body, 0)

    def close(i, source):
        owner = owner_at(order[i])
        where = pl.ds(pl.multiple_of(source * pos, pos), pos)
        for part in range(2):
            for s in range(seqs):
                y = jnp.dot(
                    tok[s, where, tok_columns(i)], wts[part, owner], preferred_element_type=F32
                )
                kv[part, s, where, :] = (acc[part, s, where, :] + y).astype(BF16)

    def steps_of_hop(hop):
        if hop == 0:
            return [0]
        first = 1 + 2 * (hop - 1)
        return [first, first + 1] if hop < hops else [first]

    def compute_hop(hop):
        if hop > 0:
            pair_ready(hop, key_pieces)
        if chunked:
            for i in steps_of_hop(hop):
                if i < len(order) - 1:
                    tokens_ready(i)
                    multiply(i)
                else:
                    close(i, tp)
                    tokens_ready(i)
                    for p in tp_peers:
                        close(i, p)

    def mix_move(k, source):
        return pltpu.make_async_remote_copy(
            src_ref=packed.at[source], dst_ref=packed.at[source],
            send_sem=mix_send.at[k - 1], recv_sem=mix_recv.at[k - 1],
            device_id={"sp": lax.rem(me + k, n)}, device_id_type=MESH,
        )

    def mix():
        for k in range(tp_count - 1):
            for which in range(2):
                read_move(k, which, source_of(k), tp).wait_recv()
        count = seqs * rows_h
        given = jnp.concatenate([pin[t] for t in range(tp_count)] + [plow[tp]], axis=0)
        product = jnp.dot(
            given, wts[1].reshape(width, cols), preferred_element_type=F32
        )
        carry = jnp.zeros((count, 1), F32)
        mixture = jnp.zeros((count, cols), F32)
        for t in range(tp_count - 1, -1, -1):
            term = product[t * count : (t + 1) * count]
            term = term + jnp.where(tp == t, 1.0, 0.0) * product[tp_count * count :]
            mixture = mixture + jnp.exp(carry) * term
            carry = carry + tot_in[t][:, :1]
        own = lax.broadcasted_iota(jnp.int32, (rows_h, cols), 0) == (
            lax.broadcasted_iota(jnp.int32, (rows_h, cols), 1) // head_dim
        )
        for s in range(seqs):
            at = slice(s * rows_h, (s + 1) * rows_h)
            packed[me, s : s + 1] = jnp.sum(
                jnp.where(own, mixture[at], 0.0), axis=0, keepdims=True
            )
            packed[me, seqs + s : seqs + s + 1] = jnp.sum(
                jnp.where(own, carry[at], 0.0), axis=0, keepdims=True
            )
        for k in range(1, n):
            launch(mix_move(k, me))

    for hop in range(1, hops + 1):
        pass_on(hop, key_pieces)
        if hop == min(MIX_HOP, hops):
            mix()
        compute_hop(hop - 1)
    compute_hop(hops)

    if not chunked:
        tokens_ready(0)
        tile = pos
        for part in range(2):
            w = wts[part].reshape(width, cols)

            def body(j, carry):
                s, r = j // (span // tile), lax.rem(j, span // tile)
                where = pl.ds(pl.multiple_of(r * tile, tile), tile)
                y = jnp.dot(tok[s, where, :], w, preferred_element_type=F32)
                kv[part, s, where, :] = y.astype(BF16)
                return carry

            lax.fori_loop(0, seqs * (span // tile), body, 0)

    for k in range(tp_count - 1):
        bias_move(k, source_of(k), tp).wait_recv()
    bias[tp] = bias_all[:, tp]
    for s in range(seqs):
        bias_out[s] = jnp.concatenate([bias[t, s] for t in range(tp_count)], axis=1)
    for k in range(1, n):
        mix_move(k, lax.rem(me + n - k, n)).wait_recv()
    for c in sent_list:
        c.wait_send()


def finish(n, head_dim, kv, bias, packed, key_out, value_out, bias_out, reading_out, sems):
    moves = [
        pltpu.make_async_copy(kv.at[0], key_out, sems.at[0]),
        pltpu.make_async_copy(kv.at[1], value_out, sems.at[1]),
        pltpu.make_async_copy(bias, bias_out, sems.at[2]),
    ]
    for c in moves:
        c.start()
    seqs, cols = reading_out.shape
    rows_h = max(8, cols // head_dim)
    row_id = lax.broadcasted_iota(jnp.int32, (rows_h, cols), 0)
    col_id = lax.broadcasted_iota(jnp.int32, (rows_h, cols), 1)
    own = row_id == col_id // head_dim
    mixture = jnp.zeros((seqs, cols), F32)
    carry = jnp.zeros((seqs, cols), F32)
    for at in range(n - 1, -1, -1):
        mixture = mixture + jnp.exp(carry) * packed[at, :seqs]
        carry = carry + packed[at, seqs:]
    for s in range(seqs):
        x = mixture[s : s + 1]
        mean = jnp.sum(jnp.where(own, x * x, 0.0), axis=1, keepdims=True) / head_dim
        scale = jnp.sum(jnp.where(own, lax.rsqrt(mean + 1e-06), 0.0), axis=0, keepdims=True)
        reading_out[s : s + 1] = x * scale
    for c in moves:
        c.wait()


def per_device(tokens, key_weight, value_weight, queries, head_offset, key_bias):
    n, tp_count = lax.axis_size("sp"), lax.axis_size("tp")
    assert n % 2 == 0 and lax.axis_size("gr") == 2
    seqs, pos, width = tokens.shape
    rows, kv_width = key_weight.shape
    head_count = head_offset.shape[0]
    head_dim = kv_width // head_count
    cols = kv_width // tp_count
    heads = head_count // tp_count
    rows_h = max(8, heads)
    span = tp_count * pos
    hops = n // 2
    bias_rows = jnp.transpose(key_bias, (0, 2, 1)).reshape(seqs, tp_count, heads, pos)
    group = tp_count * rows_h
    own_bias = jnp.pad(bias_rows, ((0, 0), (0, 0), (0, rows_h - heads), (0, 0)))
    own_bias = own_bias.reshape(seqs, group, pos)
    dims = (n, tp_count, seqs, pos, width, rows, cols, heads, head_dim, rows_h)
    peers = max(tp_count - 1, 1)
    chunks = n if (width // n) % 128 == 0 else 1
    dma = pltpu.SemaphoreType.DMA
    kv, bias_held, packed = pl.pallas_call(
        functools.partial(kernel, dims),
        out_shape=(
            jax.ShapeDtypeStruct((2, seqs, span, cols), BF16),
            jax.ShapeDtypeStruct((seqs, heads, span), BF16),
            jax.ShapeDtypeStruct((n, 2 * seqs, cols), F32),
        ),
        in_specs=[pl.BlockSpec(memory_space=pltpu.HBM)] * 7,
        out_specs=[pl.BlockSpec(memory_space=pltpu.VMEM)] * 3,
        scratch_shapes=[
            pltpu.VMEM((seqs, span, width), BF16),
            pltpu.VMEM((2, n, rows, cols), BF16),
            pltpu.VMEM((2, seqs, span, cols), F32),
            pltpu.VMEM((tp_count, seqs, heads, pos), BF16),
            pltpu.VMEM(queries.shape, BF16),
            pltpu.VMEM((1, head_count), F32),
            pltpu.VMEM((seqs, tp_count, heads, pos), BF16),
            pltpu.VMEM((seqs, group, pos), BF16),
            pltpu.VMEM((rows, kv_width), BF16),
            pltpu.VMEM((n, seqs * group, rows), BF16),
            pltpu.VMEM((seqs * group, width), BF16),
            pltpu.VMEM((tp_count, seqs * rows_h, width), BF16),
            pltpu.VMEM((tp_count, seqs * rows_h, width), BF16),
            pltpu.VMEM((tp_count, seqs * rows_h, width), BF16),
            pltpu.VMEM((tp_count, seqs * rows_h, 128), F32),
            pltpu.VMEM((tp_count, seqs * rows_h, 128), F32),
            dma((8,)),
            dma((2, hops, MARK + 1)),
            dma((2, hops, MARK + 1)),
            dma((2, hops, MARK + 1)),
            dma((2, hops, MARK + 1)),
            dma((chunks, peers)),
            dma((chunks, peers)),
            dma((peers,)),
            dma((peers,)),
            dma((2, peers)),
            dma((2, peers)),
            dma((n - 1,)),
            dma((n - 1,)),
        ],
        compiler_params=pltpu.CompilerParams(
            collective_id=0, has_side_effects=True, vmem_limit_bytes=36 * 2**20
        ),
        name="prefill",
    )(*(pltpu.with_memory_space_constraint(a, pltpu.HBM) for a in (tokens, key_weight, value_weight, queries, head_offset.reshape(1, head_count), bias_rows, own_bias)))
    key_cache, value_cache, bias_cache, reading = pl.pallas_call(
        functools.partial(finish, n, head_dim),
        out_shape=(
            jax.ShapeDtypeStruct((seqs, span, cols), BF16),
            jax.ShapeDtypeStruct((seqs, span, cols), BF16),
            jax.ShapeDtypeStruct((seqs, heads, span), BF16),
            jax.ShapeDtypeStruct((seqs, cols), F32),
        ),
        in_specs=[
            pl.BlockSpec(memory_space=pl.ANY),
            pl.BlockSpec(memory_space=pl.ANY),
            pl.BlockSpec(memory_space=pltpu.VMEM),
        ],
        out_specs=[
            pl.BlockSpec(memory_space=pl.ANY),
            pl.BlockSpec(memory_space=pl.ANY),
            pl.BlockSpec(memory_space=pl.ANY),
            pl.BlockSpec(memory_space=pltpu.VMEM),
        ],
        scratch_shapes=[dma((3,))],
        compiler_params=pltpu.CompilerParams(vmem_limit_bytes=4 * 2**20),
        name="finish",
    )(kv, bias_held, packed)
    return key_cache, value_cache, jnp.transpose(bias_cache, (0, 2, 1)), reading


def solution(mesh):
    in_specs = (
        P("gr", ("sp", "tp"), None),
        P("sp", None),
        P("sp", None),
        P("gr", None),
        P(),
        P("gr", ("sp", "tp"), None),
    )
    out_specs = (P("gr", "sp", "tp"), P("gr", "sp", "tp"), P("gr", "sp", "tp"), P("gr", "tp"))
    return jax.shard_map(
        per_device, mesh=mesh, in_specs=in_specs, out_specs=out_specs, check_vma=False
    )
```

```python
import functools

import jax
import jax.numpy as jnp
from jax import lax
from jax.experimental import pallas as pl
from jax.experimental.pallas import tpu as pltpu
from jax.sharding import PartitionSpec as P

MESH = pl.DeviceIdType.MESH
F32 = jnp.float32
BF16 = jnp.bfloat16
VALUE_SUBS = 4
KEY_SUBS = 4
MARK = VALUE_SUBS + KEY_SUBS
AHEAD = (4, 7, 10, 11)
FILL = (0, 0, 2, 4)
MIX_HOP = 2


def ring_place(index, length):
    lane, row = lax.rem(index, 2), index // 2
    return row * (1 - lane) + (length - 1 - row) * lane


def ring_index(place, length):
    lane = place // (length // 2)
    row = place * (1 - lane) + (length - 1 - place) * lane
    return 2 * row + lane


def kernel(
    dims,
    tokens, key_weight, value_weight, queries, head_offset, key_bias, own_bias,
    kv, bias_out, packed,
    tok, wts, acc, bias, query, offset, bias_all, bias_own, key_rows,
    ubuf, ucat, pout, pin, plow, tot_out, tot_in,
    local_sem, tok_load, sends, receives, ring_recv, last_recv, pair_recv, tok_recv,
):
    n, tp_count, seqs, pos, width, rows, cols, heads, head_dim, rows_h = dims
    hops = n // 2
    half_rows = rows // 2
    span = tp_count * pos
    kv_width = tp_count * cols
    me, tp, gr = lax.axis_index("sp"), lax.axis_index("tp"), lax.axis_index("gr")
    place = ring_place(me, n)

    def owner_at(step):
        return ring_index(lax.rem(place + step + n, n), n)

    right, left = owner_at(1), owner_at(-1)
    partner = 1 - gr
    col_start = pl.multiple_of(tp * cols, 128)
    chunked = (width // n) % 128 == 0
    order = [0]
    for h in range(1, hops + 1):
        order.extend([-h, h] if h < hops else [h])
    chunk = width // n if chunked else width
    chunk_count = n if chunked else 1

    def slot_of(step):
        if not chunked:
            return owner_at(step)
        return order.index(hops if abs(step) == hops else step)

    my_rows = pl.ds(pl.multiple_of(tp * pos, pos), pos)

    key_copy = pltpu.make_async_copy(key_weight, key_rows, local_sem.at[6])
    query_copy = pltpu.make_async_copy(queries, query, local_sem.at[4])
    weight_copies = [
        pltpu.make_async_copy(
            w.at[:, pl.ds(col_start, cols)], wts.at[part, slot_of(0)], local_sem.at[part]
        )
        for part, w in enumerate((key_weight, value_weight))
    ]

    def columns(i):
        return slice(i * chunk, (i + 1) * chunk)

    def columns_held(i):
        if not chunked:
            return slice(0, width)
        return pl.ds(pl.multiple_of(owner_at(order[i]) * chunk, 128), chunk)

    tok_copies = [
        pltpu.make_async_copy(
            tokens.at[:, :, columns_held(i)], tok.at[:, my_rows, columns(i)],
            tok_load.at[min(i, 1)],
        )
        for i in range(chunk_count)
    ]
    bias_copy = pltpu.make_async_copy(key_bias, bias_all, local_sem.at[3])
    own_bias_copy = pltpu.make_async_copy(own_bias, bias_own, local_sem.at[7])
    offset_copy = pltpu.make_async_copy(head_offset, offset, local_sem.at[5])
    for c in (
        weight_copies[1], tok_copies[0], query_copy, key_copy, *tok_copies[1:], weight_copies[0],
        bias_copy, own_bias_copy, offset_copy,
    ):
        c.start()

    tp_peers = [lax.rem(tp + k, tp_count) for k in range(1, tp_count)]
    barrier = pltpu.get_barrier_semaphore()
    for target in ({"sp": right}, {"sp": left}, {"gr": partner}, *({"tp": p} for p in tp_peers)):
        pl.semaphore_signal(barrier, inc=1, device_id=target, device_id_type=MESH)

    def part_of(piece):
        return 1 if piece < VALUE_SUBS else 0

    def rows_of(piece, core):
        part = part_of(piece)
        size = half_rows // (VALUE_SUBS if part == 1 else KEY_SUBS)
        sub = piece - (0 if part == 1 else VALUE_SUBS)
        return pl.ds(pl.multiple_of(core * half_rows + sub * size, size), size)

    def block_of(piece, step, core):
        if piece == MARK:
            return ubuf.at[slot_of(step)]
        return wts.at[part_of(piece), slot_of(step), rows_of(piece, core), :]

    def ring_copy(direction, hop, piece):
        return pltpu.make_async_remote_copy(
            src_ref=block_of(piece, step_of(direction, hop - 1), gr),
            dst_ref=block_of(piece, step_of(direction, hop), gr),
            send_sem=sends.at[1 if piece == MARK else 0],
            recv_sem=(last_recv.at[piece] if hop == hops else ring_recv.at[direction, hop - 1, piece]),
            device_id={"sp": right if direction == 0 else left}, device_id_type=MESH,
        )

    def step_of(direction, hop):
        return -hop if direction == 0 else hop

    def used(direction, hop, piece):
        return hop < hops or (hop == hops and piece % 2 == direction)

    def pair_copy(direction, hop, piece, core):
        block = block_of(piece, step_of(direction, hop), core)
        return pltpu.make_async_remote_copy(
            src_ref=block, dst_ref=block,
            send_sem=sends.at[2], recv_sem=pair_recv.at[part_of(piece), hop - 1],
            device_id={"gr": partner}, device_id_type=MESH,
        )

    def peer_of(k):
        return lax.rem(tp + k + 1, tp_count)

    def source_of(k):
        return lax.rem(tp + tp_count - k - 1, tp_count)

    def tok_move(i, s, k, source):
        place_rows = pl.ds(pl.multiple_of(source * pos, pos), pos)
        block = tok.at[s, place_rows, columns(i)]
        return pltpu.make_async_remote_copy(
            src_ref=block, dst_ref=block,
            send_sem=sends.at[3], recv_sem=tok_recv.at[(i + 1) // 2 if chunked else 0, s],
            device_id={"tp": peer_of(k)}, device_id_type=MESH,
        )

    def bias_move(k, source, target):
        return pltpu.make_async_remote_copy(
            src_ref=bias_all.at[:, target], dst_ref=bias.at[source],
            send_sem=sends.at[4], recv_sem=receives.at[0],
            device_id={"tp": peer_of(k)}, device_id_type=MESH,
        )

    def read_move(k, which, source, target):
        out, into = ((pout, pin), (tot_out, tot_in))[which]
        return pltpu.make_async_remote_copy(
            src_ref=out.at[target], dst_ref=into.at[source],
            send_sem=sends.at[5 + which], recv_sem=receives.at[1 + which],
            device_id={"tp": peer_of(k)}, device_id_type=MESH,
        )

    def launch(c):
        c.start()

    def counted(ref, sem):
        return pltpu.make_async_copy(ref, ref, sem)

    issued = [0]

    def load_tokens(i):
        if i == 0:
            tok_copies[0].wait()
        else:
            counted(tok.at[:, my_rows, chunk:], tok_load.at[1]).wait()

    def send_tokens(upto):
        while issued[0] < min(upto, chunk_count * seqs):
            i, s = divmod(issued[0], seqs)
            if s == 0 and i < 2:
                load_tokens(i)
            for k in range(tp_count - 1):
                launch(tok_move(i, s, k, tp))
            issued[0] += 1

    def open_ring(piece):
        for direction in range(2):
            if used(direction, 1, piece):
                launch(ring_copy(direction, 1, piece))

    def pass_on(hop, pieces):
        for piece in pieces:
            for direction in range(2):
                if not used(direction, hop, piece):
                    continue
                ring_copy(direction, hop, piece).wait_recv()
                if hop < hops and used(direction, hop + 1, piece):
                    launch(ring_copy(direction, hop + 1, piece))
                if piece != MARK:
                    launch(pair_copy(direction, hop, piece, gr))

    value_pieces = list(range(VALUE_SUBS))
    key_pieces = list(range(VALUE_SUBS, MARK))
    first_pass = value_pieces[:1] + [MARK] + value_pieces[1:]

    with jax.named_scope("barrier"):
        pl.semaphore_wait(barrier, 3 + len(tp_peers))
    with jax.named_scope("weights"):
        weight_copies[1].wait()
    open_ring(value_pieces[0])
    with jax.named_scope("tokens"):
        send_tokens(AHEAD[0])

    query_copy.wait()
    key_copy.wait()
    group = tp_count * rows_h
    row = lax.broadcasted_iota(jnp.int32, (group, kv_width), 0)
    col_head = lax.broadcasted_iota(jnp.int32, (group, kv_width), 1) // head_dim
    inner = lax.rem(row, rows_h)
    mine = (row // rows_h * heads + inner == col_head) & (inner < heads)
    q = query[...].astype(F32)
    q_rows = jnp.concatenate(
        [jnp.where(mine, q[s : s + 1], 0.0) for s in range(seqs)], axis=0
    ).astype(BF16)
    ubuf[slot_of(0)] = lax.dot_general(
        q_rows, key_rows[...], (((1,), (1,)), ((), ())), preferred_element_type=F32
    ).astype(BF16)
    for piece in value_pieces[1:]:
        open_ring(piece)
    open_ring(MARK)
    bias_copy.wait()
    for k in range(tp_count - 1):
        launch(bias_move(k, tp, peer_of(k)))
    weight_copies[0].wait()
    own_bias_copy.wait()
    offset_copy.wait()

    key_queue = [(0, piece) for piece in key_pieces]
    key_queue += [(hop, piece) for hop in range(1, hops + 1) for piece in key_pieces]

    def next_key():
        hop, piece = key_queue.pop(0)
        with jax.named_scope(f"key{hop}_{piece}"):
            if hop == 0:
                open_ring(piece)
            else:
                pass_on(hop, [piece])

    seen = set()

    def pair_ready(part, hop):
        if hop == 0 or ("pair", part, hop) in seen:
            return
        seen.add(("pair", part, hop))
        held = wts.at[part, slot_of(hop)]
        if hop == hops:
            held = held.at[pl.ds(0, half_rows), :]
        counted(held, pair_recv.at[part, hop - 1]).wait()

    def tokens_ready(hop, s):
        if ("tok", hop, s) in seen or tp_count == 1:
            return
        seen.add(("tok", hop, s))
        first, end = slots_of_hop(hop) if chunked else (0, 1)
        counted(
            tok.at[s, pl.ds(0, (tp_count - 1) * pos), slice(first * chunk, end * chunk)],
            tok_recv.at[hop, s],
        ).wait()

    def slots_of_hop(hop):
        if hop == 0:
            return 0, 1
        first = 1 + 2 * (hop - 1)
        return first, min(first + 2, n)

    def multiply(part, hop):
        if not chunked or ("done", part, hop) in seen:
            return
        seen.add(("done", part, hop))
        first, end = slots_of_hop(hop)
        with jax.named_scope(f"multiply{part}_{hop}"):
            pair_ready(part, hop)
            w = wts[part, first:end].reshape((end - first) * rows, cols)
            for s in range(seqs):
                tokens_ready(hop, s)
                y = jnp.dot(
                    tok[s, :, first * chunk : end * chunk], w, preferred_element_type=F32
                )
                if hop > 0:
                    y = acc[part, s] + y
                if hop < hops:
                    acc[part, s] = y
                else:
                    kv[part, s] = y.astype(BF16)

    for hop in range(1, hops):
        with jax.named_scope(f"value{hop}"):
            pass_on(hop, first_pass)
        send_tokens(AHEAD[min(hop, len(AHEAD) - 1)])
        for _ in range(FILL[min(hop, len(FILL) - 1)]):
            if key_queue[0][0] < hop:
                next_key()
        if hop == 2:
            multiply(1, 0)
            multiply(0, 0)
        if hop == 3:
            multiply(1, 1)
    while key_queue[0][0] == 0:
        next_key()
    with jax.named_scope("marks"):
        pass_on(hops, [MARK])

    for owner in range(n):
        ucat[:, owner * rows : (owner + 1) * rows] = ubuf[owner]
    total_heads = offset.shape[1]
    pick_row = lax.broadcasted_iota(jnp.int32, (group, total_heads), 0)
    pick_inner = lax.rem(pick_row, rows_h)
    pick = (
        lax.broadcasted_iota(jnp.int32, (group, total_heads), 1)
        == pick_row // rows_h * heads + pick_inner
    ) & (pick_inner < heads)
    offset_col = jnp.sum(jnp.where(pick, offset[...], 0.0), axis=1, keepdims=True)
    logits = []
    for s in range(seqs):
        logits.append(
            lax.dot_general(
                ucat[s * group : (s + 1) * group, :], tok[s, my_rows, :],
                (((1,), (1,)), ((), ())), preferred_element_type=F32,
            )
            * (head_dim**-0.5)
            + offset_col
            + bias_own[s].astype(F32)
        )
    logits = jnp.concatenate(logits, axis=0)
    soft = jnp.log1p(jnp.exp(-jnp.abs(logits)))
    fading = -jnp.maximum(logits, 0.0) - soft
    taking = jnp.minimum(logits, 0.0) - soft
    high = fading.astype(BF16)
    rest = fading - high.astype(F32)
    mid = rest.astype(BF16)
    low = (rest - mid.astype(F32)).astype(BF16)
    later = (
        lax.broadcasted_iota(jnp.int32, (pos, pos), 0)
        > lax.broadcasted_iota(jnp.int32, (pos, pos), 1)
    ).astype(F32).astype(BF16)
    sums = jnp.dot(
        jnp.concatenate([high, mid, low], axis=0), later, preferred_element_type=F32
    )
    m = seqs * group
    within = sums[:m] + sums[m : 2 * m] + sums[2 * m :]
    weights = jnp.exp(taking + within).astype(BF16)
    totals = jnp.sum(fading, axis=1, keepdims=True)
    spread = jnp.broadcast_to(totals, (m, 128))
    weighted = [
        jnp.dot(
            weights[s * group : (s + 1) * group], tok[s, my_rows, :],
            preferred_element_type=F32,
        )
        for s in range(seqs)
    ]
    for t in range(tp_count):
        at = slice(t * rows_h, (t + 1) * rows_h)
        tot_out[t] = jnp.concatenate(
            [spread[s * group + t * rows_h : s * group + (t + 1) * rows_h] for s in range(seqs)],
            axis=0,
        )
        whole = jnp.concatenate([weighted[s][at] for s in range(seqs)], axis=0)
        upper = whole.astype(BF16)
        pout[t] = upper
        plow[t] = (whole - upper.astype(F32)).astype(BF16)
    for k in range(tp_count - 1):
        for which in range(2):
            launch(read_move(k, which, tp, peer_of(k)))
    pin[tp] = pout[tp]
    tot_in[tp] = tot_out[tp]
    send_tokens(chunk_count * seqs)
    with jax.named_scope(f"value{hops}"):
        pass_on(hops, value_pieces)

    def mix_move(k, source):
        return pltpu.make_async_remote_copy(
            src_ref=packed.at[source], dst_ref=packed.at[source],
            send_sem=sends.at[7], recv_sem=receives.at[3],
            device_id={"sp": lax.rem(me + k, n)}, device_id_type=MESH,
        )

    def mix():
        with jax.named_scope("await_products"):
            if tp_count > 1:
                counted(pin.at[pl.ds(0, tp_count - 1)], receives.at[1]).wait()
                counted(tot_in.at[pl.ds(0, tp_count - 1)], receives.at[2]).wait()
            for hop in range(1, hops + 1):
                pair_ready(1, hop)
        count = seqs * rows_h
        given = jnp.concatenate([pin[t] for t in range(tp_count)] + [plow[tp]], axis=0)
        product = jnp.dot(
            given, wts[1].reshape(width, cols), preferred_element_type=F32
        )
        carry = jnp.zeros((count, 1), F32)
        mixture = jnp.zeros((count, cols), F32)
        for t in range(tp_count - 1, -1, -1):
            term = product[t * count : (t + 1) * count]
            term = term + jnp.where(tp == t, 1.0, 0.0) * product[tp_count * count :]
            mixture = mixture + jnp.exp(carry) * term
            carry = carry + tot_in[t][:, :1]
        own = lax.broadcasted_iota(jnp.int32, (rows_h, cols), 0) == (
            lax.broadcasted_iota(jnp.int32, (rows_h, cols), 1) // head_dim
        )
        for s in range(seqs):
            at = slice(s * rows_h, (s + 1) * rows_h)
            packed[me, s : s + 1] = jnp.sum(
                jnp.where(own, mixture[at], 0.0), axis=0, keepdims=True
            )
            packed[me, seqs + s : seqs + s + 1] = jnp.sum(
                jnp.where(own, carry[at], 0.0), axis=0, keepdims=True
            )
        for k in range(1, n):
            launch(mix_move(k, me))

    for hop in range(1, hops + 1):
        while key_queue and key_queue[0][0] <= hop:
            next_key()
        if hop == min(MIX_HOP, hops):
            mix()
        for step in range(min(hop + 1, hops)):
            multiply(1, step)
            multiply(0, step)
    multiply(1, hops)
    multiply(0, hops)

    if not chunked:
        for s in range(seqs):
            tokens_ready(0, s)
        for hop in range(1, hops + 1):
            pair_ready(0, hop)
        tile = pos
        for part in range(2):
            w = wts[part].reshape(width, cols)

            def body(j, carry):
                s, r = j // (span // tile), lax.rem(j, span // tile)
                where = pl.ds(pl.multiple_of(r * tile, tile), tile)
                y = jnp.dot(tok[s, where, :], w, preferred_element_type=F32)
                kv[part, s, where, :] = y.astype(BF16)
                return carry

            lax.fori_loop(0, seqs * (span // tile), body, 0)

    if tp_count > 1:
        counted(bias.at[pl.ds(0, tp_count - 1)], receives.at[0]).wait()
    bias[tp] = bias_all[:, tp]
    for s in range(seqs):
        bias_out[s] = jnp.concatenate([bias[t, s] for t in range(tp_count)], axis=1)
    with jax.named_scope("await_mix"):
        counted(packed.at[pl.ds(0, n - 1)], receives.at[3]).wait()
    with jax.named_scope("drain"):
        counted(wts.at[0, pl.ds(0, n - 1)], sends.at[0]).wait()
        counted(ubuf.at[pl.ds(0, n - 1)], sends.at[1]).wait()
        counted(wts.at[0, pl.ds(0, n - 1)], sends.at[2]).wait()
        if tp_count > 1:
            others = pl.ds(0, tp_count - 1)
            counted(tok.at[:, pl.ds(0, (tp_count - 1) * pos), :], sends.at[3]).wait()
            counted(bias.at[others], sends.at[4]).wait()
            counted(pin.at[others], sends.at[5]).wait()
            counted(tot_in.at[others], sends.at[6]).wait()
        counted(packed.at[pl.ds(0, n - 1)], sends.at[7]).wait()


def finish(n, head_dim, kv, bias, packed, key_out, value_out, bias_out, reading_out, sems):
    moves = [
        pltpu.make_async_copy(kv.at[0], key_out, sems.at[0]),
        pltpu.make_async_copy(kv.at[1], value_out, sems.at[1]),
        pltpu.make_async_copy(bias, bias_out, sems.at[2]),
    ]
    for c in moves:
        c.start()
    seqs, cols = reading_out.shape
    rows_h = max(8, cols // head_dim)
    row_id = lax.broadcasted_iota(jnp.int32, (rows_h, cols), 0)
    col_id = lax.broadcasted_iota(jnp.int32, (rows_h, cols), 1)
    own = row_id == col_id // head_dim
    mixture = jnp.zeros((seqs, cols), F32)
    carry = jnp.zeros((seqs, cols), F32)
    for at in range(n - 1, -1, -1):
        mixture = mixture + jnp.exp(carry) * packed[at, :seqs]
        carry = carry + packed[at, seqs:]
    for s in range(seqs):
        x = mixture[s : s + 1]
        mean = jnp.sum(jnp.where(own, x * x, 0.0), axis=1, keepdims=True) / head_dim
        scale = jnp.sum(jnp.where(own, lax.rsqrt(mean + 1e-06), 0.0), axis=0, keepdims=True)
        reading_out[s : s + 1] = x * scale
    for c in moves:
        c.wait()


def per_device(tokens, key_weight, value_weight, queries, head_offset, key_bias):
    n, tp_count = lax.axis_size("sp"), lax.axis_size("tp")
    assert n % 2 == 0 and lax.axis_size("gr") == 2
    seqs, pos, width = tokens.shape
    rows, kv_width = key_weight.shape
    head_count = head_offset.shape[0]
    head_dim = kv_width // head_count
    cols = kv_width // tp_count
    heads = head_count // tp_count
    rows_h = max(8, heads)
    span = tp_count * pos
    hops = n // 2
    bias_rows = jnp.transpose(key_bias, (0, 2, 1)).reshape(seqs, tp_count, heads, pos)
    group = tp_count * rows_h
    own_bias = jnp.pad(bias_rows, ((0, 0), (0, 0), (0, rows_h - heads), (0, 0)))
    own_bias = own_bias.reshape(seqs, group, pos)
    dims = (n, tp_count, seqs, pos, width, rows, cols, heads, head_dim, rows_h)
    groups = hops + 1 if (width // n) % 128 == 0 else 1
    dma = pltpu.SemaphoreType.DMA
    kv, bias_held, packed = pl.pallas_call(
        functools.partial(kernel, dims),
        out_shape=(
            jax.ShapeDtypeStruct((2, seqs, span, cols), BF16),
            jax.ShapeDtypeStruct((seqs, heads, span), BF16),
            jax.ShapeDtypeStruct((n, 2 * seqs, cols), F32),
        ),
        in_specs=[pl.BlockSpec(memory_space=pltpu.HBM)] * 7,
        out_specs=[pl.BlockSpec(memory_space=pltpu.VMEM)] * 3,
        scratch_shapes=[
            pltpu.VMEM((seqs, span, width), BF16),
            pltpu.VMEM((2, n, rows, cols), BF16),
            pltpu.VMEM((2, seqs, span, cols), F32),
            pltpu.VMEM((tp_count, seqs, heads, pos), BF16),
            pltpu.VMEM(queries.shape, BF16),
            pltpu.VMEM((1, head_count), F32),
            pltpu.VMEM((seqs, tp_count, heads, pos), BF16),
            pltpu.VMEM((seqs, group, pos), BF16),
            pltpu.VMEM((rows, kv_width), BF16),
            pltpu.VMEM((n, seqs * group, rows), BF16),
            pltpu.VMEM((seqs * group, width), BF16),
            pltpu.VMEM((tp_count, seqs * rows_h, width), BF16),
            pltpu.VMEM((tp_count, seqs * rows_h, width), BF16),
            pltpu.VMEM((tp_count, seqs * rows_h, width), BF16),
            pltpu.VMEM((tp_count, seqs * rows_h, 128), F32),
            pltpu.VMEM((tp_count, seqs * rows_h, 128), F32),
            dma((8,)),
            dma((2,)),
            dma((8,)),
            dma((4,)),
            dma((2, hops - 1, MARK + 1)),
            dma((MARK + 1,)),
            dma((2, hops)),
            dma((groups, seqs)),
        ],
        compiler_params=pltpu.CompilerParams(
            collective_id=0, has_side_effects=True, vmem_limit_bytes=36 * 2**20
        ),
        name="prefill",
    )(*(pltpu.with_memory_space_constraint(a, pltpu.HBM) for a in (tokens, key_weight, value_weight, queries, head_offset.reshape(1, head_count), bias_rows, own_bias)))
    key_cache, value_cache, bias_cache, reading = pl.pallas_call(
        functools.partial(finish, n, head_dim),
        out_shape=(
            jax.ShapeDtypeStruct((seqs, span, cols), BF16),
            jax.ShapeDtypeStruct((seqs, span, cols), BF16),
            jax.ShapeDtypeStruct((seqs, heads, span), BF16),
            jax.ShapeDtypeStruct((seqs, cols), F32),
        ),
        in_specs=[
            pl.BlockSpec(memory_space=pl.ANY),
            pl.BlockSpec(memory_space=pl.ANY),
            pl.BlockSpec(memory_space=pltpu.VMEM),
        ],
        out_specs=[
            pl.BlockSpec(memory_space=pl.ANY),
            pl.BlockSpec(memory_space=pl.ANY),
            pl.BlockSpec(memory_space=pl.ANY),
            pl.BlockSpec(memory_space=pltpu.VMEM),
        ],
        scratch_shapes=[dma((3,))],
        compiler_params=pltpu.CompilerParams(vmem_limit_bytes=4 * 2**20),
        name="finish",
    )(kv, bias_held, packed)
    return key_cache, value_cache, jnp.transpose(bias_cache, (0, 2, 1)), reading


def solution(mesh):
    in_specs = (
        P("gr", ("sp", "tp"), None),
        P("sp", None),
        P("sp", None),
        P("gr", None),
        P(),
        P("gr", ("sp", "tp"), None),
    )
    out_specs = (P("gr", "sp", "tp"), P("gr", "sp", "tp"), P("gr", "sp", "tp"), P("gr", "tp"))
    return jax.shard_map(
        per_device, mesh=mesh, in_specs=in_specs, out_specs=out_specs, check_vma=False
    )
```

```python
import functools

import jax
import jax.numpy as jnp
from jax import lax
from jax.experimental import pallas as pl
from jax.experimental.pallas import tpu as pltpu
from jax.sharding import PartitionSpec as P

MESH = pl.DeviceIdType.MESH
F32 = jnp.float32
BF16 = jnp.bfloat16
VALUE_SUBS = 2
KEY_SUBS = 2
MARK = VALUE_SUBS + KEY_SUBS
OPEN, PASS, TOKENS, MULTIPLY, PROJECT, READ, MIX = range(7)


def plan(hops, seqs):
    if hops == 4 and seqs == 2:
        return TUNED
    value, key = range(VALUE_SUBS), range(VALUE_SUBS, MARK)
    first = [0, MARK, *value[1:]]
    steps = [(OPEN, 0), (TOKENS, 4), (PROJECT,), *((OPEN, p) for p in first[1:])]
    for hop in range(1, hops):
        steps += [(PASS, hop, p) for p in first] + [(TOKENS, 4 + 2 * hop)]
    steps += [(OPEN, p) for p in key]
    steps += [(PASS, hops, p) for p in first] + [(READ,), (TOKENS, 4 * hops * seqs)]
    for hop in range(1, hops + 1):
        steps += [(PASS, hop, p) for p in key]
        if hop == min(2, hops):
            steps.append((MIX,))
        for h in range(hop + 1) if hop == 1 else [hop]:
            steps += [(MULTIPLY, part, h, s) for part in (1, 0) for s in range(seqs)]
    return steps


TUNED = (
    (OPEN, 0), (TOKENS, 10), (PROJECT,), (OPEN, MARK), (OPEN, 1), (PASS, 1, 0), (PASS, 1, MARK),
    (OPEN, 2), (PASS, 1, 1), (MULTIPLY, 0, 0, 0), (MULTIPLY, 1, 0, 1), (PASS, 2, MARK), (OPEN, 3),
    (PASS, 2, 0), (PASS, 3, MARK), (MULTIPLY, 1, 0, 0), (MULTIPLY, 0, 0, 1), (PASS, 2, 1),
    (PASS, 1, 2), (PASS, 1, 3), (MULTIPLY, 1, 1, 0), (PASS, 4, MARK), (READ,), (TOKENS, 15),
    (PASS, 3, 0), (MULTIPLY, 0, 1, 1), (TOKENS, 16), (PASS, 3, 1), (MULTIPLY, 1, 2, 1),
    (MULTIPLY, 0, 1, 0), (PASS, 2, 2), (MULTIPLY, 1, 1, 1), (PASS, 2, 3), (PASS, 4, 1),
    (PASS, 4, 0), (MIX,), (PASS, 3, 2), (PASS, 3, 3), (MULTIPLY, 0, 2, 0), (MULTIPLY, 1, 3, 0),
    (MULTIPLY, 0, 3, 0), (MULTIPLY, 1, 2, 0), (MULTIPLY, 1, 3, 1), (MULTIPLY, 1, 4, 0),
    (MULTIPLY, 0, 2, 1), (MULTIPLY, 0, 3, 1), (PASS, 4, 3), (PASS, 4, 2), (MULTIPLY, 1, 4, 1),
    (MULTIPLY, 0, 4, 0), (MULTIPLY, 0, 4, 1),
)


def ring_place(index, length):
    lane, row = lax.rem(index, 2), index // 2
    return row * (1 - lane) + (length - 1 - row) * lane


def ring_index(place, length):
    lane = place // (length // 2)
    row = place * (1 - lane) + (length - 1 - place) * lane
    return 2 * row + lane


def kernel(
    dims,
    tokens, key_weight, value_weight, queries, head_offset, key_bias, own_bias,
    kv, bias_out, packed,
    tok, wts, acc, bias, query, offset, bias_all, bias_own, key_rows,
    ubuf, ucat, pout, pin, plow, tot_out, tot_in,
    local_sem, tok_load, sends, receives, ring_recv, last_recv, pair_recv, tok_recv,
):
    n, tp_count, seqs, pos, width, rows, cols, heads, head_dim, rows_h = dims
    hops = n // 2
    half_rows = rows // 2
    span = tp_count * pos
    kv_width = tp_count * cols
    group = tp_count * rows_h
    me, tp, gr = lax.axis_index("sp"), lax.axis_index("tp"), lax.axis_index("gr")
    place = ring_place(me, n)

    def owner_at(step):
        return ring_index(lax.rem(place + step + n, n), n)

    right, left = owner_at(1), owner_at(-1)
    partner = 1 - gr
    col_start = pl.multiple_of(tp * cols, 128)
    chunked = (width // n) % 128 == 0
    order = [0]
    for h in range(1, hops + 1):
        order.extend([-h, h] if h < hops else [h])
    chunk = width // n if chunked else width
    chunk_count = n if chunked else 1

    def slot_of(step):
        if not chunked:
            return owner_at(step)
        return order.index(hops if abs(step) == hops else step)

    my_rows = pl.ds(pl.multiple_of(tp * pos, pos), pos)

    key_copy = pltpu.make_async_copy(key_weight, key_rows, local_sem.at[6])
    query_copy = pltpu.make_async_copy(queries, query, local_sem.at[4])
    weight_copies = [
        pltpu.make_async_copy(
            w.at[:, pl.ds(col_start, cols)], wts.at[part, slot_of(0)], local_sem.at[part]
        )
        for part, w in enumerate((key_weight, value_weight))
    ]

    def columns(i):
        return slice(i * chunk, (i + 1) * chunk)

    def columns_held(i):
        if not chunked:
            return slice(0, width)
        return pl.ds(pl.multiple_of(owner_at(order[i]) * chunk, 128), chunk)

    tok_copies = [
        pltpu.make_async_copy(
            tokens.at[:, :, columns_held(i)], tok.at[:, my_rows, columns(i)],
            tok_load.at[min(i, 1)],
        )
        for i in range(chunk_count)
    ]
    bias_copy = pltpu.make_async_copy(key_bias, bias_all, local_sem.at[3])
    own_bias_copy = pltpu.make_async_copy(own_bias, bias_own, local_sem.at[7])
    offset_copy = pltpu.make_async_copy(head_offset, offset, local_sem.at[5])
    for c in (
        weight_copies[1], tok_copies[0], query_copy, key_copy, *tok_copies[1:], weight_copies[0],
        bias_copy, own_bias_copy, offset_copy,
    ):
        c.start()

    tp_peers = [lax.rem(tp + k, tp_count) for k in range(1, tp_count)]
    barrier = pltpu.get_barrier_semaphore()
    for target in ({"sp": right}, {"sp": left}, {"gr": partner}, *({"tp": p} for p in tp_peers)):
        pl.semaphore_signal(barrier, inc=1, device_id=target, device_id_type=MESH)

    def part_of(piece):
        return 1 if piece < VALUE_SUBS else 0

    def rows_of(piece, core):
        part = part_of(piece)
        size = half_rows // (VALUE_SUBS if part == 1 else KEY_SUBS)
        sub = piece - (0 if part == 1 else VALUE_SUBS)
        return pl.ds(pl.multiple_of(core * half_rows + sub * size, size), size)

    def block_of(piece, step, core):
        if piece == MARK:
            return ubuf.at[slot_of(step)]
        return wts.at[part_of(piece), slot_of(step), rows_of(piece, core), :]

    def ring_copy(direction, hop, piece):
        return pltpu.make_async_remote_copy(
            src_ref=block_of(piece, step_of(direction, hop - 1), gr),
            dst_ref=block_of(piece, step_of(direction, hop), gr),
            send_sem=sends.at[1 if piece == MARK else 0],
            recv_sem=(last_recv.at[piece] if hop == hops else ring_recv.at[direction, hop - 1, piece]),
            device_id={"sp": right if direction == 0 else left}, device_id_type=MESH,
        )

    def step_of(direction, hop):
        return -hop if direction == 0 else hop

    def used(direction, hop, piece):
        return hop < hops or (hop == hops and piece % 2 == direction)

    def pair_copy(direction, hop, piece, core):
        block = block_of(piece, step_of(direction, hop), core)
        return pltpu.make_async_remote_copy(
            src_ref=block, dst_ref=block,
            send_sem=sends.at[2], recv_sem=pair_recv.at[part_of(piece), hop - 1],
            device_id={"gr": partner}, device_id_type=MESH,
        )

    def peer_of(k):
        return lax.rem(tp + k + 1, tp_count)

    def source_of(k):
        return lax.rem(tp + tp_count - k - 1, tp_count)

    def tok_move(i, s, k, source):
        place_rows = pl.ds(pl.multiple_of(source * pos, pos), pos)
        block = tok.at[s, place_rows, columns(i)]
        return pltpu.make_async_remote_copy(
            src_ref=block, dst_ref=block,
            send_sem=sends.at[3], recv_sem=tok_recv.at[(i + 1) // 2 if chunked else 0, s],
            device_id={"tp": peer_of(k)}, device_id_type=MESH,
        )

    def bias_move(k, source, target):
        return pltpu.make_async_remote_copy(
            src_ref=bias_all.at[:, target], dst_ref=bias.at[source],
            send_sem=sends.at[4], recv_sem=receives.at[0],
            device_id={"tp": peer_of(k)}, device_id_type=MESH,
        )

    def read_move(k, which, source, target):
        out, into = ((pout, pin), (tot_out, tot_in))[which]
        return pltpu.make_async_remote_copy(
            src_ref=out.at[target], dst_ref=into.at[source],
            send_sem=sends.at[5 + which], recv_sem=receives.at[1 + which],
            device_id={"tp": peer_of(k)}, device_id_type=MESH,
        )

    def launch(c):
        c.start()

    def counted(ref, sem):
        return pltpu.make_async_copy(ref, ref, sem)

    issued = [0]

    def load_tokens(i):
        if i == 0:
            tok_copies[0].wait()
        else:
            counted(tok.at[:, my_rows, chunk:], tok_load.at[1]).wait()

    def send_tokens(upto):
        while issued[0] < min(upto, chunk_count * seqs):
            i, s = divmod(issued[0], seqs)
            if s == 0 and i < 2:
                load_tokens(i)
            for k in range(tp_count - 1):
                launch(tok_move(i, s, k, tp))
            issued[0] += 1

    def open_ring(piece):
        for direction in range(2):
            if used(direction, 1, piece):
                launch(ring_copy(direction, 1, piece))

    def pass_on(hop, piece):
        for direction in range(2):
            if not used(direction, hop, piece):
                continue
            ring_copy(direction, hop, piece).wait_recv()
            if hop < hops and used(direction, hop + 1, piece):
                launch(ring_copy(direction, hop + 1, piece))
            if piece != MARK:
                launch(pair_copy(direction, hop, piece, gr))

    def project():
        query_copy.wait()
        key_copy.wait()
        row = lax.broadcasted_iota(jnp.int32, (group, kv_width), 0)
        col_head = lax.broadcasted_iota(jnp.int32, (group, kv_width), 1) // head_dim
        inner = lax.rem(row, rows_h)
        mine = (row // rows_h * heads + inner == col_head) & (inner < heads)
        q = query[...].astype(F32)
        q_rows = jnp.concatenate(
            [jnp.where(mine, q[s : s + 1], 0.0) for s in range(seqs)], axis=0
        ).astype(BF16)
        ubuf[slot_of(0)] = lax.dot_general(
            q_rows, key_rows[...], (((1,), (1,)), ((), ())), preferred_element_type=F32
        ).astype(BF16)
        bias_copy.wait()
        for k in range(tp_count - 1):
            launch(bias_move(k, tp, peer_of(k)))

    def read():
        own_bias_copy.wait()
        offset_copy.wait()
        for owner in range(n):
            ucat[:, owner * rows : (owner + 1) * rows] = ubuf[owner]
        total_heads = offset.shape[1]
        pick_row = lax.broadcasted_iota(jnp.int32, (group, total_heads), 0)
        pick_inner = lax.rem(pick_row, rows_h)
        pick = (
            lax.broadcasted_iota(jnp.int32, (group, total_heads), 1)
            == pick_row // rows_h * heads + pick_inner
        ) & (pick_inner < heads)
        offset_col = jnp.sum(jnp.where(pick, offset[...], 0.0), axis=1, keepdims=True)
        logits = []
        for s in range(seqs):
            logits.append(
                lax.dot_general(
                    ucat[s * group : (s + 1) * group, :], tok[s, my_rows, :],
                    (((1,), (1,)), ((), ())), preferred_element_type=F32,
                )
                * (head_dim**-0.5)
                + offset_col
                + bias_own[s].astype(F32)
            )
        logits = jnp.concatenate(logits, axis=0)
        soft = jnp.log1p(jnp.exp(-jnp.abs(logits)))
        fading = -jnp.maximum(logits, 0.0) - soft
        taking = jnp.minimum(logits, 0.0) - soft
        high = fading.astype(BF16)
        rest = fading - high.astype(F32)
        mid = rest.astype(BF16)
        low = (rest - mid.astype(F32)).astype(BF16)
        later = (
            lax.broadcasted_iota(jnp.int32, (pos, pos), 0)
            > lax.broadcasted_iota(jnp.int32, (pos, pos), 1)
        ).astype(F32).astype(BF16)
        sums = jnp.dot(
            jnp.concatenate([high, mid, low], axis=0), later, preferred_element_type=F32
        )
        m = seqs * group
        within = sums[:m] + sums[m : 2 * m] + sums[2 * m :]
        weights = jnp.exp(taking + within).astype(BF16)
        totals = jnp.sum(fading, axis=1, keepdims=True)
        spread = jnp.broadcast_to(totals, (m, 128))
        weighted = [
            jnp.dot(
                weights[s * group : (s + 1) * group], tok[s, my_rows, :],
                preferred_element_type=F32,
            )
            for s in range(seqs)
        ]
        for t in range(tp_count):
            at = slice(t * rows_h, (t + 1) * rows_h)
            tot_out[t] = jnp.concatenate(
                [spread[s * group + t * rows_h : s * group + (t + 1) * rows_h] for s in range(seqs)],
                axis=0,
            )
            whole = jnp.concatenate([weighted[s][at] for s in range(seqs)], axis=0)
            upper = whole.astype(BF16)
            pout[t] = upper
            plow[t] = (whole - upper.astype(F32)).astype(BF16)
        for k in range(tp_count - 1):
            for which in range(2):
                launch(read_move(k, which, tp, peer_of(k)))
        pin[tp] = pout[tp]
        tot_in[tp] = tot_out[tp]

    seen = set()

    def weights_here(part):
        if ("weights", part) not in seen:
            seen.add(("weights", part))
            weight_copies[part].wait()

    def pair_ready(part, hop):
        if hop == 0 or ("pair", part, hop) in seen:
            return
        seen.add(("pair", part, hop))
        held = wts.at[part, slot_of(hop)]
        if hop == hops:
            held = held.at[pl.ds(0, half_rows), :]
        counted(held, pair_recv.at[part, hop - 1]).wait()

    def tokens_ready(hop, s):
        if ("tok", hop, s) in seen or tp_count == 1:
            return
        seen.add(("tok", hop, s))
        first, end = slots_of_hop(hop) if chunked else (0, 1)
        counted(
            tok.at[s, pl.ds(0, (tp_count - 1) * pos), slice(first * chunk, end * chunk)],
            tok_recv.at[hop, s],
        ).wait()

    def slots_of_hop(hop):
        if hop == 0:
            return 0, 1
        first = 1 + 2 * (hop - 1)
        return first, min(first + 2, n)

    def multiply(part, hop, s):
        if not chunked:
            return
        first, end = slots_of_hop(hop)
        with jax.named_scope(f"multiply{part}_{hop}_{s}"):
            if hop == 0:
                weights_here(part)
            pair_ready(part, hop)
            tokens_ready(hop, s)
            y = jnp.dot(
                tok[s, :, first * chunk : end * chunk],
                wts[part, first:end].reshape((end - first) * rows, cols),
                preferred_element_type=F32,
            )
            if hop > 0:
                y = acc[part, s] + y
            if hop < hops:
                acc[part, s] = y
            else:
                kv[part, s] = y.astype(BF16)

    def mix_move(k, source):
        return pltpu.make_async_remote_copy(
            src_ref=packed.at[source], dst_ref=packed.at[source],
            send_sem=sends.at[7], recv_sem=receives.at[3],
            device_id={"sp": lax.rem(me + k, n)}, device_id_type=MESH,
        )

    def mix():
        with jax.named_scope("await_products"):
            if tp_count > 1:
                counted(pin.at[pl.ds(0, tp_count - 1)], receives.at[1]).wait()
                counted(tot_in.at[pl.ds(0, tp_count - 1)], receives.at[2]).wait()
            for hop in range(1, hops + 1):
                pair_ready(1, hop)
        count = seqs * rows_h
        given = jnp.concatenate([pin[t] for t in range(tp_count)] + [plow[tp]], axis=0)
        product = jnp.dot(
            given, wts[1].reshape(width, cols), preferred_element_type=F32
        )
        carry = jnp.zeros((count, 1), F32)
        mixture = jnp.zeros((count, cols), F32)
        for t in range(tp_count - 1, -1, -1):
            term = product[t * count : (t + 1) * count]
            term = term + jnp.where(tp == t, 1.0, 0.0) * product[tp_count * count :]
            mixture = mixture + jnp.exp(carry) * term
            carry = carry + tot_in[t][:, :1]
        own = lax.broadcasted_iota(jnp.int32, (rows_h, cols), 0) == (
            lax.broadcasted_iota(jnp.int32, (rows_h, cols), 1) // head_dim
        )
        for s in range(seqs):
            at = slice(s * rows_h, (s + 1) * rows_h)
            packed[me, s : s + 1] = jnp.sum(
                jnp.where(own, mixture[at], 0.0), axis=0, keepdims=True
            )
            packed[me, seqs + s : seqs + s + 1] = jnp.sum(
                jnp.where(own, carry[at], 0.0), axis=0, keepdims=True
            )
        for k in range(1, n):
            launch(mix_move(k, me))

    with jax.named_scope("barrier"):
        pl.semaphore_wait(barrier, 3 + len(tp_peers))
    for kind, *what in plan(hops, seqs):
        if kind == OPEN:
            if what[0] != MARK:
                weights_here(part_of(what[0]))
            open_ring(what[0])
        elif kind == PASS:
            with jax.named_scope(f"pass{what[0]}_{what[1]}"):
                pass_on(*what)
        elif kind == TOKENS:
            send_tokens(what[0])
        elif kind == MULTIPLY:
            multiply(*what)
        elif kind == PROJECT:
            with jax.named_scope("project"):
                project()
        elif kind == READ:
            with jax.named_scope("read"):
                read()
        elif kind == MIX:
            with jax.named_scope("mix"):
                mix()

    if not chunked:
        for s in range(seqs):
            tokens_ready(0, s)
        for hop in range(1, hops + 1):
            pair_ready(0, hop)
        tile = pos
        for part in range(2):
            w = wts[part].reshape(width, cols)

            def body(j, carry):
                s, r = j // (span // tile), lax.rem(j, span // tile)
                where = pl.ds(pl.multiple_of(r * tile, tile), tile)
                y = jnp.dot(tok[s, where, :], w, preferred_element_type=F32)
                kv[part, s, where, :] = y.astype(BF16)
                return carry

            lax.fori_loop(0, seqs * (span // tile), body, 0)

    if tp_count > 1:
        counted(bias.at[pl.ds(0, tp_count - 1)], receives.at[0]).wait()
    bias[tp] = bias_all[:, tp]
    for s in range(seqs):
        bias_out[s] = jnp.concatenate([bias[t, s] for t in range(tp_count)], axis=1)
    with jax.named_scope("await_mix"):
        counted(packed.at[pl.ds(0, n - 1)], receives.at[3]).wait()
    with jax.named_scope("drain"):
        counted(wts.at[0, pl.ds(0, n - 1)], sends.at[0]).wait()
        counted(ubuf.at[pl.ds(0, n - 1)], sends.at[1]).wait()
        counted(wts.at[0, pl.ds(0, n - 1)], sends.at[2]).wait()
        if tp_count > 1:
            others = pl.ds(0, tp_count - 1)
            counted(tok.at[:, pl.ds(0, (tp_count - 1) * pos), :], sends.at[3]).wait()
            counted(bias.at[others], sends.at[4]).wait()
            counted(pin.at[others], sends.at[5]).wait()
            counted(tot_in.at[others], sends.at[6]).wait()
        counted(packed.at[pl.ds(0, n - 1)], sends.at[7]).wait()


def finish(n, head_dim, kv, bias, packed, key_out, value_out, bias_out, reading_out, sems):
    moves = [
        pltpu.make_async_copy(kv.at[0], key_out, sems.at[0]),
        pltpu.make_async_copy(kv.at[1], value_out, sems.at[1]),
        pltpu.make_async_copy(bias, bias_out, sems.at[2]),
    ]
    for c in moves:
        c.start()
    seqs, cols = reading_out.shape
    rows_h = max(8, cols // head_dim)
    row_id = lax.broadcasted_iota(jnp.int32, (rows_h, cols), 0)
    col_id = lax.broadcasted_iota(jnp.int32, (rows_h, cols), 1)
    own = row_id == col_id // head_dim
    mixture = jnp.zeros((seqs, cols), F32)
    carry = jnp.zeros((seqs, cols), F32)
    for at in range(n - 1, -1, -1):
        mixture = mixture + jnp.exp(carry) * packed[at, :seqs]
        carry = carry + packed[at, seqs:]
    for s in range(seqs):
        x = mixture[s : s + 1]
        mean = jnp.sum(jnp.where(own, x * x, 0.0), axis=1, keepdims=True) / head_dim
        scale = jnp.sum(jnp.where(own, lax.rsqrt(mean + 1e-06), 0.0), axis=0, keepdims=True)
        reading_out[s : s + 1] = x * scale
    for c in moves:
        c.wait()


def per_device(tokens, key_weight, value_weight, queries, head_offset, key_bias):
    n, tp_count = lax.axis_size("sp"), lax.axis_size("tp")
    assert n % 2 == 0 and lax.axis_size("gr") == 2
    seqs, pos, width = tokens.shape
    rows, kv_width = key_weight.shape
    head_count = head_offset.shape[0]
    head_dim = kv_width // head_count
    cols = kv_width // tp_count
    heads = head_count // tp_count
    rows_h = max(8, heads)
    span = tp_count * pos
    hops = n // 2
    bias_rows = jnp.transpose(key_bias, (0, 2, 1)).reshape(seqs, tp_count, heads, pos)
    group = tp_count * rows_h
    own_bias = jnp.pad(bias_rows, ((0, 0), (0, 0), (0, rows_h - heads), (0, 0)))
    own_bias = own_bias.reshape(seqs, group, pos)
    dims = (n, tp_count, seqs, pos, width, rows, cols, heads, head_dim, rows_h)
    groups = hops + 1 if (width // n) % 128 == 0 else 1
    dma = pltpu.SemaphoreType.DMA
    kv, bias_held, packed = pl.pallas_call(
        functools.partial(kernel, dims),
        out_shape=(
            jax.ShapeDtypeStruct((2, seqs, span, cols), BF16),
            jax.ShapeDtypeStruct((seqs, heads, span), BF16),
            jax.ShapeDtypeStruct((n, 2 * seqs, cols), F32),
        ),
        in_specs=[pl.BlockSpec(memory_space=pltpu.HBM)] * 7,
        out_specs=[pl.BlockSpec(memory_space=pltpu.VMEM)] * 3,
        scratch_shapes=[
            pltpu.VMEM((seqs, span, width), BF16),
            pltpu.VMEM((2, n, rows, cols), BF16),
            pltpu.VMEM((2, seqs, span, cols), F32),
            pltpu.VMEM((tp_count, seqs, heads, pos), BF16),
            pltpu.VMEM(queries.shape, BF16),
            pltpu.VMEM((1, head_count), F32),
            pltpu.VMEM((seqs, tp_count, heads, pos), BF16),
            pltpu.VMEM((seqs, group, pos), BF16),
            pltpu.VMEM((rows, kv_width), BF16),
            pltpu.VMEM((n, seqs * group, rows), BF16),
            pltpu.VMEM((seqs * group, width), BF16),
            pltpu.VMEM((tp_count, seqs * rows_h, width), BF16),
            pltpu.VMEM((tp_count, seqs * rows_h, width), BF16),
            pltpu.VMEM((tp_count, seqs * rows_h, width), BF16),
            pltpu.VMEM((tp_count, seqs * rows_h, 128), F32),
            pltpu.VMEM((tp_count, seqs * rows_h, 128), F32),
            dma((8,)),
            dma((2,)),
            dma((8,)),
            dma((4,)),
            dma((2, hops - 1, MARK + 1)),
            dma((MARK + 1,)),
            dma((2, hops)),
            dma((groups, seqs)),
        ],
        compiler_params=pltpu.CompilerParams(
            collective_id=0, has_side_effects=True, vmem_limit_bytes=36 * 2**20
        ),
        name="prefill",
    )(*(pltpu.with_memory_space_constraint(a, pltpu.HBM) for a in (tokens, key_weight, value_weight, queries, head_offset.reshape(1, head_count), bias_rows, own_bias)))
    key_cache, value_cache, bias_cache, reading = pl.pallas_call(
        functools.partial(finish, n, head_dim),
        out_shape=(
            jax.ShapeDtypeStruct((seqs, span, cols), BF16),
            jax.ShapeDtypeStruct((seqs, span, cols), BF16),
            jax.ShapeDtypeStruct((seqs, heads, span), BF16),
            jax.ShapeDtypeStruct((seqs, cols), F32),
        ),
        in_specs=[
            pl.BlockSpec(memory_space=pl.ANY),
            pl.BlockSpec(memory_space=pl.ANY),
            pl.BlockSpec(memory_space=pltpu.VMEM),
        ],
        out_specs=[
            pl.BlockSpec(memory_space=pl.ANY),
            pl.BlockSpec(memory_space=pl.ANY),
            pl.BlockSpec(memory_space=pl.ANY),
            pl.BlockSpec(memory_space=pltpu.VMEM),
        ],
        scratch_shapes=[dma((3,))],
        compiler_params=pltpu.CompilerParams(vmem_limit_bytes=4 * 2**20),
        name="finish",
    )(kv, bias_held, packed)
    return key_cache, value_cache, jnp.transpose(bias_cache, (0, 2, 1)), reading


def solution(mesh):
    in_specs = (
        P("gr", ("sp", "tp"), None),
        P("sp", None),
        P("sp", None),
        P("gr", None),
        P(),
        P("gr", ("sp", "tp"), None),
    )
    out_specs = (P("gr", "sp", "tp"), P("gr", "sp", "tp"), P("gr", "sp", "tp"), P("gr", "tp"))
    return jax.shard_map(
        per_device, mesh=mesh, in_specs=in_specs, out_specs=out_specs, check_vma=False
    )
```

```python
import functools

import jax
import jax.numpy as jnp
from jax import lax
from jax.experimental import pallas as pl
from jax.experimental.pallas import tpu as pltpu
from jax.sharding import PartitionSpec as P

MESH = pl.DeviceIdType.MESH
F32 = jnp.float32
BF16 = jnp.bfloat16
VALUE_SUBS = 2
KEY_SUBS = 4
MARK = VALUE_SUBS + KEY_SUBS
EARLY_HOPS = 2
OPEN, PASS, TOKENS, MULTIPLY, PROJECT, READ, MIX = range(7)


def plan(hops, seqs):
    if hops == 4 and seqs == 2:
        return TUNED
    value, key = range(VALUE_SUBS), range(VALUE_SUBS, MARK)
    first = [0, MARK, *value[1:]]
    steps = [(OPEN, 0), (TOKENS, 4), (PROJECT,), *((OPEN, p) for p in first[1:])]
    for hop in range(1, hops):
        steps += [(PASS, hop, p) for p in first] + [(TOKENS, 4 + 2 * hop)]
    steps += [(OPEN, p) for p in key]
    steps += [(PASS, hops, p) for p in first] + [(READ,), (TOKENS, 4 * hops * seqs)]
    for hop in range(1, hops + 1):
        steps += [(PASS, hop, p) for p in key]
        if hop == min(2, hops):
            steps.append((MIX,))
        for h in range(hop + 1) if hop == 1 else [hop]:
            steps += [(MULTIPLY, part, h, s) for part in (1, 0) for s in range(seqs)]
    return steps


TUNED = (
    (OPEN, 0), (TOKENS, 6), (PROJECT,), (OPEN, MARK), (OPEN, 1), (OPEN, 4), (OPEN, 5),
    (PASS, 1, MARK), (MULTIPLY, 0, 0, 0), (TOKENS, 10), (PASS, 1, 0), (PASS, 1, 1), (PASS, 2, MARK),
    (OPEN, 2), (OPEN, 3), (PASS, 2, 0), (PASS, 3, MARK), (PASS, 2, 1), (PASS, 1, 4), (PASS, 1, 5),
    (PASS, 1, 2), (PASS, 1, 3), (PASS, 4, MARK), (READ,), (PASS, 3, 1), (TOKENS, 13), (TOKENS, 14),
    (PASS, 3, 0), (MULTIPLY, 1, 0, 1), (MULTIPLY, 1, 0, 0), (MULTIPLY, 1, 1, 0), (PASS, 2, 4),
    (PASS, 2, 5), (MULTIPLY, 0, 1, 0), (MULTIPLY, 1, 2, 0), (PASS, 2, 2), (PASS, 2, 3),
    (MULTIPLY, 1, 2, 1), (PASS, 4, 1), (MULTIPLY, 0, 0, 1), (PASS, 4, 0), (MIX,), (TOKENS, 16),
    (PASS, 3, 4), (PASS, 3, 5), (PASS, 3, 2), (PASS, 3, 3), (MULTIPLY, 0, 2, 1),
    (MULTIPLY, 1, 3, 0), (MULTIPLY, 1, 1, 1), (MULTIPLY, 0, 1, 1), (MULTIPLY, 0, 3, 0),
    (MULTIPLY, 0, 2, 0), (MULTIPLY, 1, 3, 1), (MULTIPLY, 0, 3, 1), (PASS, 4, 4), (PASS, 4, 5),
    (PASS, 4, 2), (PASS, 4, 3), (MULTIPLY, 1, 4, 1), (MULTIPLY, 1, 4, 0), (MULTIPLY, 0, 4, 1),
    (MULTIPLY, 0, 4, 0),
)


def ring_place(index, length):
    lane, row = lax.rem(index, 2), index // 2
    return row * (1 - lane) + (length - 1 - row) * lane


def ring_index(place, length):
    lane = place // (length // 2)
    row = place * (1 - lane) + (length - 1 - place) * lane
    return 2 * row + lane


def kernel(
    dims,
    tokens, key_weight, value_weight, queries, head_offset, key_bias, own_bias,
    kv, bias_out, packed, tok, wts, acc,
    bias, query, offset, bias_all, bias_own, key_rows,
    ubuf, ucat, pout, pin, plow, tot_out, tot_in, wout, win,
    local_sem, tok_load, sends, receives, ring_recv, last_recv, pair_recv, tok_recv, ready,
):
    n, tp_count, seqs, pos, width, rows, cols, heads, head_dim, rows_h = dims
    hops = n // 2
    half_rows = rows // 2
    span = tp_count * pos
    kv_width = tp_count * cols
    group = tp_count * rows_h
    me, tp, gr = lax.axis_index("sp"), lax.axis_index("tp"), lax.axis_index("gr")
    place = ring_place(me, n)

    def owner_at(step):
        return ring_index(lax.rem(place + step + n, n), n)

    right, left = owner_at(1), owner_at(-1)
    partner = 1 - gr
    col_start = pl.multiple_of(tp * cols, 128)
    chunked = (width // n) % 128 == 0
    order = [0]
    for h in range(1, hops + 1):
        order.extend([-h, h] if h < hops else [h])
    chunk = width // n if chunked else width
    chunk_count = n if chunked else 1
    early = min(EARLY_HOPS, hops - 1) if chunked else -1
    cut = (2 * early + 1) * chunk if chunked else 0
    tail = slice(cut, width)
    crossing = 3 if chunked else 2

    def slot_of(step):
        if not chunked:
            return owner_at(step)
        return order.index(hops if abs(step) == hops else step)

    my_rows = pl.ds(pl.multiple_of(tp * pos, pos), pos)

    key_copy = pltpu.make_async_copy(key_weight, key_rows, local_sem.at[6])
    query_copy = pltpu.make_async_copy(queries, query, local_sem.at[4])
    weight_copies = [
        pltpu.make_async_copy(
            w.at[:, pl.ds(col_start, cols)], wts.at[part, slot_of(0)], local_sem.at[part]
        )
        for part, w in enumerate((key_weight, value_weight))
    ]

    def columns(i):
        return slice(i * chunk, (i + 1) * chunk)

    def columns_held(i):
        if not chunked:
            return slice(0, width)
        return pl.ds(pl.multiple_of(owner_at(order[i]) * chunk, 128), chunk)

    tok_copies = [
        pltpu.make_async_copy(
            tokens.at[:, :, columns_held(i)], tok.at[:, my_rows, columns(i)],
            tok_load.at[min(i, 1)],
        )
        for i in range(chunk_count)
    ]
    bias_copy = pltpu.make_async_copy(key_bias, bias_all, local_sem.at[3])
    own_bias_copy = pltpu.make_async_copy(own_bias, bias_own, local_sem.at[7])
    offset_copy = pltpu.make_async_copy(head_offset, offset, local_sem.at[5])
    for c in (
        weight_copies[1], tok_copies[0], query_copy, key_copy, *tok_copies[1:], weight_copies[0],
        bias_copy, own_bias_copy, offset_copy,
    ):
        c.start()

    tp_peers = [lax.rem(tp + k, tp_count) for k in range(1, tp_count)]
    barrier = pltpu.get_barrier_semaphore()
    ring = (right, left)

    def signal(semaphore, target):
        pl.semaphore_signal(semaphore, inc=1, device_id=target, device_id_type=MESH)

    for target in ring:
        pl.when(target > me)(functools.partial(signal, barrier, {"sp": target}))
    pl.when(gr == 0)(functools.partial(signal, barrier, {"gr": partner}))
    for peer in tp_peers:
        pl.when(peer > tp)(functools.partial(signal, barrier, {"tp": peer}))

    def part_of(piece):
        return 1 if piece < VALUE_SUBS else 0

    def rows_of(piece, core):
        part = part_of(piece)
        size = half_rows // (VALUE_SUBS if part == 1 else KEY_SUBS)
        sub = piece - (0 if part == 1 else VALUE_SUBS)
        return pl.ds(pl.multiple_of(core * half_rows + sub * size, size), size)

    def block_of(piece, step, core):
        if piece == MARK:
            return ubuf.at[slot_of(step)]
        return wts.at[part_of(piece), slot_of(step), rows_of(piece, core), :]

    def ring_copy(direction, hop, piece):
        return pltpu.make_async_remote_copy(
            src_ref=block_of(piece, step_of(direction, hop - 1), gr),
            dst_ref=block_of(piece, step_of(direction, hop), gr),
            send_sem=sends.at[1 if piece == MARK else 0],
            recv_sem=(last_recv.at[piece] if hop == hops else ring_recv.at[direction, hop - 1, piece]),
            device_id={"sp": right if direction == 0 else left}, device_id_type=MESH,
        )

    def step_of(direction, hop):
        return -hop if direction == 0 else hop

    def used(direction, hop, piece):
        return hop < hops or (hop == hops and piece % 2 == direction)

    def pair_copy(direction, hop, piece, core):
        block = block_of(piece, step_of(direction, hop), core)
        return pltpu.make_async_remote_copy(
            src_ref=block, dst_ref=block,
            send_sem=sends.at[2], recv_sem=pair_recv.at[part_of(piece), hop - 1],
            device_id={"gr": partner}, device_id_type=MESH,
        )

    def peer_of(k):
        return lax.rem(tp + k + 1, tp_count)

    def source_of(k):
        return lax.rem(tp + tp_count - k - 1, tp_count)

    def tok_move(i, s, k, source):
        place_rows = pl.ds(pl.multiple_of(source * pos, pos), pos)
        block = tok.at[s, place_rows, columns(i)]
        return pltpu.make_async_remote_copy(
            src_ref=block, dst_ref=block,
            send_sem=sends.at[3], recv_sem=tok_recv.at[(i + 1) // 2 if chunked else 0, s],
            device_id={"tp": peer_of(k)}, device_id_type=MESH,
        )

    def bias_move(k, source, target):
        return pltpu.make_async_remote_copy(
            src_ref=bias_all.at[:, target], dst_ref=bias.at[source],
            send_sem=sends.at[4], recv_sem=receives.at[0],
            device_id={"tp": peer_of(k)}, device_id_type=MESH,
        )

    def read_move(k, which, source, target):
        if which == 0:
            out, into = pout.at[target, :, tail], pin.at[source, :, tail]
        elif which == 1:
            out, into = tot_out.at[target], tot_in.at[source]
        else:
            out, into = wout.at[target], win.at[source]
        return pltpu.make_async_remote_copy(
            src_ref=out, dst_ref=into,
            send_sem=sends.at[5 + which], recv_sem=receives.at[1 + which],
            device_id={"tp": peer_of(k)}, device_id_type=MESH,
        )

    def launch(c):
        c.start()

    def counted(ref, sem):
        return pltpu.make_async_copy(ref, ref, sem)

    issued = [0]

    def load_tokens(i):
        if i == 0:
            tok_copies[0].wait()
        else:
            counted(tok.at[:, my_rows, chunk:], tok_load.at[1]).wait()

    def send_tokens(upto, ahead=None):
        upto = min(upto, chunk_count * seqs)
        for i, s in (divmod(unit, seqs) for unit in range(issued[0], upto)):
            if s == 0 and i < 2 and ahead is not True:
                load_tokens(i)
            for k in range(tp_count - 1):

                def start(i=i, s=s, k=k):
                    launch(tok_move(i, s, k, tp))

                if ahead is None:
                    start()
                else:
                    pl.when((peer_of(k) > tp) == ahead)(start)
        if ahead is not False:
            issued[0] = upto

    def open_ring(piece, ahead=None):
        for direction in range(2):
            if not used(direction, 1, piece):
                continue

            def start(direction=direction):
                launch(ring_copy(direction, 1, piece))

            if ahead is None:
                start()
            else:
                pl.when((ring[direction] > me) == ahead)(start)

    def pass_on(hop, piece):
        for direction in range(2):
            if not used(direction, hop, piece):
                continue
            ring_copy(direction, hop, piece).wait_recv()
            if hop < hops and used(direction, hop + 1, piece):
                launch(ring_copy(direction, hop + 1, piece))
            if piece != MARK:
                launch(pair_copy(direction, hop, piece, gr))

    def project():
        query_copy.wait()
        key_copy.wait()
        row = lax.broadcasted_iota(jnp.int32, (group, kv_width), 0)
        col_head = lax.broadcasted_iota(jnp.int32, (group, kv_width), 1) // head_dim
        inner = lax.rem(row, rows_h)
        mine = (row // rows_h * heads + inner == col_head) & (inner < heads)
        q = query[...].astype(F32)
        q_rows = jnp.concatenate(
            [jnp.where(mine, q[s : s + 1], 0.0) for s in range(seqs)], axis=0
        ).astype(BF16)
        ubuf[slot_of(0)] = lax.dot_general(
            q_rows, key_rows[...], (((1,), (1,)), ((), ())), preferred_element_type=F32
        ).astype(BF16)

    def greet():
        behind = (right < me).astype(jnp.int32) + (left < me).astype(jnp.int32) + gr + tp
        pl.when(behind > 0)(lambda: pl.semaphore_wait(barrier, behind))
        for direction in range(2):
            target = ring[direction]
            semaphore = ready.at[1 - direction]
            pl.when(target < me)(functools.partial(signal, semaphore, {"sp": target}))
        pl.when(gr == 1)(functools.partial(signal, ready.at[2], {"gr": partner}))
        for peer in tp_peers:
            pl.when(peer < tp)(functools.partial(signal, ready.at[3], {"tp": peer}))

    def begin(steps):
        with jax.named_scope("greet"):
            greet()
        for kind, *what in steps:
            if kind == OPEN:
                if what[0] != MARK:
                    weights_here(part_of(what[0]))
                open_ring(what[0], False)
            elif kind == TOKENS:
                send_tokens(what[0], False)
            elif kind == PROJECT:
                with jax.named_scope("project"):
                    project()
        with jax.named_scope("ready"):
            for direction in range(2):
                semaphore = ready.at[direction]
                pl.when(ring[direction] > me)(
                    functools.partial(pl.semaphore_wait, semaphore, 1)
                )
            ahead = tp_count - 1 - tp
            pl.when(ahead > 0)(lambda: pl.semaphore_wait(ready.at[3], ahead))
        for kind, *what in steps:
            if kind == OPEN:
                open_ring(what[0], True)
            elif kind == TOKENS:
                send_tokens(what[0], True)
        pl.when(gr == 0)(functools.partial(pl.semaphore_wait, ready.at[2], 1))
        bias_copy.wait()
        for k in range(tp_count - 1):
            launch(bias_move(k, tp, peer_of(k)))

    def read():
        own_bias_copy.wait()
        offset_copy.wait()
        for owner in range(n):
            ucat[:, owner * rows : (owner + 1) * rows] = ubuf[owner]
        total_heads = offset.shape[1]
        pick_row = lax.broadcasted_iota(jnp.int32, (group, total_heads), 0)
        pick_inner = lax.rem(pick_row, rows_h)
        pick = (
            lax.broadcasted_iota(jnp.int32, (group, total_heads), 1)
            == pick_row // rows_h * heads + pick_inner
        ) & (pick_inner < heads)
        offset_col = jnp.sum(jnp.where(pick, offset[...], 0.0), axis=1, keepdims=True)
        logits = []
        for s in range(seqs):
            logits.append(
                lax.dot_general(
                    ucat[s * group : (s + 1) * group, :], tok[s, my_rows, :],
                    (((1,), (1,)), ((), ())), preferred_element_type=F32,
                )
                * (head_dim**-0.5)
                + offset_col
                + bias_own[s].astype(F32)
            )
        logits = jnp.concatenate(logits, axis=0)
        soft = jnp.log1p(jnp.exp(-jnp.abs(logits)))
        fading = -jnp.maximum(logits, 0.0) - soft
        taking = jnp.minimum(logits, 0.0) - soft
        high = fading.astype(BF16)
        rest = fading - high.astype(F32)
        mid = rest.astype(BF16)
        low = (rest - mid.astype(F32)).astype(BF16)
        later = (
            lax.broadcasted_iota(jnp.int32, (pos, pos), 0)
            > lax.broadcasted_iota(jnp.int32, (pos, pos), 1)
        ).astype(F32).astype(BF16)
        sums = jnp.dot(
            jnp.concatenate([high, mid, low], axis=0), later, preferred_element_type=F32
        )
        m = seqs * group
        within = sums[:m] + sums[m : 2 * m] + sums[2 * m :]
        weights = jnp.exp(taking + within)
        totals = jnp.sum(fading, axis=1, keepdims=True)
        spread = jnp.broadcast_to(totals, (m, 128))
        weighted = [
            jnp.dot(
                weights[s * group : (s + 1) * group].astype(BF16), tok[s, my_rows, :],
                preferred_element_type=F32,
            )
            for s in range(seqs)
        ]
        for t in range(tp_count):
            at = slice(t * rows_h, (t + 1) * rows_h)
            wout[t] = jnp.concatenate(
                [weights[s * group : (s + 1) * group][at] for s in range(seqs)], axis=0
            ).astype(BF16)
            tot_out[t] = jnp.concatenate(
                [spread[s * group + t * rows_h : s * group + (t + 1) * rows_h] for s in range(seqs)],
                axis=0,
            )
            whole = jnp.concatenate([weighted[s][at] for s in range(seqs)], axis=0)
            upper = whole.astype(BF16)
            pout[t] = upper
            plow[t] = (whole - upper.astype(F32)).astype(BF16)
        for k in range(tp_count - 1):
            for which in range(crossing):
                launch(read_move(k, which, tp, peer_of(k)))
        pin[tp] = pout[tp]
        tot_in[tp] = tot_out[tp]

    seen = set()

    def weights_here(part):
        if ("weights", part) not in seen:
            seen.add(("weights", part))
            weight_copies[part].wait()

    def pair_ready(part, hop):
        if hop == 0 or ("pair", part, hop) in seen:
            return
        seen.add(("pair", part, hop))
        held = wts.at[part, slot_of(hop)]
        if hop == hops:
            held = held.at[pl.ds(0, half_rows), :]
        counted(held, pair_recv.at[part, hop - 1]).wait()

    def tokens_ready(hop, s):
        if ("tok", hop, s) in seen or tp_count == 1:
            return
        seen.add(("tok", hop, s))
        first, end = slots_of_hop(hop) if chunked else (0, 1)
        counted(
            tok.at[s, pl.ds(0, (tp_count - 1) * pos), slice(first * chunk, end * chunk)],
            tok_recv.at[hop, s],
        ).wait()

    def slots_of_hop(hop):
        if hop == 0:
            return 0, 1
        first = 1 + 2 * (hop - 1)
        return first, min(first + 2, n)

    def multiply(part, hop, s):
        if not chunked:
            return
        first, end = slots_of_hop(hop)
        with jax.named_scope(f"multiply{part}_{hop}_{s}"):
            if hop == 0:
                weights_here(part)
            pair_ready(part, hop)
            tokens_ready(hop, s)
            y = jnp.dot(
                tok[s, :, first * chunk : end * chunk],
                wts[part, first:end].reshape((end - first) * rows, cols),
                preferred_element_type=F32,
            )
            if hop > 0:
                y = acc[part, s] + y
            if hop < hops:
                acc[part, s] = y
            else:
                kv[part, s] = y.astype(BF16)

    def leave():
        if chunked:
            pair_ready(0, hops)
            for s in range(seqs):
                tokens_ready(hops, s)

    def mix_move(k, source):
        return pltpu.make_async_remote_copy(
            src_ref=packed.at[source], dst_ref=packed.at[source],
            send_sem=sends.at[8], recv_sem=receives.at[4],
            device_id={"sp": lax.rem(me + k, n)}, device_id_type=MESH,
        )

    def mix():
        with jax.named_scope("await_products"):
            if tp_count > 1:
                others = pl.ds(0, tp_count - 1)
                counted(pin.at[others, :, tail], receives.at[1]).wait()
                counted(tot_in.at[others], receives.at[2]).wait()
                if chunked:
                    counted(win.at[others], receives.at[3]).wait()
            for hop in range(1, hops + 1):
                pair_ready(1, hop)
        if chunked:
            for h in range(early + 1):
                for s in range(seqs):
                    tokens_ready(h, s)
            for k in range(tp_count - 1):
                source = source_of(k)
                where = pl.ds(pl.multiple_of(source * pos, pos), pos)
                held = win[source].astype(F32)
                pin[source, :, 0:cut] = jnp.concatenate(
                    [
                        jnp.dot(
                            held[s * rows_h : (s + 1) * rows_h].astype(BF16),
                            tok[s, where, 0:cut], preferred_element_type=F32,
                        )
                        for s in range(seqs)
                    ],
                    axis=0,
                ).astype(BF16)
        count = seqs * rows_h
        given = jnp.concatenate([pin[t] for t in range(tp_count)] + [plow[tp]], axis=0)
        product = jnp.dot(
            given, wts[1].reshape(width, cols), preferred_element_type=F32
        )
        carry = jnp.zeros((count, 1), F32)
        mixture = jnp.zeros((count, cols), F32)
        for t in range(tp_count - 1, -1, -1):
            term = product[t * count : (t + 1) * count]
            term = term + jnp.where(tp == t, 1.0, 0.0) * product[tp_count * count :]
            mixture = mixture + jnp.exp(carry) * term
            carry = carry + tot_in[t][:, :1]
        own = lax.broadcasted_iota(jnp.int32, (rows_h, cols), 0) == (
            lax.broadcasted_iota(jnp.int32, (rows_h, cols), 1) // head_dim
        )
        for s in range(seqs):
            at = slice(s * rows_h, (s + 1) * rows_h)
            packed[me, s : s + 1] = jnp.sum(
                jnp.where(own, mixture[at], 0.0), axis=0, keepdims=True
            )
            packed[me, seqs + s : seqs + s + 1] = jnp.sum(
                jnp.where(own, carry[at], 0.0), axis=0, keepdims=True
            )
        for k in range(1, n):
            launch(mix_move(k, me))

    steps = list(plan(hops, seqs))
    opening = next(i for i, step in enumerate(steps) if step[0] == PASS)
    begin(steps[:opening])
    for kind, *what in steps[opening:]:
        if kind == OPEN:
            if what[0] != MARK:
                weights_here(part_of(what[0]))
            open_ring(what[0])
        elif kind == PASS:
            with jax.named_scope(f"pass{what[0]}_{what[1]}"):
                pass_on(*what)
        elif kind == TOKENS:
            send_tokens(what[0])
        elif kind == MULTIPLY:
            if what[:2] != [0, hops]:
                multiply(*what)
        elif kind == READ:
            with jax.named_scope("read"):
                read()
        elif kind == MIX:
            with jax.named_scope("mix"):
                mix()

    leave()
    if not chunked:
        for s in range(seqs):
            tokens_ready(0, s)
        for hop in range(1, hops + 1):
            pair_ready(0, hop)
        tile = pos
        for part in range(2):
            w = wts[part].reshape(width, cols)

            def body(j, carry):
                s, r = j // (span // tile), lax.rem(j, span // tile)
                where = pl.ds(pl.multiple_of(r * tile, tile), tile)
                y = jnp.dot(tok[s, where, :], w, preferred_element_type=F32)
                kv[part, s, where, :] = y.astype(BF16)
                return carry

            lax.fori_loop(0, seqs * (span // tile), body, 0)

    if tp_count > 1:
        counted(bias.at[pl.ds(0, tp_count - 1)], receives.at[0]).wait()
    bias[tp] = bias_all[:, tp]
    for s in range(seqs):
        bias_out[s] = jnp.concatenate([bias[t, s] for t in range(tp_count)], axis=1)
    with jax.named_scope("await_mix"):
        counted(packed.at[pl.ds(0, n - 1)], receives.at[4]).wait()
    with jax.named_scope("drain"):
        counted(wts.at[0, pl.ds(0, n - 1)], sends.at[0]).wait()
        counted(ubuf.at[pl.ds(0, n - 1)], sends.at[1]).wait()
        counted(wts.at[0, pl.ds(0, n - 1)], sends.at[2]).wait()
        if tp_count > 1:
            others = pl.ds(0, tp_count - 1)
            counted(tok.at[:, pl.ds(0, (tp_count - 1) * pos), :], sends.at[3]).wait()
            counted(bias.at[others], sends.at[4]).wait()
            counted(pin.at[others, :, tail], sends.at[5]).wait()
            counted(tot_in.at[others], sends.at[6]).wait()
            if chunked:
                counted(win.at[others], sends.at[7]).wait()
        counted(packed.at[pl.ds(0, n - 1)], sends.at[8]).wait()


def finish(
    n, head_dim, kv, bias, packed, tok, wts, acc,
    key_out, value_out, bias_out, reading_out, key, sems,
):
    _, _, rows, _ = wts.shape
    chunked = rows % 128 == 0
    moves = [
        pltpu.make_async_copy(kv.at[1], value_out, sems.at[0]),
        pltpu.make_async_copy(bias, bias_out, sems.at[1]),
    ]
    if not chunked:
        moves.append(pltpu.make_async_copy(kv.at[0], key_out, sems.at[2]))
    for c in moves:
        c.start()
    if chunked:
        for s in range(key_out.shape[0]):
            y = jnp.dot(
                tok[s, :, (n - 1) * rows :], wts[0, n - 1], preferred_element_type=F32
            )
            key[s] = (acc[0, s] + y).astype(BF16)
            moves.append(pltpu.make_async_copy(key.at[s], key_out.at[s], sems.at[2 + s]))
            moves[-1].start()
    seqs, cols = reading_out.shape
    rows_h = max(8, cols // head_dim)
    row_id = lax.broadcasted_iota(jnp.int32, (rows_h, cols), 0)
    col_id = lax.broadcasted_iota(jnp.int32, (rows_h, cols), 1)
    own = row_id == col_id // head_dim
    mixture = jnp.zeros((seqs, cols), F32)
    carry = jnp.zeros((seqs, cols), F32)
    for at in range(n - 1, -1, -1):
        mixture = mixture + jnp.exp(carry) * packed[at, :seqs]
        carry = carry + packed[at, seqs:]
    for s in range(seqs):
        x = mixture[s : s + 1]
        mean = jnp.sum(jnp.where(own, x * x, 0.0), axis=1, keepdims=True) / head_dim
        scale = jnp.sum(jnp.where(own, lax.rsqrt(mean + 1e-06), 0.0), axis=0, keepdims=True)
        reading_out[s : s + 1] = x * scale
    for c in moves:
        c.wait()


def per_device(tokens, key_weight, value_weight, queries, head_offset, key_bias):
    n, tp_count = lax.axis_size("sp"), lax.axis_size("tp")
    assert n % 2 == 0 and lax.axis_size("gr") == 2
    seqs, pos, width = tokens.shape
    rows, kv_width = key_weight.shape
    head_count = head_offset.shape[0]
    head_dim = kv_width // head_count
    cols = kv_width // tp_count
    heads = head_count // tp_count
    rows_h = max(8, heads)
    span = tp_count * pos
    hops = n // 2
    bias_rows = jnp.transpose(key_bias, (0, 2, 1)).reshape(seqs, tp_count, heads, pos)
    group = tp_count * rows_h
    own_bias = jnp.pad(bias_rows, ((0, 0), (0, 0), (0, rows_h - heads), (0, 0)))
    own_bias = own_bias.reshape(seqs, group, pos)
    dims = (n, tp_count, seqs, pos, width, rows, cols, heads, head_dim, rows_h)
    groups = hops + 1 if (width // n) % 128 == 0 else 1
    dma = pltpu.SemaphoreType.DMA
    kv, bias_held, packed, tok, wts, acc = pl.pallas_call(
        functools.partial(kernel, dims),
        out_shape=(
            jax.ShapeDtypeStruct((2, seqs, span, cols), BF16),
            jax.ShapeDtypeStruct((seqs, heads, span), BF16),
            jax.ShapeDtypeStruct((n, 2 * seqs, cols), F32),
            jax.ShapeDtypeStruct((seqs, span, width), BF16),
            jax.ShapeDtypeStruct((2, n, rows, cols), BF16),
            jax.ShapeDtypeStruct((2, seqs, span, cols), F32),
        ),
        in_specs=[pl.BlockSpec(memory_space=pltpu.HBM)] * 7,
        out_specs=[pl.BlockSpec(memory_space=pltpu.VMEM)] * 6,
        scratch_shapes=[
            pltpu.VMEM((tp_count, seqs, heads, pos), BF16),
            pltpu.VMEM(queries.shape, BF16),
            pltpu.VMEM((1, head_count), F32),
            pltpu.VMEM((seqs, tp_count, heads, pos), BF16),
            pltpu.VMEM((seqs, group, pos), BF16),
            pltpu.VMEM((rows, kv_width), BF16),
            pltpu.VMEM((n, seqs * group, rows), BF16),
            pltpu.VMEM((seqs * group, width), BF16),
            pltpu.VMEM((tp_count, seqs * rows_h, width), BF16),
            pltpu.VMEM((tp_count, seqs * rows_h, width), BF16),
            pltpu.VMEM((tp_count, seqs * rows_h, width), BF16),
            pltpu.VMEM((tp_count, seqs * rows_h, 128), F32),
            pltpu.VMEM((tp_count, seqs * rows_h, 128), F32),
            pltpu.VMEM((tp_count, seqs * rows_h, pos), BF16),
            pltpu.VMEM((tp_count, seqs * rows_h, pos), BF16),
            dma((8,)),
            dma((2,)),
            dma((9,)),
            dma((5,)),
            dma((2, hops - 1, MARK + 1)),
            dma((MARK + 1,)),
            dma((2, hops)),
            dma((groups, seqs)),
            pltpu.SemaphoreType.REGULAR((4,)),
        ],
        compiler_params=pltpu.CompilerParams(
            collective_id=0, has_side_effects=True, vmem_limit_bytes=36 * 2**20
        ),
        name="prefill",
    )(*(pltpu.with_memory_space_constraint(a, pltpu.HBM) for a in (tokens, key_weight, value_weight, queries, head_offset.reshape(1, head_count), bias_rows, own_bias)))
    key_cache, value_cache, bias_cache, reading = pl.pallas_call(
        functools.partial(finish, n, head_dim),
        out_shape=(
            jax.ShapeDtypeStruct((seqs, span, cols), BF16),
            jax.ShapeDtypeStruct((seqs, span, cols), BF16),
            jax.ShapeDtypeStruct((seqs, heads, span), BF16),
            jax.ShapeDtypeStruct((seqs, cols), F32),
        ),
        in_specs=[
            pl.BlockSpec(memory_space=pl.ANY),
            pl.BlockSpec(memory_space=pl.ANY),
            *[pl.BlockSpec(memory_space=pltpu.VMEM)] * 4,
        ],
        out_specs=[
            pl.BlockSpec(memory_space=pl.ANY),
            pl.BlockSpec(memory_space=pl.ANY),
            pl.BlockSpec(memory_space=pl.ANY),
            pl.BlockSpec(memory_space=pltpu.VMEM),
        ],
        scratch_shapes=[pltpu.VMEM((seqs, span, cols), BF16), dma((2 + seqs,))],
        compiler_params=pltpu.CompilerParams(vmem_limit_bytes=16 * 2**20),
        name="finish",
    )(kv, bias_held, packed, tok, wts, acc)
    return key_cache, value_cache, jnp.transpose(bias_cache, (0, 2, 1)), reading


def solution(mesh):
    in_specs = (
        P("gr", ("sp", "tp"), None),
        P("sp", None),
        P("sp", None),
        P("gr", None),
        P(),
        P("gr", ("sp", "tp"), None),
    )
    out_specs = (P("gr", "sp", "tp"), P("gr", "sp", "tp"), P("gr", "sp", "tp"), P("gr", "tp"))
    return jax.shard_map(
        per_device, mesh=mesh, in_specs=in_specs, out_specs=out_specs, check_vma=False
    )
```

```python
import functools

import jax
import jax.numpy as jnp
from jax import lax
from jax.experimental import pallas as pl
from jax.experimental.pallas import tpu as pltpu
from jax.sharding import PartitionSpec as P

MESH = pl.DeviceIdType.MESH
F32 = jnp.float32
BF16 = jnp.bfloat16
VALUE_SUBS = 2
KEY_SUBS = 4
MARK = VALUE_SUBS + KEY_SUBS
EARLY_HOPS = 2
OPEN, PASS, TOKENS, MULTIPLY, PROJECT, READ, MIX = range(7)


def plan(hops, seqs):
    if hops == 4 and seqs == 2:
        return TUNED
    value, key = range(VALUE_SUBS), range(VALUE_SUBS, MARK)
    first = [0, MARK, *value[1:]]
    steps = [(OPEN, 0), (TOKENS, 4), (PROJECT,), *((OPEN, p) for p in first[1:])]
    for hop in range(1, hops):
        steps += [(PASS, hop, p) for p in first] + [(TOKENS, 4 + 2 * hop)]
    steps += [(OPEN, p) for p in key]
    steps += [(PASS, hops, p) for p in first] + [(READ,), (TOKENS, 4 * hops * seqs)]
    for hop in range(1, hops + 1):
        steps += [(PASS, hop, p) for p in key]
        if hop == min(2, hops):
            steps.append((MIX,))
        for h in range(hop + 1) if hop == 1 else [hop]:
            steps += [(MULTIPLY, part, h, s) for part in (1, 0) for s in range(seqs)]
    return steps


TUNED = (
    (OPEN, 0), (TOKENS, 10), (PROJECT,), (OPEN, MARK), (OPEN, 1), (OPEN, 4), (PASS, 1, MARK),
    (OPEN, 3), (PASS, 1, 0), (PASS, 1, 1), (PASS, 2, MARK), (OPEN, 2), (OPEN, 5), (PASS, 2, 0),
    (PASS, 3, MARK), (MULTIPLY, 0, 0, 0), (PASS, 2, 1), (PASS, 1, 2), (PASS, 1, 4), (PASS, 1, 5),
    (PASS, 4, MARK), (PASS, 1, 3), (MULTIPLY, 1, 0, 0), (READ,), (PASS, 3, 0), (MULTIPLY, 1, 1, 0),
    (PASS, 3, 1), (TOKENS, 13), (TOKENS, 14), (MULTIPLY, 0, 1, 0), (PASS, 2, 4), (PASS, 2, 2),
    (MULTIPLY, 1, 2, 0), (MULTIPLY, 0, 0, 1), (PASS, 2, 5), (MULTIPLY, 1, 0, 1), (TOKENS, 16),
    (MULTIPLY, 1, 2, 1), (PASS, 2, 3), (PASS, 4, 1), (PASS, 4, 0), (MIX,), (PASS, 3, 4),
    (MULTIPLY, 1, 1, 1), (PASS, 3, 5), (PASS, 3, 2), (PASS, 3, 3), (MULTIPLY, 0, 2, 0),
    (MULTIPLY, 1, 3, 0), (MULTIPLY, 0, 3, 0), (MULTIPLY, 0, 3, 1), (MULTIPLY, 0, 2, 1),
    (PASS, 4, 4), (MULTIPLY, 1, 3, 1), (PASS, 4, 2), (PASS, 4, 5), (PASS, 4, 3),
    (MULTIPLY, 0, 1, 1), (MULTIPLY, 1, 4, 0), (MULTIPLY, 1, 4, 1), (MULTIPLY, 0, 4, 0),
    (MULTIPLY, 0, 4, 1),
)


def ring_place(index, length):
    lane, row = lax.rem(index, 2), index // 2
    return row * (1 - lane) + (length - 1 - row) * lane


def ring_index(place, length):
    lane = place // (length // 2)
    row = place * (1 - lane) + (length - 1 - place) * lane
    return 2 * row + lane


def kernel(
    dims,
    tokens, key_weight, value_weight, queries, head_offset, key_bias, own_bias,
    kv, bias_out, packed, tok, wts, acc,
    bias, query, offset, bias_all, bias_own, key_rows,
    ubuf, ucat, pout, pin, plow, tot_out, tot_in, wout, win,
    local_sem, tok_load, sends, receives, ring_recv, last_recv, pair_recv, tok_recv, ready,
):
    n, tp_count, seqs, pos, width, rows, cols, heads, head_dim, rows_h = dims
    hops = n // 2
    half_rows = rows // 2
    span = tp_count * pos
    kv_width = tp_count * cols
    group = tp_count * rows_h
    me, tp, gr = lax.axis_index("sp"), lax.axis_index("tp"), lax.axis_index("gr")
    place = ring_place(me, n)

    def owner_at(step):
        return ring_index(lax.rem(place + step + n, n), n)

    right, left = owner_at(1), owner_at(-1)
    partner = 1 - gr
    col_start = pl.multiple_of(tp * cols, 128)
    chunked = (width // n) % 128 == 0
    order = [0]
    for h in range(1, hops + 1):
        order.extend([-h, h] if h < hops else [h])
    chunk = width // n if chunked else width
    chunk_count = n if chunked else 1
    early = min(EARLY_HOPS, hops - 1) if chunked else -1
    cut = (2 * early + 1) * chunk if chunked else 0
    tail = slice(cut, width)
    crossing = 3 if chunked else 2

    def slot_of(step):
        if not chunked:
            return owner_at(step)
        return order.index(hops if abs(step) == hops else step)

    my_rows = pl.ds(pl.multiple_of(tp * pos, pos), pos)

    key_copy = pltpu.make_async_copy(key_weight, key_rows, local_sem.at[6])
    query_copy = pltpu.make_async_copy(queries, query, local_sem.at[4])
    weight_copies = [
        pltpu.make_async_copy(
            w.at[:, pl.ds(col_start, cols)], wts.at[part, slot_of(0)], local_sem.at[part]
        )
        for part, w in enumerate((key_weight, value_weight))
    ]

    def columns(i):
        return slice(i * chunk, (i + 1) * chunk)

    def columns_held(i):
        if not chunked:
            return slice(0, width)
        return pl.ds(pl.multiple_of(owner_at(order[i]) * chunk, 128), chunk)

    tok_copies = [
        pltpu.make_async_copy(
            tokens.at[:, :, columns_held(i)], tok.at[:, my_rows, columns(i)],
            tok_load.at[min(i, 1)],
        )
        for i in range(chunk_count)
    ]
    bias_copy = pltpu.make_async_copy(key_bias, bias_all, local_sem.at[3])
    own_bias_copy = pltpu.make_async_copy(own_bias, bias_own, local_sem.at[7])
    offset_copy = pltpu.make_async_copy(head_offset, offset, local_sem.at[5])
    for c in (
        weight_copies[1], tok_copies[0], query_copy, key_copy, *tok_copies[1:], weight_copies[0],
        bias_copy, own_bias_copy, offset_copy,
    ):
        c.start()

    tp_peers = [lax.rem(tp + k, tp_count) for k in range(1, tp_count)]
    barrier = pltpu.get_barrier_semaphore()
    ring = (right, left)

    def signal(semaphore, target):
        pl.semaphore_signal(semaphore, inc=1, device_id=target, device_id_type=MESH)

    for target in ring:
        pl.when(target > me)(functools.partial(signal, barrier, {"sp": target}))
    pl.when(gr == 0)(functools.partial(signal, barrier, {"gr": partner}))
    for peer in tp_peers:
        pl.when(peer > tp)(functools.partial(signal, barrier, {"tp": peer}))

    def part_of(piece):
        return 1 if piece < VALUE_SUBS else 0

    def rows_of(piece, core):
        part = part_of(piece)
        size = half_rows // (VALUE_SUBS if part == 1 else KEY_SUBS)
        sub = piece - (0 if part == 1 else VALUE_SUBS)
        return pl.ds(pl.multiple_of(core * half_rows + sub * size, size), size)

    def block_of(piece, step, core):
        if piece == MARK:
            return ubuf.at[slot_of(step)]
        return wts.at[part_of(piece), slot_of(step), rows_of(piece, core), :]

    def ring_copy(direction, hop, piece):
        return pltpu.make_async_remote_copy(
            src_ref=block_of(piece, step_of(direction, hop - 1), gr),
            dst_ref=block_of(piece, step_of(direction, hop), gr),
            send_sem=sends.at[1 if piece == MARK else 0],
            recv_sem=(last_recv.at[piece] if hop == hops else ring_recv.at[direction, hop - 1, piece]),
            device_id={"sp": right if direction == 0 else left}, device_id_type=MESH,
        )

    def step_of(direction, hop):
        return -hop if direction == 0 else hop

    def used(direction, hop, piece):
        return hop < hops or (hop == hops and piece % 2 == direction)

    def pair_copy(direction, hop, piece, core):
        block = block_of(piece, step_of(direction, hop), core)
        return pltpu.make_async_remote_copy(
            src_ref=block, dst_ref=block,
            send_sem=sends.at[2], recv_sem=pair_recv.at[part_of(piece), hop - 1],
            device_id={"gr": partner}, device_id_type=MESH,
        )

    def peer_of(k):
        return lax.rem(tp + k + 1, tp_count)

    def source_of(k):
        return lax.rem(tp + tp_count - k - 1, tp_count)

    def tok_move(i, s, k, source):
        place_rows = pl.ds(pl.multiple_of(source * pos, pos), pos)
        block = tok.at[s, place_rows, columns(i)]
        return pltpu.make_async_remote_copy(
            src_ref=block, dst_ref=block,
            send_sem=sends.at[3], recv_sem=tok_recv.at[(i + 1) // 2 if chunked else 0, s],
            device_id={"tp": peer_of(k)}, device_id_type=MESH,
        )

    def bias_move(k, source, target):
        return pltpu.make_async_remote_copy(
            src_ref=bias_all.at[:, target], dst_ref=bias.at[source],
            send_sem=sends.at[4], recv_sem=receives.at[0],
            device_id={"tp": peer_of(k)}, device_id_type=MESH,
        )

    def read_move(k, which, source, target):
        if which == 0:
            out, into = pout.at[target, :, tail], pin.at[source, :, tail]
        elif which == 1:
            out, into = tot_out.at[target], tot_in.at[source]
        else:
            out, into = wout.at[target], win.at[source]
        return pltpu.make_async_remote_copy(
            src_ref=out, dst_ref=into,
            send_sem=sends.at[5 + which], recv_sem=receives.at[1 + which],
            device_id={"tp": peer_of(k)}, device_id_type=MESH,
        )

    def launch(c):
        c.start()

    def counted(ref, sem):
        return pltpu.make_async_copy(ref, ref, sem)

    issued = [0]

    def load_tokens(i):
        if i == 0:
            tok_copies[0].wait()
        else:
            counted(tok.at[:, my_rows, chunk:], tok_load.at[1]).wait()

    def send_tokens(upto, ahead=None):
        upto = min(upto, chunk_count * seqs)
        for i, s in (divmod(unit, seqs) for unit in range(issued[0], upto)):
            if s == 0 and i < 2 and ahead is not True:
                load_tokens(i)
            for k in range(tp_count - 1):

                def start(i=i, s=s, k=k):
                    launch(tok_move(i, s, k, tp))

                if ahead is None:
                    start()
                else:
                    pl.when((peer_of(k) > tp) == ahead)(start)
        if ahead is not False:
            issued[0] = upto

    def open_ring(piece, ahead=None):
        for direction in range(2):
            if not used(direction, 1, piece):
                continue

            def start(direction=direction):
                launch(ring_copy(direction, 1, piece))

            if ahead is None:
                start()
            else:
                pl.when((ring[direction] > me) == ahead)(start)

    def pass_on(hop, piece):
        for direction in range(2):
            if not used(direction, hop, piece):
                continue
            ring_copy(direction, hop, piece).wait_recv()
            if hop < hops and used(direction, hop + 1, piece):
                launch(ring_copy(direction, hop + 1, piece))
            if piece != MARK:
                launch(pair_copy(direction, hop, piece, gr))

    def project():
        query_copy.wait()
        key_copy.wait()
        row = lax.broadcasted_iota(jnp.int32, (group, kv_width), 0)
        col_head = lax.broadcasted_iota(jnp.int32, (group, kv_width), 1) // head_dim
        inner = lax.rem(row, rows_h)
        mine = (row // rows_h * heads + inner == col_head) & (inner < heads)
        q = query[...].astype(F32)
        q_rows = jnp.concatenate(
            [jnp.where(mine, q[s : s + 1], 0.0) for s in range(seqs)], axis=0
        ).astype(BF16)
        ubuf[slot_of(0)] = lax.dot_general(
            q_rows, key_rows[...], (((1,), (1,)), ((), ())), preferred_element_type=F32
        ).astype(BF16)

    def greet():
        behind = (right < me).astype(jnp.int32) + (left < me).astype(jnp.int32) + gr + tp
        pl.when(behind > 0)(lambda: pl.semaphore_wait(barrier, behind))
        for direction in range(2):
            target = ring[direction]
            semaphore = ready.at[1 - direction]
            pl.when(target < me)(functools.partial(signal, semaphore, {"sp": target}))
        pl.when(gr == 1)(functools.partial(signal, ready.at[2], {"gr": partner}))
        for peer in tp_peers:
            pl.when(peer < tp)(functools.partial(signal, ready.at[3], {"tp": peer}))

    def begin(steps):
        with jax.named_scope("greet"):
            greet()
        for kind, *what in steps:
            if kind == OPEN:
                if what[0] != MARK:
                    weights_here(part_of(what[0]))
                open_ring(what[0], False)
            elif kind == TOKENS:
                send_tokens(what[0], False)
            elif kind == PROJECT:
                with jax.named_scope("project"):
                    project()
        with jax.named_scope("ready"):
            for direction in range(2):
                semaphore = ready.at[direction]
                pl.when(ring[direction] > me)(
                    functools.partial(pl.semaphore_wait, semaphore, 1)
                )
            ahead = tp_count - 1 - tp
            pl.when(ahead > 0)(lambda: pl.semaphore_wait(ready.at[3], ahead))
        for kind, *what in steps:
            if kind == OPEN:
                open_ring(what[0], True)
            elif kind == TOKENS:
                send_tokens(what[0], True)
        pl.when(gr == 0)(functools.partial(pl.semaphore_wait, ready.at[2], 1))
        bias_copy.wait()
        for k in range(tp_count - 1):
            launch(bias_move(k, tp, peer_of(k)))

    def read():
        own_bias_copy.wait()
        offset_copy.wait()
        for owner in range(n):
            ucat[:, owner * rows : (owner + 1) * rows] = ubuf[owner]
        total_heads = offset.shape[1]
        pick_row = lax.broadcasted_iota(jnp.int32, (group, total_heads), 0)
        pick_inner = lax.rem(pick_row, rows_h)
        pick = (
            lax.broadcasted_iota(jnp.int32, (group, total_heads), 1)
            == pick_row // rows_h * heads + pick_inner
        ) & (pick_inner < heads)
        offset_col = jnp.sum(jnp.where(pick, offset[...], 0.0), axis=1, keepdims=True)
        logits = []
        for s in range(seqs):
            logits.append(
                lax.dot_general(
                    ucat[s * group : (s + 1) * group, :], tok[s, my_rows, :],
                    (((1,), (1,)), ((), ())), preferred_element_type=F32,
                )
                * (head_dim**-0.5)
                + offset_col
                + bias_own[s].astype(F32)
            )
        logits = jnp.concatenate(logits, axis=0)
        soft = jnp.log1p(jnp.exp(-jnp.abs(logits)))
        fading = -jnp.maximum(logits, 0.0) - soft
        taking = jnp.minimum(logits, 0.0) - soft
        high = fading.astype(BF16)
        rest = fading - high.astype(F32)
        mid = rest.astype(BF16)
        low = (rest - mid.astype(F32)).astype(BF16)
        later = (
            lax.broadcasted_iota(jnp.int32, (pos, pos), 0)
            > lax.broadcasted_iota(jnp.int32, (pos, pos), 1)
        ).astype(F32).astype(BF16)
        sums = jnp.dot(
            jnp.concatenate([high, mid, low], axis=0), later, preferred_element_type=F32
        )
        m = seqs * group
        within = sums[:m] + sums[m : 2 * m] + sums[2 * m :]
        weights = jnp.exp(taking + within)
        totals = jnp.sum(fading, axis=1, keepdims=True)
        spread = jnp.broadcast_to(totals, (m, 128))
        weighted = [
            jnp.dot(
                weights[s * group : (s + 1) * group].astype(BF16), tok[s, my_rows, :],
                preferred_element_type=F32,
            )
            for s in range(seqs)
        ]
        for t in range(tp_count):
            at = slice(t * rows_h, (t + 1) * rows_h)
            wout[t] = jnp.concatenate(
                [weights[s * group : (s + 1) * group][at] for s in range(seqs)], axis=0
            ).astype(BF16)
            tot_out[t] = jnp.concatenate(
                [spread[s * group + t * rows_h : s * group + (t + 1) * rows_h] for s in range(seqs)],
                axis=0,
            )
            whole = jnp.concatenate([weighted[s][at] for s in range(seqs)], axis=0)
            upper = whole.astype(BF16)
            pout[t] = upper
            plow[t] = (whole - upper.astype(F32)).astype(BF16)
        for k in range(tp_count - 1):
            for which in range(crossing):
                launch(read_move(k, which, tp, peer_of(k)))
        pin[tp] = pout[tp]
        tot_in[tp] = tot_out[tp]

    seen = set()

    def weights_here(part):
        if ("weights", part) not in seen:
            seen.add(("weights", part))
            weight_copies[part].wait()

    def pair_ready(part, hop):
        if hop == 0 or ("pair", part, hop) in seen:
            return
        seen.add(("pair", part, hop))
        held = wts.at[part, slot_of(hop)]
        if hop == hops:
            held = held.at[pl.ds(0, half_rows), :]
        counted(held, pair_recv.at[part, hop - 1]).wait()

    def tokens_ready(hop, s):
        if ("tok", hop, s) in seen or tp_count == 1:
            return
        seen.add(("tok", hop, s))
        first, end = slots_of_hop(hop) if chunked else (0, 1)
        counted(
            tok.at[s, pl.ds(0, (tp_count - 1) * pos), slice(first * chunk, end * chunk)],
            tok_recv.at[hop, s],
        ).wait()

    def slots_of_hop(hop):
        if hop == 0:
            return 0, 1
        first = 1 + 2 * (hop - 1)
        return first, min(first + 2, n)

    def multiply(part, hop, s):
        if not chunked:
            return
        first, end = slots_of_hop(hop)
        with jax.named_scope(f"multiply{part}_{hop}_{s}"):
            if hop == 0:
                weights_here(part)
            pair_ready(part, hop)
            tokens_ready(hop, s)
            y = jnp.dot(
                tok[s, :, first * chunk : end * chunk],
                wts[part, first:end].reshape((end - first) * rows, cols),
                preferred_element_type=F32,
            )
            if hop > 0:
                y = acc[part, s] + y
            if hop < hops:
                acc[part, s] = y
            else:
                kv[part, s] = y.astype(BF16)

    def leave():
        if chunked:
            pair_ready(0, hops)
            for s in range(seqs):
                tokens_ready(hops, s)

    def mix_move(k, source):
        return pltpu.make_async_remote_copy(
            src_ref=packed.at[source], dst_ref=packed.at[source],
            send_sem=sends.at[8], recv_sem=receives.at[4],
            device_id={"sp": lax.rem(me + k, n)}, device_id_type=MESH,
        )

    def mix():
        with jax.named_scope("await_products"):
            if tp_count > 1:
                others = pl.ds(0, tp_count - 1)
                counted(pin.at[others, :, tail], receives.at[1]).wait()
                counted(tot_in.at[others], receives.at[2]).wait()
                if chunked:
                    counted(win.at[others], receives.at[3]).wait()
            for hop in range(1, hops + 1):
                pair_ready(1, hop)
        if chunked:
            for h in range(early + 1):
                for s in range(seqs):
                    tokens_ready(h, s)
            for k in range(tp_count - 1):
                source = source_of(k)
                where = pl.ds(pl.multiple_of(source * pos, pos), pos)
                held = win[source].astype(F32)
                pin[source, :, 0:cut] = jnp.concatenate(
                    [
                        jnp.dot(
                            held[s * rows_h : (s + 1) * rows_h].astype(BF16),
                            tok[s, where, 0:cut], preferred_element_type=F32,
                        )
                        for s in range(seqs)
                    ],
                    axis=0,
                ).astype(BF16)
        count = seqs * rows_h
        given = jnp.concatenate([pin[t] for t in range(tp_count)] + [plow[tp]], axis=0)
        product = jnp.dot(
            given, wts[1].reshape(width, cols), preferred_element_type=F32
        )
        carry = jnp.zeros((count, 1), F32)
        mixture = jnp.zeros((count, cols), F32)
        for t in range(tp_count - 1, -1, -1):
            term = product[t * count : (t + 1) * count]
            term = term + jnp.where(tp == t, 1.0, 0.0) * product[tp_count * count :]
            mixture = mixture + jnp.exp(carry) * term
            carry = carry + tot_in[t][:, :1]
        own = lax.broadcasted_iota(jnp.int32, (rows_h, cols), 0) == (
            lax.broadcasted_iota(jnp.int32, (rows_h, cols), 1) // head_dim
        )
        for s in range(seqs):
            at = slice(s * rows_h, (s + 1) * rows_h)
            packed[me, s : s + 1] = jnp.sum(
                jnp.where(own, mixture[at], 0.0), axis=0, keepdims=True
            )
            packed[me, seqs + s : seqs + s + 1] = jnp.sum(
                jnp.where(own, carry[at], 0.0), axis=0, keepdims=True
            )
        for k in range(1, n):
            launch(mix_move(k, me))

    steps = list(plan(hops, seqs))
    opening = next(i for i, step in enumerate(steps) if step[0] == PASS)
    begin(steps[:opening])
    for kind, *what in steps[opening:]:
        if kind == OPEN:
            if what[0] != MARK:
                weights_here(part_of(what[0]))
            open_ring(what[0])
        elif kind == PASS:
            with jax.named_scope(f"pass{what[0]}_{what[1]}"):
                pass_on(*what)
        elif kind == TOKENS:
            send_tokens(what[0])
        elif kind == MULTIPLY:
            if what[:2] != [0, hops]:
                multiply(*what)
        elif kind == READ:
            with jax.named_scope("read"):
                read()
        elif kind == MIX:
            with jax.named_scope("mix"):
                mix()

    leave()
    if not chunked:
        for s in range(seqs):
            tokens_ready(0, s)
        for hop in range(1, hops + 1):
            pair_ready(0, hop)
        tile = pos
        for part in range(2):
            w = wts[part].reshape(width, cols)

            def body(j, carry):
                s, r = j // (span // tile), lax.rem(j, span // tile)
                where = pl.ds(pl.multiple_of(r * tile, tile), tile)
                y = jnp.dot(tok[s, where, :], w, preferred_element_type=F32)
                kv[part, s, where, :] = y.astype(BF16)
                return carry

            lax.fori_loop(0, seqs * (span // tile), body, 0)

    if tp_count > 1:
        counted(bias.at[pl.ds(0, tp_count - 1)], receives.at[0]).wait()
    bias[tp] = bias_all[:, tp]
    for s in range(seqs):
        bias_out[s] = jnp.concatenate([bias[t, s] for t in range(tp_count)], axis=1)
    with jax.named_scope("await_mix"):
        counted(packed.at[pl.ds(0, n - 1)], receives.at[4]).wait()
    with jax.named_scope("drain"):
        counted(wts.at[0, pl.ds(0, n - 1)], sends.at[0]).wait()
        counted(ubuf.at[pl.ds(0, n - 1)], sends.at[1]).wait()
        counted(wts.at[0, pl.ds(0, n - 1)], sends.at[2]).wait()
        if tp_count > 1:
            others = pl.ds(0, tp_count - 1)
            counted(tok.at[:, pl.ds(0, (tp_count - 1) * pos), :], sends.at[3]).wait()
            counted(bias.at[others], sends.at[4]).wait()
            counted(pin.at[others, :, tail], sends.at[5]).wait()
            counted(tot_in.at[others], sends.at[6]).wait()
            if chunked:
                counted(win.at[others], sends.at[7]).wait()
        counted(packed.at[pl.ds(0, n - 1)], sends.at[8]).wait()


def finish(
    n, head_dim, kv, bias, packed, tok, wts, acc,
    key_out, value_out, bias_out, reading_out, key, reading, sems,
):
    _, _, rows, _ = wts.shape
    chunked = rows % 128 == 0
    moves = [
        pltpu.make_async_copy(kv.at[1], value_out, sems.at[0]),
        pltpu.make_async_copy(bias, bias_out, sems.at[1]),
    ]
    if not chunked:
        moves.append(pltpu.make_async_copy(kv.at[0], key_out, sems.at[2]))
    for c in moves:
        c.start()
    if chunked:
        for s in range(key_out.shape[0]):
            y = jnp.dot(
                tok[s, :, (n - 1) * rows :], wts[0, n - 1], preferred_element_type=F32
            )
            key[s] = (acc[0, s] + y).astype(BF16)
            moves.append(pltpu.make_async_copy(key.at[s], key_out.at[s], sems.at[4 + s]))
            moves[-1].start()
    seqs, cols = reading_out.shape
    rows_h = max(8, cols // head_dim)
    row_id = lax.broadcasted_iota(jnp.int32, (rows_h, cols), 0)
    col_id = lax.broadcasted_iota(jnp.int32, (rows_h, cols), 1)
    own = row_id == col_id // head_dim
    mixture = jnp.zeros((seqs, cols), F32)
    carry = jnp.zeros((seqs, cols), F32)
    for at in range(n - 1, -1, -1):
        mixture = mixture + jnp.exp(carry) * packed[at, :seqs]
        carry = carry + packed[at, seqs:]
    for s in range(seqs):
        x = mixture[s : s + 1]
        mean = jnp.sum(jnp.where(own, x * x, 0.0), axis=1, keepdims=True) / head_dim
        scale = jnp.sum(jnp.where(own, lax.rsqrt(mean + 1e-06), 0.0), axis=0, keepdims=True)
        reading[s : s + 1] = x * scale
    moves.append(pltpu.make_async_copy(reading, reading_out, sems.at[3]))
    moves[-1].start()
    for c in moves:
        c.wait()


def per_device(tokens, key_weight, value_weight, queries, head_offset, key_bias):
    n, tp_count = lax.axis_size("sp"), lax.axis_size("tp")
    assert n % 2 == 0 and lax.axis_size("gr") == 2
    seqs, pos, width = tokens.shape
    rows, kv_width = key_weight.shape
    head_count = head_offset.shape[0]
    head_dim = kv_width // head_count
    cols = kv_width // tp_count
    heads = head_count // tp_count
    rows_h = max(8, heads)
    span = tp_count * pos
    hops = n // 2
    bias_rows = jnp.transpose(key_bias, (0, 2, 1)).reshape(seqs, tp_count, heads, pos)
    group = tp_count * rows_h
    own_bias = jnp.pad(bias_rows, ((0, 0), (0, 0), (0, rows_h - heads), (0, 0)))
    own_bias = own_bias.reshape(seqs, group, pos)
    dims = (n, tp_count, seqs, pos, width, rows, cols, heads, head_dim, rows_h)
    groups = hops + 1 if (width // n) % 128 == 0 else 1
    dma = pltpu.SemaphoreType.DMA
    kv, bias_held, packed, tok, wts, acc = pl.pallas_call(
        functools.partial(kernel, dims),
        out_shape=(
            jax.ShapeDtypeStruct((2, seqs, span, cols), BF16),
            jax.ShapeDtypeStruct((seqs, heads, span), BF16),
            jax.ShapeDtypeStruct((n, 2 * seqs, cols), F32),
            jax.ShapeDtypeStruct((seqs, span, width), BF16),
            jax.ShapeDtypeStruct((2, n, rows, cols), BF16),
            jax.ShapeDtypeStruct((2, seqs, span, cols), F32),
        ),
        in_specs=[pl.BlockSpec(memory_space=pltpu.HBM)] * 7,
        out_specs=[pl.BlockSpec(memory_space=pltpu.VMEM)] * 6,
        scratch_shapes=[
            pltpu.VMEM((tp_count, seqs, heads, pos), BF16),
            pltpu.VMEM(queries.shape, BF16),
            pltpu.VMEM((1, head_count), F32),
            pltpu.VMEM((seqs, tp_count, heads, pos), BF16),
            pltpu.VMEM((seqs, group, pos), BF16),
            pltpu.VMEM((rows, kv_width), BF16),
            pltpu.VMEM((n, seqs * group, rows), BF16),
            pltpu.VMEM((seqs * group, width), BF16),
            pltpu.VMEM((tp_count, seqs * rows_h, width), BF16),
            pltpu.VMEM((tp_count, seqs * rows_h, width), BF16),
            pltpu.VMEM((tp_count, seqs * rows_h, width), BF16),
            pltpu.VMEM((tp_count, seqs * rows_h, 128), F32),
            pltpu.VMEM((tp_count, seqs * rows_h, 128), F32),
            pltpu.VMEM((tp_count, seqs * rows_h, pos), BF16),
            pltpu.VMEM((tp_count, seqs * rows_h, pos), BF16),
            dma((8,)),
            dma((2,)),
            dma((9,)),
            dma((5,)),
            dma((2, hops - 1, MARK + 1)),
            dma((MARK + 1,)),
            dma((2, hops)),
            dma((groups, seqs)),
            pltpu.SemaphoreType.REGULAR((4,)),
        ],
        compiler_params=pltpu.CompilerParams(
            collective_id=0, has_side_effects=True, vmem_limit_bytes=36 * 2**20
        ),
        name="prefill",
    )(*(pltpu.with_memory_space_constraint(a, pltpu.HBM) for a in (tokens, key_weight, value_weight, queries, head_offset.reshape(1, head_count), bias_rows, own_bias)))
    key_cache, value_cache, bias_cache, reading = pl.pallas_call(
        functools.partial(finish, n, head_dim),
        out_shape=(
            jax.ShapeDtypeStruct((seqs, span, cols), BF16),
            jax.ShapeDtypeStruct((seqs, span, cols), BF16),
            jax.ShapeDtypeStruct((seqs, heads, span), BF16),
            jax.ShapeDtypeStruct((seqs, cols), F32),
        ),
        in_specs=[
            pl.BlockSpec(memory_space=pl.ANY),
            pl.BlockSpec(memory_space=pl.ANY),
            *[pl.BlockSpec(memory_space=pltpu.VMEM)] * 4,
        ],
        out_specs=[
            pl.BlockSpec(memory_space=pl.ANY),
            pl.BlockSpec(memory_space=pl.ANY),
            pl.BlockSpec(memory_space=pl.ANY),
            pl.BlockSpec(memory_space=pl.ANY),
        ],
        scratch_shapes=[
            pltpu.VMEM((seqs, span, cols), BF16), pltpu.VMEM((seqs, cols), F32), dma((4 + seqs,))
        ],
        compiler_params=pltpu.CompilerParams(vmem_limit_bytes=16 * 2**20),
        name="finish",
    )(kv, bias_held, packed, tok, wts, acc)
    return key_cache, value_cache, jnp.transpose(bias_cache, (0, 2, 1)), reading


def solution(mesh):
    in_specs = (
        P("gr", ("sp", "tp"), None),
        P("sp", None),
        P("sp", None),
        P("gr", None),
        P(),
        P("gr", ("sp", "tp"), None),
    )
    out_specs = (P("gr", "sp", "tp"), P("gr", "sp", "tp"), P("gr", "sp", "tp"), P("gr", "tp"))
    return jax.shard_map(
        per_device, mesh=mesh, in_specs=in_specs, out_specs=out_specs, check_vma=False
    )
```

```python
import functools

import jax
import jax.numpy as jnp
from jax import lax
from jax.experimental import pallas as pl
from jax.experimental.pallas import tpu as pltpu
from jax.sharding import PartitionSpec as P

MESH = pl.DeviceIdType.MESH
F32 = jnp.float32
BF16 = jnp.bfloat16
VALUE_SUBS = 2
KEY_SUBS = 4
MARK = VALUE_SUBS + KEY_SUBS
EARLY_HOPS = 2
OPEN, PASS, TOKENS, MULTIPLY, PROJECT, READ, MIX = range(7)


def plan(hops, seqs):
    if hops == 4 and seqs == 2:
        return TUNED
    value, key = range(VALUE_SUBS), range(VALUE_SUBS, MARK)
    first = [0, MARK, *value[1:]]
    steps = [(OPEN, 0), (TOKENS, 4), (PROJECT,), *((OPEN, p) for p in first[1:])]
    for hop in range(1, hops):
        steps += [(PASS, hop, p) for p in first] + [(TOKENS, 4 + 2 * hop)]
    steps += [(OPEN, p) for p in key]
    steps += [(PASS, hops, p) for p in first] + [(READ,), (TOKENS, 4 * hops * seqs)]
    for hop in range(1, hops + 1):
        steps += [(PASS, hop, p) for p in key]
        if hop == min(2, hops):
            steps.append((MIX,))
        for h in range(hop + 1) if hop == 1 else [hop]:
            steps += [(MULTIPLY, part, h, s) for part in (1, 0) for s in range(seqs)]
    return steps


TUNED = (
    (OPEN, 0), (TOKENS, 6), (PROJECT,), (OPEN, MARK), (OPEN, 1), (OPEN, 4), (OPEN, 5),
    (PASS, 1, MARK), (MULTIPLY, 0, 0, 0), (TOKENS, 10), (PASS, 1, 0), (PASS, 1, 1), (PASS, 2, MARK),
    (OPEN, 2), (OPEN, 3), (PASS, 2, 0), (PASS, 3, MARK), (PASS, 2, 1), (PASS, 1, 4), (PASS, 1, 5),
    (PASS, 1, 2), (PASS, 1, 3), (PASS, 4, MARK), (READ,), (PASS, 3, 1), (TOKENS, 13), (TOKENS, 15),
    (PASS, 3, 0), (MULTIPLY, 1, 0, 1), (MULTIPLY, 1, 0, 0), (MULTIPLY, 1, 1, 0), (PASS, 2, 4),
    (PASS, 2, 5), (MULTIPLY, 0, 1, 0), (MULTIPLY, 1, 2, 0), (PASS, 2, 2), (PASS, 2, 3),
    (MULTIPLY, 1, 2, 1), (PASS, 4, 1), (MULTIPLY, 0, 0, 1), (PASS, 4, 0), (MIX,), (TOKENS, 16),
    (PASS, 3, 4), (PASS, 3, 5), (PASS, 3, 2), (PASS, 3, 3), (MULTIPLY, 0, 2, 1),
    (MULTIPLY, 0, 1, 1), (MULTIPLY, 0, 3, 0), (MULTIPLY, 1, 3, 0), (MULTIPLY, 1, 1, 1),
    (MULTIPLY, 0, 2, 0), (MULTIPLY, 1, 3, 1), (MULTIPLY, 0, 3, 1), (PASS, 4, 4), (PASS, 4, 5),
    (PASS, 4, 2), (PASS, 4, 3), (MULTIPLY, 1, 4, 0), (MULTIPLY, 1, 4, 1), (MULTIPLY, 0, 4, 1),
    (MULTIPLY, 0, 4, 0),
)


def ring_place(index, length):
    lane, row = lax.rem(index, 2), index // 2
    return row * (1 - lane) + (length - 1 - row) * lane


def ring_index(place, length):
    lane = place // (length // 2)
    row = place * (1 - lane) + (length - 1 - place) * lane
    return 2 * row + lane


def kernel(
    dims,
    tokens, key_weight, value_weight, queries, head_offset, key_bias, own_bias,
    kv, bias_out, packed, tok, wts, acc,
    bias, query, offset, bias_all, bias_own, key_rows,
    ubuf, ucat, pout, pin, plow, tot_out, tot_in, wout, win,
    local_sem, tok_load, sends, receives, ring_recv, last_recv, pair_recv, tok_recv, ready,
):
    n, tp_count, seqs, pos, width, rows, cols, heads, head_dim, rows_h = dims
    hops = n // 2
    half_rows = rows // 2
    span = tp_count * pos
    kv_width = tp_count * cols
    group = tp_count * rows_h
    me, tp, gr = lax.axis_index("sp"), lax.axis_index("tp"), lax.axis_index("gr")
    place = ring_place(me, n)

    def owner_at(step):
        return ring_index(lax.rem(place + step + n, n), n)

    right, left = owner_at(1), owner_at(-1)
    partner = 1 - gr
    col_start = pl.multiple_of(tp * cols, 128)
    chunked = (width // n) % 128 == 0
    order = [0]
    for h in range(1, hops + 1):
        order.extend([-h, h] if h < hops else [h])
    chunk = width // n if chunked else width
    chunk_count = n if chunked else 1
    early = min(EARLY_HOPS, hops - 1) if chunked else -1
    cut = (2 * early + 1) * chunk if chunked else 0
    tail = slice(cut, width)
    crossing = 3 if chunked else 2

    def slot_of(step):
        if not chunked:
            return owner_at(step)
        return order.index(hops if abs(step) == hops else step)

    my_rows = pl.ds(pl.multiple_of(tp * pos, pos), pos)

    key_copy = pltpu.make_async_copy(key_weight, key_rows, local_sem.at[6])
    query_copy = pltpu.make_async_copy(queries, query, local_sem.at[4])
    weight_copies = [
        pltpu.make_async_copy(
            w.at[:, pl.ds(col_start, cols)], wts.at[part, slot_of(0)], local_sem.at[part]
        )
        for part, w in enumerate((key_weight, value_weight))
    ]

    def columns(i):
        return slice(i * chunk, (i + 1) * chunk)

    def columns_held(i):
        if not chunked:
            return slice(0, width)
        return pl.ds(pl.multiple_of(owner_at(order[i]) * chunk, 128), chunk)

    tok_copies = [
        pltpu.make_async_copy(
            tokens.at[:, :, columns_held(i)], tok.at[:, my_rows, columns(i)],
            tok_load.at[min(i, 1)],
        )
        for i in range(chunk_count)
    ]
    bias_copy = pltpu.make_async_copy(key_bias, bias_all, local_sem.at[3])
    own_bias_copy = pltpu.make_async_copy(own_bias, bias_own, local_sem.at[7])
    offset_copy = pltpu.make_async_copy(head_offset, offset, local_sem.at[5])
    for c in (
        weight_copies[1], tok_copies[0], query_copy, key_copy, *tok_copies[1:], weight_copies[0],
        bias_copy, own_bias_copy, offset_copy,
    ):
        c.start()

    tp_peers = [lax.rem(tp + k, tp_count) for k in range(1, tp_count)]
    barrier = pltpu.get_barrier_semaphore()
    ring = (right, left)

    def signal(semaphore, target):
        pl.semaphore_signal(semaphore, inc=1, device_id=target, device_id_type=MESH)

    for target in ring:
        pl.when(target > me)(functools.partial(signal, barrier, {"sp": target}))
    pl.when(gr == 0)(functools.partial(signal, barrier, {"gr": partner}))
    for peer in tp_peers:
        pl.when(peer > tp)(functools.partial(signal, barrier, {"tp": peer}))

    def part_of(piece):
        return 1 if piece < VALUE_SUBS else 0

    def rows_of(piece, core):
        part = part_of(piece)
        size = half_rows // (VALUE_SUBS if part == 1 else KEY_SUBS)
        sub = piece - (0 if part == 1 else VALUE_SUBS)
        return pl.ds(pl.multiple_of(core * half_rows + sub * size, size), size)

    def block_of(piece, step, core):
        if piece == MARK:
            return ubuf.at[slot_of(step)]
        return wts.at[part_of(piece), slot_of(step), rows_of(piece, core), :]

    def ring_copy(direction, hop, piece):
        return pltpu.make_async_remote_copy(
            src_ref=block_of(piece, step_of(direction, hop - 1), gr),
            dst_ref=block_of(piece, step_of(direction, hop), gr),
            send_sem=sends.at[1 if piece == MARK else 0],
            recv_sem=(last_recv.at[piece] if hop == hops else ring_recv.at[hop - 1, piece]),
            device_id={"sp": right if direction == 0 else left}, device_id_type=MESH,
        )

    def step_of(direction, hop):
        return -hop if direction == 0 else hop

    def used(direction, hop, piece):
        return hop < hops or (hop == hops and piece % 2 == direction)

    def pair_copy(direction, hop, piece, core):
        block = block_of(piece, step_of(direction, hop), core)
        return pltpu.make_async_remote_copy(
            src_ref=block, dst_ref=block,
            send_sem=sends.at[2], recv_sem=pair_recv.at[part_of(piece), hop - 1],
            device_id={"gr": partner}, device_id_type=MESH,
        )

    def peer_of(k):
        return lax.rem(tp + k + 1, tp_count)

    def source_of(k):
        return lax.rem(tp + tp_count - k - 1, tp_count)

    def tok_move(i, s, k, source):
        place_rows = pl.ds(pl.multiple_of(source * pos, pos), pos)
        block = tok.at[s, place_rows, columns(i)]
        return pltpu.make_async_remote_copy(
            src_ref=block, dst_ref=block,
            send_sem=sends.at[3], recv_sem=tok_recv.at[(i + 1) // 2 if chunked else 0, s],
            device_id={"tp": peer_of(k)}, device_id_type=MESH,
        )

    def bias_move(k, source, target):
        return pltpu.make_async_remote_copy(
            src_ref=bias_all.at[:, target], dst_ref=bias.at[source],
            send_sem=sends.at[4], recv_sem=receives.at[0],
            device_id={"tp": peer_of(k)}, device_id_type=MESH,
        )

    def read_move(k, which, source, target):
        if which == 0:
            out, into = pout.at[target, :, tail], pin.at[source, :, tail]
        elif which == 1:
            out, into = tot_out.at[target], tot_in.at[source]
        else:
            out, into = wout.at[target], win.at[source]
        return pltpu.make_async_remote_copy(
            src_ref=out, dst_ref=into,
            send_sem=sends.at[5 + which], recv_sem=receives.at[1 + which],
            device_id={"tp": peer_of(k)}, device_id_type=MESH,
        )

    def launch(c):
        c.start()

    def counted(ref, sem):
        return pltpu.make_async_copy(ref, ref, sem)

    issued = [0]

    def load_tokens(i):
        if i == 0:
            tok_copies[0].wait()
        else:
            counted(tok.at[:, my_rows, chunk:], tok_load.at[1]).wait()

    def send_tokens(upto, ahead=None):
        upto = min(upto, chunk_count * seqs)
        for i, s in (divmod(unit, seqs) for unit in range(issued[0], upto)):
            if s == 0 and i < 2 and ahead is not True:
                load_tokens(i)
            for k in range(tp_count - 1):

                def start(i=i, s=s, k=k):
                    launch(tok_move(i, s, k, tp))

                if ahead is None:
                    start()
                else:
                    pl.when((peer_of(k) > tp) == ahead)(start)
        if ahead is not False:
            issued[0] = upto

    def open_ring(piece, ahead=None):
        for direction in range(2):
            if not used(direction, 1, piece):
                continue

            def start(direction=direction):
                launch(ring_copy(direction, 1, piece))

            if ahead is None:
                start()
            else:
                pl.when((ring[direction] > me) == ahead)(start)

    def arrived(hop, piece):
        if hop == hops:
            last = next(d for d in range(2) if used(d, hop, piece))
            ring_copy(last, hop, piece).wait_recv()
        elif piece == MARK:
            counted(ubuf.at[pl.ds(0, 2)], ring_recv.at[hop - 1, piece]).wait()
        else:
            part = part_of(piece)
            both = 2 * (half_rows // (VALUE_SUBS if part == 1 else KEY_SUBS))
            counted(wts.at[part, 0, pl.ds(0, both)], ring_recv.at[hop - 1, piece]).wait()

    def pass_on(hop, piece):
        arrived(hop, piece)
        for direction in range(2):
            if not used(direction, hop, piece):
                continue
            if hop < hops and used(direction, hop + 1, piece):
                launch(ring_copy(direction, hop + 1, piece))
            if piece != MARK:
                launch(pair_copy(direction, hop, piece, gr))

    def project():
        query_copy.wait()
        key_copy.wait()
        row = lax.broadcasted_iota(jnp.int32, (group, kv_width), 0)
        col_head = lax.broadcasted_iota(jnp.int32, (group, kv_width), 1) // head_dim
        inner = lax.rem(row, rows_h)
        mine = (row // rows_h * heads + inner == col_head) & (inner < heads)
        q = query[...].astype(F32)
        q_rows = jnp.concatenate(
            [jnp.where(mine, q[s : s + 1], 0.0) for s in range(seqs)], axis=0
        ).astype(BF16)
        ubuf[slot_of(0)] = lax.dot_general(
            q_rows, key_rows[...], (((1,), (1,)), ((), ())), preferred_element_type=F32
        ).astype(BF16)

    def greet():
        behind = (right < me).astype(jnp.int32) + (left < me).astype(jnp.int32) + gr + tp
        pl.when(behind > 0)(lambda: pl.semaphore_wait(barrier, behind))
        for direction in range(2):
            target = ring[direction]
            semaphore = ready.at[1 - direction]
            pl.when(target < me)(functools.partial(signal, semaphore, {"sp": target}))
        pl.when(gr == 1)(functools.partial(signal, ready.at[2], {"gr": partner}))
        for peer in tp_peers:
            pl.when(peer < tp)(functools.partial(signal, ready.at[3], {"tp": peer}))

    def begin(steps):
        with jax.named_scope("greet"):
            greet()
        for kind, *what in steps:
            if kind == OPEN:
                if what[0] != MARK:
                    weights_here(part_of(what[0]))
                open_ring(what[0], False)
            elif kind == TOKENS:
                send_tokens(what[0], False)
            elif kind == PROJECT:
                with jax.named_scope("project"):
                    project()
        with jax.named_scope("ready"):
            for direction in range(2):
                semaphore = ready.at[direction]
                pl.when(ring[direction] > me)(
                    functools.partial(pl.semaphore_wait, semaphore, 1)
                )
            ahead = tp_count - 1 - tp
            pl.when(ahead > 0)(lambda: pl.semaphore_wait(ready.at[3], ahead))
        for kind, *what in steps:
            if kind == OPEN:
                open_ring(what[0], True)
            elif kind == TOKENS:
                send_tokens(what[0], True)
        pl.when(gr == 0)(functools.partial(pl.semaphore_wait, ready.at[2], 1))
        bias_copy.wait()
        for k in range(tp_count - 1):
            launch(bias_move(k, tp, peer_of(k)))

    def read():
        own_bias_copy.wait()
        offset_copy.wait()
        for owner in range(n):
            ucat[:, owner * rows : (owner + 1) * rows] = ubuf[owner]
        total_heads = offset.shape[1]
        pick_row = lax.broadcasted_iota(jnp.int32, (group, total_heads), 0)
        pick_inner = lax.rem(pick_row, rows_h)
        pick = (
            lax.broadcasted_iota(jnp.int32, (group, total_heads), 1)
            == pick_row // rows_h * heads + pick_inner
        ) & (pick_inner < heads)
        offset_col = jnp.sum(jnp.where(pick, offset[...], 0.0), axis=1, keepdims=True)
        logits = []
        for s in range(seqs):
            logits.append(
                lax.dot_general(
                    ucat[s * group : (s + 1) * group, :], tok[s, my_rows, :],
                    (((1,), (1,)), ((), ())), preferred_element_type=F32,
                )
                * (head_dim**-0.5)
                + offset_col
                + bias_own[s].astype(F32)
            )
        logits = jnp.concatenate(logits, axis=0)
        soft = jnp.log1p(jnp.exp(-jnp.abs(logits)))
        fading = -jnp.maximum(logits, 0.0) - soft
        taking = jnp.minimum(logits, 0.0) - soft
        high = fading.astype(BF16)
        rest = fading - high.astype(F32)
        mid = rest.astype(BF16)
        low = (rest - mid.astype(F32)).astype(BF16)
        later = (
            lax.broadcasted_iota(jnp.int32, (pos, pos), 0)
            > lax.broadcasted_iota(jnp.int32, (pos, pos), 1)
        ).astype(F32).astype(BF16)
        sums = jnp.dot(
            jnp.concatenate([high, mid, low], axis=0), later, preferred_element_type=F32
        )
        m = seqs * group
        within = sums[:m] + sums[m : 2 * m] + sums[2 * m :]
        weights = jnp.exp(taking + within)
        totals = jnp.sum(fading, axis=1, keepdims=True)
        spread = jnp.broadcast_to(totals, (m, 128))
        weighted = [
            jnp.dot(
                weights[s * group : (s + 1) * group].astype(BF16), tok[s, my_rows, :],
                preferred_element_type=F32,
            )
            for s in range(seqs)
        ]
        for t in range(tp_count):
            at = slice(t * rows_h, (t + 1) * rows_h)
            wout[t] = jnp.concatenate(
                [weights[s * group : (s + 1) * group][at] for s in range(seqs)], axis=0
            ).astype(BF16)
            tot_out[t] = jnp.concatenate(
                [spread[s * group + t * rows_h : s * group + (t + 1) * rows_h] for s in range(seqs)],
                axis=0,
            )
            whole = jnp.concatenate([weighted[s][at] for s in range(seqs)], axis=0)
            upper = whole.astype(BF16)
            pout[t] = upper
            plow[t] = (whole - upper.astype(F32)).astype(BF16)
        for k in range(tp_count - 1):
            for which in range(crossing):
                launch(read_move(k, which, tp, peer_of(k)))
        pin[tp] = pout[tp]
        tot_in[tp] = tot_out[tp]

    seen = set()

    def weights_here(part):
        if ("weights", part) not in seen:
            seen.add(("weights", part))
            weight_copies[part].wait()

    def pair_ready(part, hop):
        if hop == 0 or ("pair", part, hop) in seen:
            return
        seen.add(("pair", part, hop))
        held = wts.at[part, slot_of(hop)]
        if hop == hops:
            held = held.at[pl.ds(0, half_rows), :]
        counted(held, pair_recv.at[part, hop - 1]).wait()

    def tokens_ready(hop, s):
        if ("tok", hop, s) in seen or tp_count == 1:
            return
        seen.add(("tok", hop, s))
        first, end = slots_of_hop(hop) if chunked else (0, 1)
        counted(
            tok.at[s, pl.ds(0, (tp_count - 1) * pos), slice(first * chunk, end * chunk)],
            tok_recv.at[hop, s],
        ).wait()

    def slots_of_hop(hop):
        if hop == 0:
            return 0, 1
        first = 1 + 2 * (hop - 1)
        return first, min(first + 2, n)

    def multiply(part, hop, s):
        if not chunked:
            return
        first, end = slots_of_hop(hop)
        with jax.named_scope(f"multiply{part}_{hop}_{s}"):
            if hop == 0:
                weights_here(part)
            pair_ready(part, hop)
            tokens_ready(hop, s)
            y = jnp.dot(
                tok[s, :, first * chunk : end * chunk],
                wts[part, first:end].reshape((end - first) * rows, cols),
                preferred_element_type=F32,
            )
            if hop > 0:
                y = acc[part, s] + y
            if hop < hops:
                acc[part, s] = y
            else:
                kv[part, s] = y.astype(BF16)

    def leave():
        if chunked:
            pair_ready(0, hops)
            for s in range(seqs):
                tokens_ready(hops, s)

    def mix_move(k, source):
        return pltpu.make_async_remote_copy(
            src_ref=packed.at[source], dst_ref=packed.at[source],
            send_sem=sends.at[8], recv_sem=receives.at[4],
            device_id={"sp": lax.rem(me + k, n)}, device_id_type=MESH,
        )

    def mix():
        with jax.named_scope("await_products"):
            if tp_count > 1:
                others = pl.ds(0, tp_count - 1)
                counted(pin.at[others, :, tail], receives.at[1]).wait()
                counted(tot_in.at[others], receives.at[2]).wait()
                if chunked:
                    counted(win.at[others], receives.at[3]).wait()
            for hop in range(1, hops + 1):
                pair_ready(1, hop)
        if chunked:
            for h in range(early + 1):
                for s in range(seqs):
                    tokens_ready(h, s)
            for k in range(tp_count - 1):
                source = source_of(k)
                where = pl.ds(pl.multiple_of(source * pos, pos), pos)
                held = win[source].astype(F32)
                pin[source, :, 0:cut] = jnp.concatenate(
                    [
                        jnp.dot(
                            held[s * rows_h : (s + 1) * rows_h].astype(BF16),
                            tok[s, where, 0:cut], preferred_element_type=F32,
                        )
                        for s in range(seqs)
                    ],
                    axis=0,
                ).astype(BF16)
        count = seqs * rows_h
        given = jnp.concatenate([pin[t] for t in range(tp_count)] + [plow[tp]], axis=0)
        product = jnp.dot(
            given, wts[1].reshape(width, cols), preferred_element_type=F32
        )
        carry = jnp.zeros((count, 1), F32)
        mixture = jnp.zeros((count, cols), F32)
        for t in range(tp_count - 1, -1, -1):
            term = product[t * count : (t + 1) * count]
            term = term + jnp.where(tp == t, 1.0, 0.0) * product[tp_count * count :]
            mixture = mixture + jnp.exp(carry) * term
            carry = carry + tot_in[t][:, :1]
        own = lax.broadcasted_iota(jnp.int32, (rows_h, cols), 0) == (
            lax.broadcasted_iota(jnp.int32, (rows_h, cols), 1) // head_dim
        )
        for s in range(seqs):
            at = slice(s * rows_h, (s + 1) * rows_h)
            packed[me, s : s + 1] = jnp.sum(
                jnp.where(own, mixture[at], 0.0), axis=0, keepdims=True
            )
            packed[me, seqs + s : seqs + s + 1] = jnp.sum(
                jnp.where(own, carry[at], 0.0), axis=0, keepdims=True
            )
        for k in range(1, n):
            launch(mix_move(k, me))

    steps = list(plan(hops, seqs))
    opening = next(i for i, step in enumerate(steps) if step[0] == PASS)
    begin(steps[:opening])
    for kind, *what in steps[opening:]:
        if kind == OPEN:
            if what[0] != MARK:
                weights_here(part_of(what[0]))
            open_ring(what[0])
        elif kind == PASS:
            with jax.named_scope(f"pass{what[0]}_{what[1]}"):
                pass_on(*what)
        elif kind == TOKENS:
            send_tokens(what[0])
        elif kind == MULTIPLY:
            if what[:2] != [0, hops]:
                multiply(*what)
        elif kind == READ:
            with jax.named_scope("read"):
                read()
        elif kind == MIX:
            with jax.named_scope("mix"):
                mix()

    leave()
    if not chunked:
        for s in range(seqs):
            tokens_ready(0, s)
        for hop in range(1, hops + 1):
            pair_ready(0, hop)
        tile = pos
        for part in range(2):
            w = wts[part].reshape(width, cols)

            def body(j, carry):
                s, r = j // (span // tile), lax.rem(j, span // tile)
                where = pl.ds(pl.multiple_of(r * tile, tile), tile)
                y = jnp.dot(tok[s, where, :], w, preferred_element_type=F32)
                kv[part, s, where, :] = y.astype(BF16)
                return carry

            lax.fori_loop(0, seqs * (span // tile), body, 0)

    if tp_count > 1:
        counted(bias.at[pl.ds(0, tp_count - 1)], receives.at[0]).wait()
    bias[tp] = bias_all[:, tp]
    for s in range(seqs):
        bias_out[s] = jnp.concatenate([bias[t, s] for t in range(tp_count)], axis=1)
    with jax.named_scope("await_mix"):
        counted(packed.at[pl.ds(0, n - 1)], receives.at[4]).wait()
    with jax.named_scope("drain"):
        counted(wts.at[0, pl.ds(0, n - 1)], sends.at[0]).wait()
        counted(ubuf.at[pl.ds(0, n - 1)], sends.at[1]).wait()
        counted(wts.at[0, pl.ds(0, n - 1)], sends.at[2]).wait()
        if tp_count > 1:
            others = pl.ds(0, tp_count - 1)
            counted(tok.at[:, pl.ds(0, (tp_count - 1) * pos), :], sends.at[3]).wait()
            counted(bias.at[others], sends.at[4]).wait()
            counted(pin.at[others, :, tail], sends.at[5]).wait()
            counted(tot_in.at[others], sends.at[6]).wait()
            if chunked:
                counted(win.at[others], sends.at[7]).wait()
        counted(packed.at[pl.ds(0, n - 1)], sends.at[8]).wait()


def finish(
    n, head_dim, kv, bias, packed, tok, wts, acc,
    key_out, value_out, bias_out, reading_out, key, reading, sems,
):
    _, _, rows, _ = wts.shape
    chunked = rows % 128 == 0
    moves = [
        pltpu.make_async_copy(kv.at[1], value_out, sems.at[0]),
        pltpu.make_async_copy(bias, bias_out, sems.at[1]),
    ]
    if not chunked:
        moves.append(pltpu.make_async_copy(kv.at[0], key_out, sems.at[2]))
    for c in moves:
        c.start()
    if chunked:
        for s in range(key_out.shape[0]):
            y = jnp.dot(
                tok[s, :, (n - 1) * rows :], wts[0, n - 1], preferred_element_type=F32
            )
            key[s] = (acc[0, s] + y).astype(BF16)
            moves.append(pltpu.make_async_copy(key.at[s], key_out.at[s], sems.at[4 + s]))
            moves[-1].start()
    seqs, cols = reading_out.shape
    rows_h = max(8, cols // head_dim)
    row_id = lax.broadcasted_iota(jnp.int32, (rows_h, cols), 0)
    col_id = lax.broadcasted_iota(jnp.int32, (rows_h, cols), 1)
    own = row_id == col_id // head_dim
    mixture = jnp.zeros((seqs, cols), F32)
    carry = jnp.zeros((seqs, cols), F32)
    for at in range(n - 1, -1, -1):
        mixture = mixture + jnp.exp(carry) * packed[at, :seqs]
        carry = carry + packed[at, seqs:]
    for s in range(seqs):
        x = mixture[s : s + 1]
        mean = jnp.sum(jnp.where(own, x * x, 0.0), axis=1, keepdims=True) / head_dim
        scale = jnp.sum(jnp.where(own, lax.rsqrt(mean + 1e-06), 0.0), axis=0, keepdims=True)
        reading[s : s + 1] = x * scale
    moves.append(pltpu.make_async_copy(reading, reading_out, sems.at[3]))
    moves[-1].start()
    for c in moves:
        c.wait()


def per_device(tokens, key_weight, value_weight, queries, head_offset, key_bias):
    n, tp_count = lax.axis_size("sp"), lax.axis_size("tp")
    assert n % 2 == 0 and lax.axis_size("gr") == 2
    seqs, pos, width = tokens.shape
    rows, kv_width = key_weight.shape
    head_count = head_offset.shape[0]
    head_dim = kv_width // head_count
    cols = kv_width // tp_count
    heads = head_count // tp_count
    rows_h = max(8, heads)
    span = tp_count * pos
    hops = n // 2
    bias_rows = jnp.transpose(key_bias, (0, 2, 1)).reshape(seqs, tp_count, heads, pos)
    group = tp_count * rows_h
    own_bias = jnp.pad(bias_rows, ((0, 0), (0, 0), (0, rows_h - heads), (0, 0)))
    own_bias = own_bias.reshape(seqs, group, pos)
    dims = (n, tp_count, seqs, pos, width, rows, cols, heads, head_dim, rows_h)
    groups = hops + 1 if (width // n) % 128 == 0 else 1
    dma = pltpu.SemaphoreType.DMA
    kv, bias_held, packed, tok, wts, acc = pl.pallas_call(
        functools.partial(kernel, dims),
        out_shape=(
            jax.ShapeDtypeStruct((2, seqs, span, cols), BF16),
            jax.ShapeDtypeStruct((seqs, heads, span), BF16),
            jax.ShapeDtypeStruct((n, 2 * seqs, cols), F32),
            jax.ShapeDtypeStruct((seqs, span, width), BF16),
            jax.ShapeDtypeStruct((2, n, rows, cols), BF16),
            jax.ShapeDtypeStruct((2, seqs, span, cols), F32),
        ),
        in_specs=[pl.BlockSpec(memory_space=pltpu.HBM)] * 7,
        out_specs=[pl.BlockSpec(memory_space=pltpu.VMEM)] * 6,
        scratch_shapes=[
            pltpu.VMEM((tp_count, seqs, heads, pos), BF16),
            pltpu.VMEM(queries.shape, BF16),
            pltpu.VMEM((1, head_count), F32),
            pltpu.VMEM((seqs, tp_count, heads, pos), BF16),
            pltpu.VMEM((seqs, group, pos), BF16),
            pltpu.VMEM((rows, kv_width), BF16),
            pltpu.VMEM((n, seqs * group, rows), BF16),
            pltpu.VMEM((seqs * group, width), BF16),
            pltpu.VMEM((tp_count, seqs * rows_h, width), BF16),
            pltpu.VMEM((tp_count, seqs * rows_h, width), BF16),
            pltpu.VMEM((tp_count, seqs * rows_h, width), BF16),
            pltpu.VMEM((tp_count, seqs * rows_h, 128), F32),
            pltpu.VMEM((tp_count, seqs * rows_h, 128), F32),
            pltpu.VMEM((tp_count, seqs * rows_h, pos), BF16),
            pltpu.VMEM((tp_count, seqs * rows_h, pos), BF16),
            dma((8,)),
            dma((2,)),
            dma((9,)),
            dma((5,)),
            dma((hops - 1, MARK + 1)),
            dma((MARK + 1,)),
            dma((2, hops)),
            dma((groups, seqs)),
            pltpu.SemaphoreType.REGULAR((4,)),
        ],
        compiler_params=pltpu.CompilerParams(
            collective_id=0, has_side_effects=True, vmem_limit_bytes=36 * 2**20
        ),
        name="prefill",
    )(*(pltpu.with_memory_space_constraint(a, pltpu.HBM) for a in (tokens, key_weight, value_weight, queries, head_offset.reshape(1, head_count), bias_rows, own_bias)))
    key_cache, value_cache, bias_cache, reading = pl.pallas_call(
        functools.partial(finish, n, head_dim),
        out_shape=(
            jax.ShapeDtypeStruct((seqs, span, cols), BF16),
            jax.ShapeDtypeStruct((seqs, span, cols), BF16),
            jax.ShapeDtypeStruct((seqs, heads, span), BF16),
            jax.ShapeDtypeStruct((seqs, cols), F32),
        ),
        in_specs=[
            pl.BlockSpec(memory_space=pl.ANY),
            pl.BlockSpec(memory_space=pl.ANY),
            *[pl.BlockSpec(memory_space=pltpu.VMEM)] * 4,
        ],
        out_specs=[
            pl.BlockSpec(memory_space=pl.ANY),
            pl.BlockSpec(memory_space=pl.ANY),
            pl.BlockSpec(memory_space=pl.ANY),
            pl.BlockSpec(memory_space=pl.ANY),
        ],
        scratch_shapes=[
            pltpu.VMEM((seqs, span, cols), BF16), pltpu.VMEM((seqs, cols), F32), dma((4 + seqs,))
        ],
        compiler_params=pltpu.CompilerParams(vmem_limit_bytes=16 * 2**20),
        name="finish",
    )(kv, bias_held, packed, tok, wts, acc)
    return key_cache, value_cache, jnp.transpose(bias_cache, (0, 2, 1)), reading


def solution(mesh):
    in_specs = (
        P("gr", ("sp", "tp"), None),
        P("sp", None),
        P("sp", None),
        P("gr", None),
        P(),
        P("gr", ("sp", "tp"), None),
    )
    out_specs = (P("gr", "sp", "tp"), P("gr", "sp", "tp"), P("gr", "sp", "tp"), P("gr", "tp"))
    return jax.shard_map(
        per_device, mesh=mesh, in_specs=in_specs, out_specs=out_specs, check_vma=False
    )
```

```python
import functools

import jax
import jax.numpy as jnp
from jax import lax
from jax.experimental import pallas as pl
from jax.experimental.pallas import tpu as pltpu
from jax.sharding import PartitionSpec as P

MESH = pl.DeviceIdType.MESH
F32 = jnp.float32
BF16 = jnp.bfloat16
VALUE_SUBS = 2
KEY_SUBS = 4
MARK = VALUE_SUBS + KEY_SUBS
EARLY_HOPS = 2
OPEN, PASS, TOKENS, MULTIPLY, PROJECT, READ, MIX = range(7)


def plan(hops, seqs):
    if hops == 4 and seqs == 2:
        return TUNED
    value, key = range(VALUE_SUBS), range(VALUE_SUBS, MARK)
    first = [0, MARK, *value[1:]]
    steps = [(OPEN, 0), (TOKENS, 4), (PROJECT,), *((OPEN, p) for p in first[1:])]
    for hop in range(1, hops):
        steps += [(PASS, hop, p) for p in first] + [(TOKENS, 4 + 2 * hop)]
    steps += [(OPEN, p) for p in key]
    steps += [(PASS, hops, p) for p in first] + [(READ,), (TOKENS, 4 * hops * seqs)]
    for hop in range(1, hops + 1):
        steps += [(PASS, hop, p) for p in key]
        if hop == min(2, hops):
            steps.append((MIX,))
        for h in range(hop + 1) if hop == 1 else [hop]:
            steps += [(MULTIPLY, part, h, s) for part in (1, 0) for s in range(seqs)]
    return steps


TUNED = (
    (OPEN, 0), (TOKENS, 6), (PROJECT,), (OPEN, MARK), (OPEN, 1), (OPEN, 4), (OPEN, 5),
    (PASS, 1, MARK), (MULTIPLY, 0, 0, 0), (TOKENS, 10), (PASS, 1, 0), (PASS, 1, 1), (PASS, 2, MARK),
    (OPEN, 2), (OPEN, 3), (PASS, 2, 0), (PASS, 3, MARK), (PASS, 2, 1), (PASS, 1, 4), (PASS, 1, 5),
    (PASS, 1, 2), (PASS, 1, 3), (PASS, 4, MARK), (READ,), (PASS, 3, 1), (TOKENS, 13), (TOKENS, 15),
    (PASS, 3, 0), (MULTIPLY, 1, 0, 1), (MULTIPLY, 1, 0, 0), (MULTIPLY, 1, 1, 0), (PASS, 2, 4),
    (PASS, 2, 5), (MULTIPLY, 0, 1, 0), (MULTIPLY, 1, 2, 0), (PASS, 2, 2), (PASS, 2, 3),
    (MULTIPLY, 1, 2, 1), (PASS, 4, 1), (MULTIPLY, 0, 0, 1), (PASS, 4, 0), (MIX,), (TOKENS, 16),
    (PASS, 3, 4), (PASS, 3, 5), (PASS, 3, 2), (PASS, 3, 3), (MULTIPLY, 0, 2, 1),
    (MULTIPLY, 0, 1, 1), (MULTIPLY, 0, 3, 0), (MULTIPLY, 1, 3, 0), (MULTIPLY, 1, 1, 1),
    (MULTIPLY, 0, 2, 0), (MULTIPLY, 1, 3, 1), (MULTIPLY, 0, 3, 1), (PASS, 4, 4), (PASS, 4, 5),
    (PASS, 4, 2), (PASS, 4, 3), (MULTIPLY, 1, 4, 0), (MULTIPLY, 1, 4, 1), (MULTIPLY, 0, 4, 1),
    (MULTIPLY, 0, 4, 0),
)


def ring_place(index, length):
    lane, row = lax.rem(index, 2), index // 2
    return row * (1 - lane) + (length - 1 - row) * lane


def ring_index(place, length):
    lane = place // (length // 2)
    row = place * (1 - lane) + (length - 1 - place) * lane
    return 2 * row + lane


def kernel(
    dims,
    tokens, key_weight, value_weight, queries, head_offset, key_bias, own_bias,
    kv, bias_out, packed, tok, wts, acc,
    bias, query, offset, bias_all, bias_own, key_rows,
    ubuf, ucat, pout, pin, plow, tot_out, tot_in, wout, win,
    local_sem, tok_load, sends, receives, ring_recv, last_recv, pair_recv, tok_recv, ready,
):
    n, tp_count, seqs, pos, width, rows, cols, heads, head_dim, rows_h = dims
    hops = n // 2
    half_rows = rows // 2
    span = tp_count * pos
    kv_width = tp_count * cols
    group = tp_count * rows_h
    me, tp, gr = lax.axis_index("sp"), lax.axis_index("tp"), lax.axis_index("gr")
    place = ring_place(me, n)

    def owner_at(step):
        return ring_index(lax.rem(place + step + n, n), n)

    right, left = owner_at(1), owner_at(-1)
    partner = 1 - gr
    col_start = pl.multiple_of(tp * cols, 128)
    chunked = (width // n) % 128 == 0
    order = [0]
    for h in range(1, hops + 1):
        order.extend([-h, h] if h < hops else [h])
    chunk = width // n if chunked else width
    chunk_count = n if chunked else 1
    early = min(EARLY_HOPS, hops - 1) if chunked else -1
    cut = (2 * early + 1) * chunk if chunked else 0
    tail = slice(cut, width)
    crossing = 3 if chunked else 2

    def slot_of(step):
        if not chunked:
            return owner_at(step)
        return order.index(hops if abs(step) == hops else step)

    my_rows = pl.ds(pl.multiple_of(tp * pos, pos), pos)

    key_copy = pltpu.make_async_copy(key_weight, key_rows, local_sem.at[6])
    query_copy = pltpu.make_async_copy(queries, query, local_sem.at[4])
    weight_copies = [
        pltpu.make_async_copy(
            w.at[:, pl.ds(col_start, cols)], wts.at[part, slot_of(0)], local_sem.at[part]
        )
        for part, w in enumerate((key_weight, value_weight))
    ]

    def columns(i):
        return slice(i * chunk, (i + 1) * chunk)

    def columns_held(i):
        if not chunked:
            return slice(0, width)
        return pl.ds(pl.multiple_of(owner_at(order[i]) * chunk, 128), chunk)

    tok_copies = [
        pltpu.make_async_copy(
            tokens.at[:, :, columns_held(i)], tok.at[:, my_rows, columns(i)],
            tok_load.at[min(i, 1)],
        )
        for i in range(chunk_count)
    ]
    bias_copy = pltpu.make_async_copy(key_bias, bias_all, local_sem.at[3])
    own_bias_copy = pltpu.make_async_copy(own_bias, bias_own, local_sem.at[7])
    offset_copy = pltpu.make_async_copy(head_offset, offset, local_sem.at[5])
    for c in (
        weight_copies[1], tok_copies[0], query_copy, key_copy, *tok_copies[1:], weight_copies[0],
        bias_copy, own_bias_copy, offset_copy,
    ):
        c.start()

    tp_peers = [lax.rem(tp + k, tp_count) for k in range(1, tp_count)]
    barrier = pltpu.get_barrier_semaphore()
    ring = (right, left)

    def signal(semaphore, target):
        pl.semaphore_signal(semaphore, inc=1, device_id=target, device_id_type=MESH)

    for target in ring:
        pl.when(target > me)(functools.partial(signal, barrier, {"sp": target}))
    pl.when(gr == 0)(functools.partial(signal, barrier, {"gr": partner}))
    for peer in tp_peers:
        pl.when(peer > tp)(functools.partial(signal, barrier, {"tp": peer}))

    def part_of(piece):
        return 1 if piece < VALUE_SUBS else 0

    def rows_of(piece, core):
        part = part_of(piece)
        size = half_rows // (VALUE_SUBS if part == 1 else KEY_SUBS)
        sub = piece - (0 if part == 1 else VALUE_SUBS)
        return pl.ds(pl.multiple_of(core * half_rows + sub * size, size), size)

    def block_of(piece, step, core):
        if piece == MARK:
            return ubuf.at[slot_of(step)]
        return wts.at[part_of(piece), slot_of(step), rows_of(piece, core), :]

    def ring_copy(direction, hop, piece):
        return pltpu.make_async_remote_copy(
            src_ref=block_of(piece, step_of(direction, hop - 1), gr),
            dst_ref=block_of(piece, step_of(direction, hop), gr),
            send_sem=sends.at[1 if piece == MARK else 0],
            recv_sem=(last_recv.at[piece] if hop == hops else ring_recv.at[hop - 1, piece]),
            device_id={"sp": right if direction == 0 else left}, device_id_type=MESH,
        )

    def step_of(direction, hop):
        return -hop if direction == 0 else hop

    def used(direction, hop, piece):
        return hop < hops or (hop == hops and piece % 2 == direction)

    def pair_copy(direction, hop, piece, core):
        block = block_of(piece, step_of(direction, hop), core)
        return pltpu.make_async_remote_copy(
            src_ref=block, dst_ref=block,
            send_sem=sends.at[2], recv_sem=pair_recv.at[part_of(piece), hop - 1],
            device_id={"gr": partner}, device_id_type=MESH,
        )

    def peer_of(k):
        return lax.rem(tp + k + 1, tp_count)

    def source_of(k):
        return lax.rem(tp + tp_count - k - 1, tp_count)

    def tok_move(i, s, k, source):
        place_rows = pl.ds(pl.multiple_of(source * pos, pos), pos)
        block = tok.at[s, place_rows, columns(i)]
        return pltpu.make_async_remote_copy(
            src_ref=block, dst_ref=block,
            send_sem=sends.at[3], recv_sem=tok_recv.at[(i + 1) // 2 if chunked else 0],
            device_id={"tp": peer_of(k)}, device_id_type=MESH,
        )

    def bias_move(k, source, target):
        return pltpu.make_async_remote_copy(
            src_ref=bias_all.at[:, target], dst_ref=bias.at[source],
            send_sem=sends.at[4], recv_sem=receives.at[0],
            device_id={"tp": peer_of(k)}, device_id_type=MESH,
        )

    def read_move(k, which, source, target):
        if which == 0:
            out, into = pout.at[target, :, tail], pin.at[source, :, tail]
        elif which == 1:
            out, into = tot_out.at[target], tot_in.at[source]
        else:
            out, into = wout.at[target], win.at[source]
        return pltpu.make_async_remote_copy(
            src_ref=out, dst_ref=into,
            send_sem=sends.at[5 + which], recv_sem=receives.at[1 + which],
            device_id={"tp": peer_of(k)}, device_id_type=MESH,
        )

    def launch(c):
        c.start()

    def counted(ref, sem):
        return pltpu.make_async_copy(ref, ref, sem)

    issued = [0]

    def load_tokens(i):
        if i == 0:
            tok_copies[0].wait()
        else:
            counted(tok.at[:, my_rows, chunk:], tok_load.at[1]).wait()

    def send_tokens(upto, ahead=None):
        upto = min(upto, chunk_count * seqs)
        for i, s in (divmod(unit, seqs) for unit in range(issued[0], upto)):
            if s == 0 and i < 2 and ahead is not True:
                load_tokens(i)
            for k in range(tp_count - 1):

                def start(i=i, s=s, k=k):
                    launch(tok_move(i, s, k, tp))

                if ahead is None:
                    start()
                else:
                    pl.when((peer_of(k) > tp) == ahead)(start)
        if ahead is not False:
            issued[0] = upto

    def open_ring(piece, ahead=None):
        for direction in range(2):
            if not used(direction, 1, piece):
                continue

            def start(direction=direction):
                launch(ring_copy(direction, 1, piece))

            if ahead is None:
                start()
            else:
                pl.when((ring[direction] > me) == ahead)(start)

    def arrived(hop, piece):
        if hop == hops:
            last = next(d for d in range(2) if used(d, hop, piece))
            ring_copy(last, hop, piece).wait_recv()
        elif piece == MARK:
            counted(ubuf.at[pl.ds(0, 2)], ring_recv.at[hop - 1, piece]).wait()
        else:
            part = part_of(piece)
            both = 2 * (half_rows // (VALUE_SUBS if part == 1 else KEY_SUBS))
            counted(wts.at[part, 0, pl.ds(0, both)], ring_recv.at[hop - 1, piece]).wait()

    def pass_on(hop, piece):
        arrived(hop, piece)
        for direction in range(2):
            if not used(direction, hop, piece):
                continue
            if hop < hops and used(direction, hop + 1, piece):
                launch(ring_copy(direction, hop + 1, piece))
            if piece != MARK:
                launch(pair_copy(direction, hop, piece, gr))

    def project():
        query_copy.wait()
        key_copy.wait()
        row = lax.broadcasted_iota(jnp.int32, (group, kv_width), 0)
        col_head = lax.broadcasted_iota(jnp.int32, (group, kv_width), 1) // head_dim
        inner = lax.rem(row, rows_h)
        mine = (row // rows_h * heads + inner == col_head) & (inner < heads)
        q = query[...].astype(F32)
        q_rows = jnp.concatenate(
            [jnp.where(mine, q[s : s + 1], 0.0) for s in range(seqs)], axis=0
        ).astype(BF16)
        ubuf[slot_of(0)] = lax.dot_general(
            q_rows, key_rows[...], (((1,), (1,)), ((), ())), preferred_element_type=F32
        ).astype(BF16)

    def greet():
        behind = (right < me).astype(jnp.int32) + (left < me).astype(jnp.int32) + gr + tp
        pl.when(behind > 0)(lambda: pl.semaphore_wait(barrier, behind))
        for direction in range(2):
            target = ring[direction]
            semaphore = ready.at[1 - direction]
            pl.when(target < me)(functools.partial(signal, semaphore, {"sp": target}))
        pl.when(gr == 1)(functools.partial(signal, ready.at[2], {"gr": partner}))
        for peer in tp_peers:
            pl.when(peer < tp)(functools.partial(signal, ready.at[3], {"tp": peer}))

    def begin(steps):
        with jax.named_scope("greet"):
            greet()
        for kind, *what in steps:
            if kind == OPEN:
                if what[0] != MARK:
                    weights_here(part_of(what[0]))
                open_ring(what[0], False)
            elif kind == TOKENS:
                send_tokens(what[0], False)
            elif kind == PROJECT:
                with jax.named_scope("project"):
                    project()
        with jax.named_scope("ready"):
            for direction in range(2):
                semaphore = ready.at[direction]
                pl.when(ring[direction] > me)(
                    functools.partial(pl.semaphore_wait, semaphore, 1)
                )
            ahead = tp_count - 1 - tp
            pl.when(ahead > 0)(lambda: pl.semaphore_wait(ready.at[3], ahead))
        for kind, *what in steps:
            if kind == OPEN:
                open_ring(what[0], True)
            elif kind == TOKENS:
                send_tokens(what[0], True)
        pl.when(gr == 0)(functools.partial(pl.semaphore_wait, ready.at[2], 1))
        bias_copy.wait()
        for k in range(tp_count - 1):
            launch(bias_move(k, tp, peer_of(k)))

    def read():
        own_bias_copy.wait()
        offset_copy.wait()
        for owner in range(n):
            ucat[:, owner * rows : (owner + 1) * rows] = ubuf[owner]
        total_heads = offset.shape[1]
        pick_row = lax.broadcasted_iota(jnp.int32, (group, total_heads), 0)
        pick_inner = lax.rem(pick_row, rows_h)
        pick = (
            lax.broadcasted_iota(jnp.int32, (group, total_heads), 1)
            == pick_row // rows_h * heads + pick_inner
        ) & (pick_inner < heads)
        offset_col = jnp.sum(jnp.where(pick, offset[...], 0.0), axis=1, keepdims=True)
        logits = []
        for s in range(seqs):
            logits.append(
                lax.dot_general(
                    ucat[s * group : (s + 1) * group, :], tok[s, my_rows, :],
                    (((1,), (1,)), ((), ())), preferred_element_type=F32,
                )
                * (head_dim**-0.5)
                + offset_col
                + bias_own[s].astype(F32)
            )
        logits = jnp.concatenate(logits, axis=0)
        soft = jnp.log1p(jnp.exp(-jnp.abs(logits)))
        fading = -jnp.maximum(logits, 0.0) - soft
        taking = jnp.minimum(logits, 0.0) - soft
        high = fading.astype(BF16)
        rest = fading - high.astype(F32)
        mid = rest.astype(BF16)
        low = (rest - mid.astype(F32)).astype(BF16)
        later = (
            lax.broadcasted_iota(jnp.int32, (pos, pos), 0)
            > lax.broadcasted_iota(jnp.int32, (pos, pos), 1)
        ).astype(F32).astype(BF16)
        sums = jnp.dot(
            jnp.concatenate([high, mid, low], axis=0), later, preferred_element_type=F32
        )
        m = seqs * group
        within = sums[:m] + sums[m : 2 * m] + sums[2 * m :]
        weights = jnp.exp(taking + within)
        totals = jnp.sum(fading, axis=1, keepdims=True)
        spread = jnp.broadcast_to(totals, (m, 128))
        weighted = [
            jnp.dot(
                weights[s * group : (s + 1) * group].astype(BF16), tok[s, my_rows, :],
                preferred_element_type=F32,
            )
            for s in range(seqs)
        ]
        for t in range(tp_count):
            at = slice(t * rows_h, (t + 1) * rows_h)
            wout[t] = jnp.concatenate(
                [weights[s * group : (s + 1) * group][at] for s in range(seqs)], axis=0
            ).astype(BF16)
            tot_out[t] = jnp.concatenate(
                [spread[s * group + t * rows_h : s * group + (t + 1) * rows_h] for s in range(seqs)],
                axis=0,
            )
            whole = jnp.concatenate([weighted[s][at] for s in range(seqs)], axis=0)
            upper = whole.astype(BF16)
            pout[t] = upper
            plow[t] = (whole - upper.astype(F32)).astype(BF16)
        for k in range(tp_count - 1):
            for which in range(crossing):
                launch(read_move(k, which, tp, peer_of(k)))
        pin[tp] = pout[tp]
        tot_in[tp] = tot_out[tp]

    seen = set()

    def weights_here(part):
        if ("weights", part) not in seen:
            seen.add(("weights", part))
            weight_copies[part].wait()

    def pair_ready(part, hop):
        if hop == 0 or ("pair", part, hop) in seen:
            return
        seen.add(("pair", part, hop))
        held = wts.at[part, slot_of(hop)]
        if hop == hops:
            held = held.at[pl.ds(0, half_rows), :]
        counted(held, pair_recv.at[part, hop - 1]).wait()

    def tokens_ready(hop, s):
        if ("tok", hop) in seen or tp_count == 1:
            return
        seen.add(("tok", hop))
        first, end = slots_of_hop(hop) if chunked else (0, 1)
        counted(
            tok.at[:, pl.ds(0, (tp_count - 1) * pos), slice(first * chunk, end * chunk)],
            tok_recv.at[hop],
        ).wait()

    def slots_of_hop(hop):
        if hop == 0:
            return 0, 1
        first = 1 + 2 * (hop - 1)
        return first, min(first + 2, n)

    def multiply(part, hop, s):
        if not chunked:
            return
        first, end = slots_of_hop(hop)
        with jax.named_scope(f"multiply{part}_{hop}_{s}"):
            if hop == 0:
                weights_here(part)
            pair_ready(part, hop)
            tokens_ready(hop, s)
            y = jnp.dot(
                tok[s, :, first * chunk : end * chunk],
                wts[part, first:end].reshape((end - first) * rows, cols),
                preferred_element_type=F32,
            )
            if hop > 0:
                y = acc[part, s] + y
            if hop < hops:
                acc[part, s] = y
            else:
                kv[part, s] = y.astype(BF16)

    def leave():
        if chunked:
            pair_ready(0, hops)
            for s in range(seqs):
                tokens_ready(hops, s)

    def mix_move(k, source):
        return pltpu.make_async_remote_copy(
            src_ref=packed.at[source], dst_ref=packed.at[source],
            send_sem=sends.at[8], recv_sem=receives.at[4],
            device_id={"sp": lax.rem(me + k, n)}, device_id_type=MESH,
        )

    def mix():
        with jax.named_scope("await_products"):
            if tp_count > 1:
                others = pl.ds(0, tp_count - 1)
                counted(pin.at[others, :, tail], receives.at[1]).wait()
                counted(tot_in.at[others], receives.at[2]).wait()
                if chunked:
                    counted(win.at[others], receives.at[3]).wait()
            for hop in range(1, hops + 1):
                pair_ready(1, hop)
        if chunked:
            for h in range(early + 1):
                for s in range(seqs):
                    tokens_ready(h, s)
            for k in range(tp_count - 1):
                source = source_of(k)
                where = pl.ds(pl.multiple_of(source * pos, pos), pos)
                held = win[source].astype(F32)
                pin[source, :, 0:cut] = jnp.concatenate(
                    [
                        jnp.dot(
                            held[s * rows_h : (s + 1) * rows_h].astype(BF16),
                            tok[s, where, 0:cut], preferred_element_type=F32,
                        )
                        for s in range(seqs)
                    ],
                    axis=0,
                ).astype(BF16)
        count = seqs * rows_h
        given = jnp.concatenate([pin[t] for t in range(tp_count)] + [plow[tp]], axis=0)
        product = jnp.dot(
            given, wts[1].reshape(width, cols), preferred_element_type=F32
        )
        carry = jnp.zeros((count, 1), F32)
        mixture = jnp.zeros((count, cols), F32)
        for t in range(tp_count - 1, -1, -1):
            term = product[t * count : (t + 1) * count]
            term = term + jnp.where(tp == t, 1.0, 0.0) * product[tp_count * count :]
            mixture = mixture + jnp.exp(carry) * term
            carry = carry + tot_in[t][:, :1]
        own = lax.broadcasted_iota(jnp.int32, (rows_h, cols), 0) == (
            lax.broadcasted_iota(jnp.int32, (rows_h, cols), 1) // head_dim
        )
        for s in range(seqs):
            at = slice(s * rows_h, (s + 1) * rows_h)
            packed[me, s : s + 1] = jnp.sum(
                jnp.where(own, mixture[at], 0.0), axis=0, keepdims=True
            )
            packed[me, seqs + s : seqs + s + 1] = jnp.sum(
                jnp.where(own, carry[at], 0.0), axis=0, keepdims=True
            )
        for k in range(1, n):
            launch(mix_move(k, me))

    steps = list(plan(hops, seqs))
    opening = next(i for i, step in enumerate(steps) if step[0] == PASS)
    begin(steps[:opening])
    for kind, *what in steps[opening:]:
        if kind == OPEN:
            if what[0] != MARK:
                weights_here(part_of(what[0]))
            open_ring(what[0])
        elif kind == PASS:
            with jax.named_scope(f"pass{what[0]}_{what[1]}"):
                pass_on(*what)
        elif kind == TOKENS:
            send_tokens(what[0])
        elif kind == MULTIPLY:
            if what[:2] != [0, hops]:
                multiply(*what)
        elif kind == READ:
            with jax.named_scope("read"):
                read()
        elif kind == MIX:
            with jax.named_scope("mix"):
                mix()

    leave()
    if not chunked:
        for s in range(seqs):
            tokens_ready(0, s)
        for hop in range(1, hops + 1):
            pair_ready(0, hop)
        tile = pos
        for part in range(2):
            w = wts[part].reshape(width, cols)

            def body(j, carry):
                s, r = j // (span // tile), lax.rem(j, span // tile)
                where = pl.ds(pl.multiple_of(r * tile, tile), tile)
                y = jnp.dot(tok[s, where, :], w, preferred_element_type=F32)
                kv[part, s, where, :] = y.astype(BF16)
                return carry

            lax.fori_loop(0, seqs * (span // tile), body, 0)

    if tp_count > 1:
        counted(bias.at[pl.ds(0, tp_count - 1)], receives.at[0]).wait()
    bias[tp] = bias_all[:, tp]
    for s in range(seqs):
        bias_out[s] = jnp.concatenate([bias[t, s] for t in range(tp_count)], axis=1)
    with jax.named_scope("await_mix"):
        counted(packed.at[pl.ds(0, n - 1)], receives.at[4]).wait()
    with jax.named_scope("drain"):
        counted(wts.at[0, pl.ds(0, n - 1)], sends.at[0]).wait()
        counted(ubuf.at[pl.ds(0, n - 1)], sends.at[1]).wait()
        counted(wts.at[0, pl.ds(0, n - 1)], sends.at[2]).wait()
        if tp_count > 1:
            others = pl.ds(0, tp_count - 1)
            counted(tok.at[:, pl.ds(0, (tp_count - 1) * pos), :], sends.at[3]).wait()
            counted(bias.at[others], sends.at[4]).wait()
            counted(pin.at[others, :, tail], sends.at[5]).wait()
            counted(tot_in.at[others], sends.at[6]).wait()
            if chunked:
                counted(win.at[others], sends.at[7]).wait()
        counted(packed.at[pl.ds(0, n - 1)], sends.at[8]).wait()


def finish(
    n, head_dim, kv, bias, packed, tok, wts, acc,
    key_out, value_out, bias_out, reading_out, key, reading, sems,
):
    _, _, rows, _ = wts.shape
    chunked = rows % 128 == 0
    moves = [
        pltpu.make_async_copy(kv.at[1], value_out, sems.at[0]),
        pltpu.make_async_copy(bias, bias_out, sems.at[1]),
    ]
    if not chunked:
        moves.append(pltpu.make_async_copy(kv.at[0], key_out, sems.at[2]))
    for c in moves:
        c.start()
    if chunked:
        for s in range(key_out.shape[0]):
            y = jnp.dot(
                tok[s, :, (n - 1) * rows :], wts[0, n - 1], preferred_element_type=F32
            )
            key[s] = (acc[0, s] + y).astype(BF16)
            moves.append(pltpu.make_async_copy(key.at[s], key_out.at[s], sems.at[4 + s]))
            moves[-1].start()
    seqs, cols = reading_out.shape
    rows_h = max(8, cols // head_dim)
    row_id = lax.broadcasted_iota(jnp.int32, (rows_h, cols), 0)
    col_id = lax.broadcasted_iota(jnp.int32, (rows_h, cols), 1)
    own = row_id == col_id // head_dim
    mixture = jnp.zeros((seqs, cols), F32)
    carry = jnp.zeros((seqs, cols), F32)
    for at in range(n - 1, -1, -1):
        mixture = mixture + jnp.exp(carry) * packed[at, :seqs]
        carry = carry + packed[at, seqs:]
    for s in range(seqs):
        x = mixture[s : s + 1]
        mean = jnp.sum(jnp.where(own, x * x, 0.0), axis=1, keepdims=True) / head_dim
        scale = jnp.sum(jnp.where(own, lax.rsqrt(mean + 1e-06), 0.0), axis=0, keepdims=True)
        reading[s : s + 1] = x * scale
    moves.append(pltpu.make_async_copy(reading, reading_out, sems.at[3]))
    moves[-1].start()
    for c in moves:
        c.wait()


def per_device(tokens, key_weight, value_weight, queries, head_offset, key_bias):
    n, tp_count = lax.axis_size("sp"), lax.axis_size("tp")
    assert n % 2 == 0 and lax.axis_size("gr") == 2
    seqs, pos, width = tokens.shape
    rows, kv_width = key_weight.shape
    head_count = head_offset.shape[0]
    head_dim = kv_width // head_count
    cols = kv_width // tp_count
    heads = head_count // tp_count
    rows_h = max(8, heads)
    span = tp_count * pos
    hops = n // 2
    bias_rows = jnp.transpose(key_bias, (0, 2, 1)).reshape(seqs, tp_count, heads, pos)
    group = tp_count * rows_h
    own_bias = jnp.pad(bias_rows, ((0, 0), (0, 0), (0, rows_h - heads), (0, 0)))
    own_bias = own_bias.reshape(seqs, group, pos)
    dims = (n, tp_count, seqs, pos, width, rows, cols, heads, head_dim, rows_h)
    groups = hops + 1 if (width // n) % 128 == 0 else 1
    dma = pltpu.SemaphoreType.DMA
    kv, bias_held, packed, tok, wts, acc = pl.pallas_call(
        functools.partial(kernel, dims),
        out_shape=(
            jax.ShapeDtypeStruct((2, seqs, span, cols), BF16),
            jax.ShapeDtypeStruct((seqs, heads, span), BF16),
            jax.ShapeDtypeStruct((n, 2 * seqs, cols), F32),
            jax.ShapeDtypeStruct((seqs, span, width), BF16),
            jax.ShapeDtypeStruct((2, n, rows, cols), BF16),
            jax.ShapeDtypeStruct((2, seqs, span, cols), F32),
        ),
        in_specs=[pl.BlockSpec(memory_space=pltpu.HBM)] * 7,
        out_specs=[pl.BlockSpec(memory_space=pltpu.VMEM)] * 6,
        scratch_shapes=[
            pltpu.VMEM((tp_count, seqs, heads, pos), BF16),
            pltpu.VMEM(queries.shape, BF16),
            pltpu.VMEM((1, head_count), F32),
            pltpu.VMEM((seqs, tp_count, heads, pos), BF16),
            pltpu.VMEM((seqs, group, pos), BF16),
            pltpu.VMEM((rows, kv_width), BF16),
            pltpu.VMEM((n, seqs * group, rows), BF16),
            pltpu.VMEM((seqs * group, width), BF16),
            pltpu.VMEM((tp_count, seqs * rows_h, width), BF16),
            pltpu.VMEM((tp_count, seqs * rows_h, width), BF16),
            pltpu.VMEM((tp_count, seqs * rows_h, width), BF16),
            pltpu.VMEM((tp_count, seqs * rows_h, 128), F32),
            pltpu.VMEM((tp_count, seqs * rows_h, 128), F32),
            pltpu.VMEM((tp_count, seqs * rows_h, pos), BF16),
            pltpu.VMEM((tp_count, seqs * rows_h, pos), BF16),
            dma((8,)),
            dma((2,)),
            dma((9,)),
            dma((5,)),
            dma((hops - 1, MARK + 1)),
            dma((MARK + 1,)),
            dma((2, hops)),
            dma((groups,)),
            pltpu.SemaphoreType.REGULAR((4,)),
        ],
        compiler_params=pltpu.CompilerParams(
            collective_id=0, has_side_effects=True, vmem_limit_bytes=36 * 2**20
        ),
        name="prefill",
    )(*(pltpu.with_memory_space_constraint(a, pltpu.HBM) for a in (tokens, key_weight, value_weight, queries, head_offset.reshape(1, head_count), bias_rows, own_bias)))
    key_cache, value_cache, bias_cache, reading = pl.pallas_call(
        functools.partial(finish, n, head_dim),
        out_shape=(
            jax.ShapeDtypeStruct((seqs, span, cols), BF16),
            jax.ShapeDtypeStruct((seqs, span, cols), BF16),
            jax.ShapeDtypeStruct((seqs, heads, span), BF16),
            jax.ShapeDtypeStruct((seqs, cols), F32),
        ),
        in_specs=[
            pl.BlockSpec(memory_space=pl.ANY),
            pl.BlockSpec(memory_space=pl.ANY),
            *[pl.BlockSpec(memory_space=pltpu.VMEM)] * 4,
        ],
        out_specs=[
            pl.BlockSpec(memory_space=pl.ANY),
            pl.BlockSpec(memory_space=pl.ANY),
            pl.BlockSpec(memory_space=pl.ANY),
            pl.BlockSpec(memory_space=pl.ANY),
        ],
        scratch_shapes=[
            pltpu.VMEM((seqs, span, cols), BF16), pltpu.VMEM((seqs, cols), F32), dma((4 + seqs,))
        ],
        compiler_params=pltpu.CompilerParams(vmem_limit_bytes=16 * 2**20),
        name="finish",
    )(kv, bias_held, packed, tok, wts, acc)
    return key_cache, value_cache, jnp.transpose(bias_cache, (0, 2, 1)), reading


def solution(mesh):
    in_specs = (
        P("gr", ("sp", "tp"), None),
        P("sp", None),
        P("sp", None),
        P("gr", None),
        P(),
        P("gr", ("sp", "tp"), None),
    )
    out_specs = (P("gr", "sp", "tp"), P("gr", "sp", "tp"), P("gr", "sp", "tp"), P("gr", "tp"))
    return jax.shard_map(
        per_device, mesh=mesh, in_specs=in_specs, out_specs=out_specs, check_vma=False
    )
```
